32 devices in a mesh: sp: 8 (over z, x), tp: 4 (over y, core).
Axes of the slice: x: 2, y: 2, z: 4, core: 2. Of those that a mesh axis runs over, the one named last changes fastest.
Arguments:
- latents: bfloat16 [4096, 2048], P(('sp', 'tp')), may hold values from -6 to 6
- context: bfloat16 [512, 2048], P('sp'), may hold values from -6 to 6
- cond: float32 [2048], P('sp'), may hold values from -6 to 6
- ctx_cond: float32 [2048], P('sp'), may hold values from -6 to 6
- mod_weight: float32 [2048, 6144], P('sp', 'tp'), may hold values from -0.125 to 0.125
- query_weight: bfloat16 [2048, 2048], P(None, 'tp'), may hold values from -1 to 1, as said below
- key_matrix: bfloat16 [2048, 1024], P(None, 'tp'), may hold values from -1 to 1, as said below
- value_matrix: bfloat16 [2048, 1024], P(None, 'tp'), may hold values from -0.125 to 0.125
- out_weight: bfloat16 [2048, 2048], P('tp'), may hold values from -0.125 to 0.125
- query_gain: float32 [128], replicated, may hold values from 0.7 to 7
- key_gain: float32 [128], replicated, may hold values from 0.7 to 7
Outputs:
- updated: bfloat16 [4096, 2048], P(('sp', 'tp'))
The draws below stay inside these ranges and needn't reach their ends.
Inputs may be any that keep to these rules, and one draw needn't show every extreme that they name: `query_weight`: entries of order 2048 to the power -1/2. `key_matrix`: entries of order 2048 to the power -1/2.
All inputs are finite; a program needn't handle non-finite values.
Results may differ from the reference program's by a relative error of at most 0.0085.
The reference program's roundings to bfloat16 on the way count: a program that leaves them out, or rounds other values in their place, can miss the bound.
Values may be sent and summed in bfloat16 or wider, within the bound.
A program may use at most 128 MiB of HBM per device.

```python
import math
import jax
import jax.numpy as jnp
from jax import lax

MODEL_DIM = 2048
HEAD_SIZE = 128
QUERY_HEAD_COUNT = 16
KEY_VALUE_HEADS = 8
GRID_W = 64
CTX = 512
TOKENS = 4096


def paired_weights(key):
    query_base = jax.random.normal(jax.random.fold_in(key, 11), (MODEL_DIM, QUERY_HEAD_COUNT * HEAD_SIZE), jnp.float32) * MODEL_DIM ** (-0.5)
    key_start = jax.random.normal(jax.random.fold_in(key, 12), (MODEL_DIM, KEY_VALUE_HEADS * HEAD_SIZE), jnp.float32) * MODEL_DIM ** (-0.5)
    return (query_base, key_start)


def draw_query_weight(key, part):
    return paired_weights(key)[0].astype(jnp.bfloat16)


def draw_key_matrix(key, part):
    return paired_weights(key)[1].astype(jnp.bfloat16)


def draw_query_gain(key, part):
    return jax.random.uniform(jax.random.fold_in(key, 21), (HEAD_SIZE,), jnp.float32, 0.7, 1.3)


def draw_key_gain(key, part):
    return jax.random.uniform(jax.random.fold_in(key, 22), (HEAD_SIZE,), jnp.float32, 0.7, 1.3)


def shard_levels(rng, dims, shards, smallest, high):
    loudness, own = 1.0, jax.random.fold_in(rng, 6)
    for position, parts in shards:
        draws = jnp.exp(jax.random.uniform(jax.random.fold_in(own, position), (parts,), jnp.float32, smallest / len(shards), high / len(shards)))
        loudness = loudness * jnp.repeat(draws, dims[position] // parts).reshape([-1 if axis == position else 1 for axis in range(len(dims))])
    return loudness


def centred(stream_key, dims, width, most, pieces=(), kind=jnp.bfloat16):
    result = jax.random.normal(stream_key, dims, jnp.float32) * width
    if len(pieces) > 0:
        result = shard_levels(stream_key, dims, pieces, -0.22, 0.18) * result
    return jnp.clip(result, min=-most, max=most).astype(kind)


def setup_inputs(seed: int = 0) -> dict:
    key_of = jax.random.split(jax.random.key(seed), 12)
    latents = centred(key_of[0], (TOKENS, MODEL_DIM), 1.0, 6.0, ((0, 32),))
    context = centred(key_of[1], (CTX, MODEL_DIM), 1.0, 6.0, ((0, 8),))
    cond = centred(key_of[2], (MODEL_DIM,), 1.0, 6.0, ((0, 8),), jnp.float32)
    ctx_cond = centred(key_of[3], (MODEL_DIM,), 1.0, 6.0, ((0, 8),), jnp.float32)
    mod_weight = centred(key_of[4], (MODEL_DIM, 3 * MODEL_DIM), MODEL_DIM ** -0.5, 0.125, ((0, 8), (1, 4)), jnp.float32)
    query_weight = draw_query_weight(jax.random.fold_in(key_of[11], 71), 0)
    key_matrix = draw_key_matrix(jax.random.fold_in(key_of[11], 71), 0)
    value_matrix = centred(key_of[7], (MODEL_DIM, KEY_VALUE_HEADS * HEAD_SIZE), MODEL_DIM ** -0.5, 0.125, ((1, 4),))
    out_weight = centred(key_of[8], (QUERY_HEAD_COUNT * HEAD_SIZE, MODEL_DIM), (QUERY_HEAD_COUNT * HEAD_SIZE) ** -0.5, 0.125, ((0, 4),))
    query_gain = draw_query_gain(jax.random.fold_in(key_of[11], 71), 0)
    key_gain = draw_key_gain(jax.random.fold_in(key_of[11], 71), 0)
    return {"latents": latents, "context": context, "cond": cond, "ctx_cond": ctx_cond, "mod_weight": mod_weight, "query_weight": query_weight, "key_matrix": key_matrix, "value_matrix": value_matrix, "out_weight": out_weight, "query_gain": query_gain, "key_gain": key_gain}


NORM_EPS = 1e-06
ROPE_BASE = 10000.0

def normalize(latent_value_rows):
    return latent_value_rows * lax.rsqrt(lax.optimization_barrier(jnp.mean(latent_value_rows * latent_value_rows, axis=-1, keepdims=True)) + NORM_EPS)

def rotate(latent_value_rows, positions):
    quarter = latent_value_rows.shape[-1] // 2
    inv_freq = ROPE_BASE ** (-jnp.arange(quarter, dtype=jnp.float32) / quarter)
    angles = positions.astype(jnp.float32)[:, None] * inv_freq[None, :]
    cos_table = jnp.cos(angles)[:, None, :]
    sin_table = jnp.sin(angles)[:, None, :]
    first, second = (latent_value_rows[..., :quarter], latent_value_rows[..., quarter:])
    return jnp.concatenate([first * cos_table - second * sin_table, second * cos_table + first * sin_table], axis=-1)

def axial(latent_value_rows, positions):
    half_dim = latent_value_rows.shape[-1] // 2
    return jnp.concatenate([rotate(latent_value_rows[..., :half_dim], positions // GRID_W), rotate(latent_value_rows[..., half_dim:], positions % GRID_W)], axis=-1)

def modulate(latent_value_rows, mod_row):
    model_width = latent_value_rows.shape[-1]
    shift_vec = mod_row[:model_width]
    scale_vec = mod_row[model_width:2 * model_width]
    return (normalize(latent_value_rows.astype(jnp.float32)) * (1.0 + scale_vec) + shift_vec).astype(jnp.bfloat16)

def reference(latents, context, cond, ctx_cond, mod_weight, query_weight, key_matrix, value_matrix, out_weight, query_gain, key_gain):
    model_width = latents.shape[1]
    latent_count = latents.shape[0]
    prefix_count = context.shape[0]
    modulation = jnp.dot(jax.nn.silu(jnp.stack([cond, ctx_cond])), mod_weight, precision=lax.Precision.HIGHEST)
    gate_vec = modulation[0, 2 * model_width:]
    normalised_rows = modulate(latents, modulation[0])
    prefix_normalised = modulate(context, modulation[1])
    positions = jnp.arange(latent_count, dtype=jnp.int32)
    query_rows = jnp.dot(normalised_rows, query_weight, preferred_element_type=jnp.float32).reshape(latent_count, QUERY_HEAD_COUNT, HEAD_SIZE)
    query_rows = axial(normalize(query_rows) * query_gain, positions).astype(jnp.bfloat16)
    latent_key_rows = jnp.dot(normalised_rows, key_matrix, preferred_element_type=jnp.float32).reshape(latent_count, KEY_VALUE_HEADS, HEAD_SIZE)
    latent_key_rows = axial(normalize(latent_key_rows) * key_gain, positions).astype(jnp.bfloat16)
    latent_value_rows = jnp.dot(normalised_rows, value_matrix, preferred_element_type=jnp.float32).reshape(latent_count, KEY_VALUE_HEADS, HEAD_SIZE).astype(jnp.bfloat16)
    prefix_keys = jnp.dot(prefix_normalised, key_matrix, preferred_element_type=jnp.float32).reshape(prefix_count, KEY_VALUE_HEADS, HEAD_SIZE)
    prefix_keys = (normalize(prefix_keys) * key_gain).astype(jnp.bfloat16)
    prefix_values = jnp.dot(prefix_normalised, value_matrix, preferred_element_type=jnp.float32).reshape(prefix_count, KEY_VALUE_HEADS, HEAD_SIZE).astype(jnp.bfloat16)
    keys_all = jnp.concatenate([prefix_keys, latent_key_rows], axis=0).astype(jnp.float32)
    values_all = jnp.concatenate([prefix_values, latent_value_rows], axis=0).astype(jnp.float32)
    lift = math.log(latent_count / (2.0 * prefix_count))
    lift_row = jnp.concatenate([jnp.full((prefix_count,), lift, jnp.float32), jnp.zeros((latent_count,), jnp.float32)])
    group_size = QUERY_HEAD_COUNT // KEY_VALUE_HEADS
    rows_per_block = math.gcd(latent_count, 256)
    token_blocks = query_rows.reshape(latent_count // rows_per_block, rows_per_block, KEY_VALUE_HEADS, group_size, HEAD_SIZE)
    inv_root = HEAD_SIZE ** (-0.5)

    def one_block(block):
        scores = jnp.einsum('qhgd,khd->hgqk', block.astype(jnp.float32), keys_all) * inv_root + lift_row
        top_row = lax.optimization_barrier(jnp.max(scores, axis=-1, keepdims=True))
        weights = jnp.exp(scores - top_row)
        total = lax.optimization_barrier(jnp.sum(weights, axis=-1))
        probs = lax.optimization_barrier(weights.astype(jnp.bfloat16)).astype(jnp.float32)
        summed = jnp.einsum('hgqk,khd->qhgd', probs, values_all)
        return (summed / jnp.transpose(total, (2, 0, 1))[..., None]).astype(jnp.bfloat16)
    attended = lax.map(one_block, token_blocks).reshape(latent_count, QUERY_HEAD_COUNT * HEAD_SIZE)
    mixed = jnp.dot(attended, out_weight, preferred_element_type=jnp.float32)
    return (latents.astype(jnp.float32) + gate_vec * normalize(mixed)).astype(jnp.bfloat16)
```

```python
import functools
import math

import jax
import jax.numpy as jnp
from jax import lax
from jax.experimental import pallas as pl
from jax.experimental.pallas import tpu as pltpu
from jax.sharding import PartitionSpec as P

GRID_W = 64
NORM_EPS = 1e-06
ROPE_BASE = 10000.0
MESH = pl.DeviceIdType.MESH
BF16 = jnp.bfloat16
F32 = jnp.float32
VMEM_BYTES = 67043328


def row_size(sp_count):
    size = 1
    while 4 * size * size <= sp_count:
        size *= 2
    return size


def tables(positions, head_dim):
    quarter = head_dim // 4
    inv_freq = ROPE_BASE ** (-jnp.arange(quarter, dtype=F32) / quarter)
    where = jnp.stack([positions // GRID_W, positions % GRID_W]).astype(F32)
    angles = where[:, None, :] * inv_freq[None, :, None]
    return jnp.cos(angles), jnp.sin(angles)


def remote(src, dst, send, recv, dev):
    return pltpu.make_async_remote_copy(
        src_ref=src, dst_ref=dst, send_sem=send, recv_sem=recv, device_id=dev, device_id_type=MESH
    )


def front_kernel(
    sp_count, tp_count, head_dim,
    cond_ref, cond_1_ref, mw_hbm, lat_hbm, ctx_ref, wq_hbm, wk_hbm, wv_hbm, qg_ref, kg_ref, cos_ref, sin_ref,
    qt_ref, k_ref, vt_ref, ckv_ref, gate_ref,
    mw, lat, wq, wk, wv, part, tot, mod, xn, load_sem,
    lat_send, lat_recv, part_send, part_recv, tot_send, tot_recv,
    wo_hbm, wo_vm, wo_sem,
):
    s, t = lax.axis_index("sp"), lax.axis_index("tp")
    y, c = t // 2, t % 2
    y_count = tp_count // 2
    partner = y * 2 + 1 - c
    rows = lat.shape[1]
    width = lat.shape[2]
    model_cols = mod.shape[1]

    own = pltpu.make_async_copy(lat_hbm, lat.at[t], load_sem.at[0])
    own.start()
    loads = [
        pltpu.make_async_copy(a, b, load_sem.at[1 + i])
        for i, (a, b) in enumerate(((mw_hbm, mw), (wq_hbm, wq), (wk_hbm, wk), (wv_hbm, wv)))
    ]
    for one in loads:
        one.start()

    pltpu.make_async_copy(wo_hbm, wo_vm, wo_sem.at[0]).start()

    barrier = pltpu.get_barrier_semaphore()
    for j in range(1, sp_count):
        pl.semaphore_signal(barrier, inc=1, device_id=((s + j) % sp_count, t), device_id_type=MESH)
    for j in range(1, tp_count):
        pl.semaphore_signal(barrier, inc=1, device_id=(s, (t + j) % tp_count), device_id_type=MESH)
    pl.semaphore_wait(barrier, sp_count + tp_count - 2)

    own.wait()
    sends = []
    for j in range(1, y_count):
        peer = ((y + j) % y_count) * 2 + c
        sends.append(remote(lat.at[t], lat.at[t], lat_send.at[j], lat_recv.at[t], (s, peer)))
    sends.append(remote(lat.at[t], lat.at[t], lat_send.at[0], lat_recv.at[t], (s, partner)))
    for one in sends:
        one.start()

    loads[0].wait()
    lines = lax.broadcasted_iota(jnp.int32, (8, cond_ref.shape[1]), 0)
    cond = jnp.where(lines == 0, cond_ref[...], jnp.where(lines == 1, cond_1_ref[...], 0.0))
    cond = cond * jax.nn.sigmoid(cond)
    part[s] = jnp.dot(
        cond, mw[...], precision=lax.Precision.HIGHEST, preferred_element_type=F32
    )[:2]
    more = [
        remote(part.at[s], part.at[s], part_send.at[j], part_recv.at[s], ((s + j) % sp_count, t))
        for j in range(1, sp_count)
    ]
    for one in more:
        one.start()
    for j in range(1, sp_count):
        src = (s + j) % sp_count
        remote(part.at[src], part.at[src], part_send.at[0], part_recv.at[src], (s, t)).wait_recv()
    total = part[0]
    for j in range(1, sp_count):
        total = total + part[j]
    tot[t] = total
    last = [
        remote(tot.at[t], tot.at[t], tot_send.at[j], tot_recv.at[t], (s, (t + j) % tp_count))
        for j in range(1, tp_count)
    ]
    for one in last:
        one.start()
    for j in range(1, tp_count):
        src = (t + j) % tp_count
        remote(tot.at[src], tot.at[src], tot_send.at[0], tot_recv.at[src], (s, t)).wait_recv()
    cols = model_cols // tp_count
    for j in range(tp_count):
        mod[:, j * cols : (j + 1) * cols] = tot[j]
    gate_ref[...] = mod[0:1, 2 * width :]

    def modulate(x, r):
        x = x.astype(F32)
        scaled = x * lax.rsqrt(jnp.mean(x * x, axis=-1, keepdims=True) + NORM_EPS)
        shift, scale = mod[r : r + 1, :width], mod[r : r + 1, width : 2 * width]
        return (scaled * (1.0 + scale) + shift).astype(BF16)

    for one in loads[1:]:
        one.wait()

    cn = modulate(ctx_ref[...], 1)
    kc = jnp.dot(cn, wk[...], preferred_element_type=F32)
    vc = jnp.dot(cn, wv[...], preferred_element_type=F32)
    for h in range(kc.shape[1] // head_dim):
        kh = kc[:, h * head_dim : (h + 1) * head_dim]
        kh = kh * lax.rsqrt(jnp.mean(kh * kh, axis=-1, keepdims=True) + NORM_EPS) * kg_ref[...]
        ckv_ref[h, 0] = kh.astype(BF16)
        ckv_ref[h, 1] = vc[:, h * head_dim : (h + 1) * head_dim].astype(BF16)

    q4 = head_dim // 4
    qgain, kgain = qg_ref[...], kg_ref[...]

    def turn(yt, cos, sin):
        out = []
        for n in range(2):
            a = yt[2 * n * q4 : (2 * n + 1) * q4]
            b = yt[(2 * n + 1) * q4 : (2 * n + 2) * q4]
            out += [a * cos[n] - b * sin[n], b * cos[n] + a * sin[n]]
        return jnp.concatenate(out, axis=0)

    def unit(yh, gain):
        return yh * lax.rsqrt(jnp.mean(yh * yh, axis=-1, keepdims=True) + NORM_EPS) * gain

    span = 2 * rows
    relays = []
    for j in range(y_count):
        yy = (y + j) % y_count
        if j > 0:
            src = yy * 2 + c
            remote(lat.at[src], lat.at[src], lat_send.at[0], lat_recv.at[src], (s, t)).wait_recv()
            one = remote(
                lat.at[src], lat.at[src], lat_send.at[y_count - 1 + j], lat_recv.at[src], (s, partner)
            )
            one.start()
            relays.append(one)
        other = yy * 2 + 1 - c
        remote(lat.at[other], lat.at[other], lat_send.at[0], lat_recv.at[other], (s, t)).wait_recv()
        for i in range(2):
            xn[i * rows : (i + 1) * rows, :] = modulate(lat[yy * 2 + i], 0)
        x = xn[...]
        at = pl.ds(pl.multiple_of(yy * span, span), span)
        cos, sin = cos_ref[:, :, at], sin_ref[:, :, at]
        for w, kind in ((wq, 0), (wk, 1), (wv, 2)):
            step = min(2 * head_dim, w.shape[1])
            for n in range(0, w.shape[1], step):
                full = jnp.dot(x, w[:, n : n + step], preferred_element_type=F32)
                for m in range(0, step, head_dim):
                    h = (n + m) // head_dim
                    yh = full[:, m : m + head_dim]
                    if kind == 0:
                        qt_ref[h, :, at] = turn(unit(yh, qgain).T, cos, sin).astype(BF16)
                    elif kind == 1:
                        k_ref[h, at, :] = turn(unit(yh, kgain).T, cos, sin).T.astype(BF16)
                    else:
                        vt_ref[h, :, at] = yh.T.astype(BF16)
    for one in sends + more + last + relays:
        one.wait_send()


def attend_kernel(
    sp_count, x_count, group, lift,
    k_hbm, vt_hbm, ckv_hbm, qt_ref,
    out_ref,
    kb, vb, cb, top, tot, acc, load_sem, send_sem, recv_sem,
):
    s, t = lax.axis_index("sp"), lax.axis_index("tp")
    z, x = s // x_count, s % x_count
    z_count = sp_count // x_count
    heads, head_dim, rows = qt_ref.shape
    kv_heads = heads // group
    factor = head_dim ** (-0.5) * math.log2(math.e)

    loads = [
        pltpu.make_async_copy(a, b, load_sem.at[i])
        for i, (a, b) in enumerate(
            (
                (ckv_hbm, cb.at[s]),
                (k_hbm, kb.at[s]),
                (vt_hbm, vb.at[s]),
            )
        )
    ]
    for one in loads:
        one.start()
    targets = []
    for sign in (1, -1):
        ok = (z + sign >= 0) & (z + sign < z_count)
        peer = ((z + sign + z_count) % z_count) * x_count + x
        targets.append((ok, peer))

    top[...] = jnp.full_like(top, -1e30)
    tot[...] = jnp.zeros_like(tot)
    acc[...] = jnp.zeros_like(acc)
    for one in loads:
        one.wait()

    bufs = (cb, kb, vb)

    def copies(src, way, peer):
        return [
            remote(b.at[src], b.at[src], send_sem.at[i, src, way], recv_sem.at[i, src], (peer, t))
            for i, b in enumerate(bufs)
        ]

    def source(k):
        low = jnp.minimum(z, z_count - 1 - z)
        both = k <= 2 * low
        dist = jnp.where(both, (k + 1) // 2, k - low)
        up = jnp.where(both, k % 2 == 1, z < z_count - 1 - z)
        return jnp.where(up, z + dist, z - dist)

    def update(i, keys, values_t, bias):
        sc = jnp.dot(keys, qt_ref[i], preferred_element_type=F32) * factor
        if bias != 0.0:
            sc = sc + bias
        old = top[i]
        new = jnp.maximum(old, jnp.max(sc, axis=0, keepdims=True))
        p = jnp.exp2(sc - new)
        f = jnp.exp2(old - new)
        top[i] = new
        tot[i] = tot[i] * f + jnp.sum(p, axis=0, keepdims=True)
        acc[i] = acc[i] * f + jnp.dot(values_t, p.astype(BF16), preferred_element_type=F32)

    def block(src):
        def head(i, carry):
            h = i // group
            update(i, kb[src, h], vb[src, h], 0.0)
            return carry

        lax.fori_loop(0, heads, head, 0)

    def wait_from(src):
        for one in copies(src, 0, s):
            one.wait_recv()

    def step(k, carry):
        zz = source(k)
        src = zz * x_count + x

        @pl.when(k > 0)
        def _():
            wait_from(src)

        for way, (ok, peer) in enumerate(targets):
            mine = zz <= z if way == 0 else zz >= z

            @pl.when(ok & mine)
            def _():
                for one in copies(src, way, peer):
                    one.start()

        for j in range(1, x_count):
            for one in copies(src, 1 + j, z * x_count + (x + j) % x_count):
                one.start()
        block(src)

        @pl.when(k > 0)
        def _():
            before = source(k - 1)
            for j in range(1, x_count):
                old = before * x_count + (x + j) % x_count
                wait_from(old)
                block(old)

        return carry

    lax.fori_loop(0, z_count, step, 0)
    final = source(z_count - 1)
    ends = [final * x_count + (x + j) % x_count for j in range(1, x_count)]
    for src in ends:
        copies(src, 0, s)[0].wait_recv()
    for i in range(heads):
        h = i // group
        keys = jnp.concatenate([cb[j, h, 0] for j in range(sp_count)], axis=0)
        vals = jnp.concatenate([cb[j, h, 1] for j in range(sp_count)], axis=0)
        update(i, keys, vals.astype(F32).T.astype(BF16), lift * math.log2(math.e))
    for src in ends:
        for one in copies(src, 0, s)[1:]:
            one.wait_recv()
        block(src)
    for i in range(heads):
        out_ref[:, i * head_dim : (i + 1) * head_dim] = (acc[i] / tot[i]).T.astype(BF16)

    def drain(k, carry):
        zz = source(k)
        src = zz * x_count + x
        for way, (ok, peer) in enumerate(targets):
            mine = zz <= z if way == 0 else zz >= z

            @pl.when(ok & mine)
            def _():
                for one in copies(src, way, peer):
                    one.wait_send()

        for j in range(1, x_count):
            for one in copies(src, 1 + j, z * x_count + (x + j) % x_count):
                one.wait_send()
        return carry

    lax.fori_loop(0, z_count, drain, 0)


def quad_kernel(sp_count, head_dim, lift, chunks, *refs):
    (
        cond_ref, cond_1_ref, mw_hbm, lat_hbm, ctx_hbm, wq_hbm, wk_hbm, wv_hbm, qg_ref, kg_ref,
        cos_hbm, sin_hbm, wo_hbm,
        out_ref,
        mw, lat, ctx, wq, wk, wv, wo, cos_ref, sin_ref, part, tot, mod, xn,
        qt, kk, vt, ckv, qb, kb, vb, cb, top, ttl, acc, stats, stats_in, acc_in,
        score, prob, fade, ob, att, core_out, core_in, mesh_out, mesh_in, mixed,
        load_sem, lat_send, lat_recv, part_send, part_recv, tot_send, tot_recv,
        kv_send, kv_recv, c_send, c_recv, q_send, q_recv, relay_send,
        a_send, a_recv, s_sem, o_send, o_recv, core_send, core_recv, mesh_send, mesh_recv,
    ) = refs
    s, t = lax.axis_index("sp"), lax.axis_index("tp")
    y, c = t // 2, t % 2
    z, x = s // 2, s % 2
    z_count = sp_count // 2
    quads = z_count // 2
    quad, low = z // 2, z % 2
    place = low * 2 + x
    partner, across = y * 2 + 1 - c, (1 - y) * 2 + c
    target = (z + x) % 2
    owner = low == c
    rows, width = lat.shape[1], lat.shape[2]
    all_rows = 4 * rows
    span = 2 * rows
    first = max(rows * 3 // 128 * 16, 16)

    load_pairs = (
        (lat_hbm, lat.at[t]), (mw_hbm, mw), (wk_hbm, wk), (wv_hbm, wv), (wq_hbm, wq), (ctx_hbm, ctx),
        (cos_hbm, cos_ref), (sin_hbm, sin_ref), (wo_hbm, wo),
    )
    loads = [pltpu.make_async_copy(a, b, load_sem.at[i]) for i, (a, b) in enumerate(load_pairs)]
    for one in loads:
        one.start()

    barrier = pltpu.get_barrier_semaphore()
    for j in range(sp_count):
        for k in range(2):
            if j + k > 0:
                dev = ((s + j) % sp_count, y * 2 + (c + k) % 2)
                pl.semaphore_signal(barrier, inc=1, device_id=dev, device_id_type=MESH)
    for k in range(2):
        dev = (s, (1 - y) * 2 + (c + k) % 2)
        pl.semaphore_signal(barrier, inc=1, device_id=dev, device_id_type=MESH)

    loads[1].wait()
    lines = lax.broadcasted_iota(jnp.int32, (8, cond_ref.shape[1]), 0)
    cond = jnp.where(lines == 0, cond_ref[...], jnp.where(lines == 1, cond_1_ref[...], 0.0))
    cond = cond * jax.nn.sigmoid(cond)
    part[s] = jnp.dot(
        cond, mw[...], precision=lax.Precision.HIGHEST, preferred_element_type=F32
    )[:2]
    loads[0].wait()
    pl.semaphore_wait(barrier, 2 * sp_count + 1)

    sends = [
        remote(part.at[s], part.at[s], part_send.at[j], part_recv.at[s], ((s + j) % sp_count, t))
        for j in range(1, sp_count)
    ]
    sends.append(remote(lat.at[t], lat.at[t], lat_send.at[2], lat_recv.at[2], (s, partner)))
    pieces = (pl.ds(0, first), pl.ds(first, rows - first))
    halves = [
        remote(lat.at[t, at], lat.at[t, at], lat_send.at[i], lat_recv.at[i], (s, across))
        for i, at in enumerate(pieces)
    ]
    for one in sends + halves[:1]:
        one.start()
    for j in range(1, sp_count):
        src = (s + j) % sp_count
        remote(part.at[src], part.at[src], part_send.at[0], part_recv.at[src], (s, partner)).wait_recv()
    total = part[0]
    for j in range(1, sp_count):
        total = total + part[j]
    tot[t] = total
    last = [
        remote(tot.at[t], tot.at[t], tot_send.at[j], tot_recv.at[t], (s, (t + j) % 4))
        for j in range(1, 4)
    ]
    for one in last + halves[1:]:
        one.start()
    sends += last + halves
    for j in range(1, 4):
        src = (t + j) % 4
        remote(tot.at[src], tot.at[src], tot_send.at[0], tot_recv.at[src], (s, partner)).wait_recv()
    cols = tot.shape[2]
    for j in range(4):
        mod[:, j * cols : (j + 1) * cols] = tot[j]

    def relay_rows(i):
        at = pieces[i]
        remote(lat.at[across, at], lat.at[across, at], lat_send.at[0], lat_recv.at[i], (s, partner)).wait_recv()
        one = remote(
            lat.at[across, at], lat.at[across, at], lat_send.at[3 + i], lat_recv.at[3 + i], (s, partner)
        )
        one.start()
        sends.append(one)

    def modulate(value, r):
        value = value.astype(F32)
        scaled = value * lax.rsqrt(jnp.mean(value * value, axis=-1, keepdims=True) + NORM_EPS)
        shift, scale = mod[r : r + 1, :width], mod[r : r + 1, width : 2 * width]
        return (scaled * (1.0 + scale) + shift).astype(BF16)

    q4 = head_dim // 4
    qgain = qg_ref[...] * (head_dim ** (-0.5) * math.log2(math.e))
    kgain = kg_ref[...]

    def turn(yt, cos, sin):
        out = []
        for n in range(2):
            a = yt[2 * n * q4 : (2 * n + 1) * q4]
            b = yt[(2 * n + 1) * q4 : (2 * n + 2) * q4]
            out += [a * cos[n] - b * sin[n], b * cos[n] + a * sin[n]]
        return jnp.concatenate(out, axis=0)

    def unit(yh, gain):
        return yh * lax.rsqrt(jnp.mean(yh * yh, axis=-1, keepdims=True) + NORM_EPS) * gain

    def column(yy):
        return pl.ds(pl.multiple_of(yy * span, span), span)

    def dest(i, n):
        to = (((quad + n) % quads) * 2 + c) * 2 + i
        here = (to == s) & (target == c)
        return to, here

    def send_kv(ph, act):
        at = column((y + ph) % 2)
        for n in range(quads):
            for i in range(2):
                to, here = dest(i, n)
                for kind, src, dst in (
                    (0, kk.at[i, at], kb.at[z, at]), (1, vt.at[i, :, at], vb.at[z, :, at]),
                ):

                    @pl.when(jnp.logical_not(here))
                    def _():
                        act(remote(
                            src, dst, kv_send.at[kind, ph, n, i], kv_recv.at[kind, ph, z],
                            (to, y * 2 + target),
                        ))

    def send_ctx(act):
        for n in range(quads):
            for i in range(2):
                to, here = dest(i, n)

                @pl.when(jnp.logical_not(here))
                def _():
                    act(remote(
                        ckv.at[i], cb.at[z], c_send.at[n, i], c_recv.at[z], (to, y * 2 + target)
                    ))

    def send_q(ph, act):
        at = column((y + ph) % 2)
        for i in range(2):
            to = (quad * 2 + c) * 2 + i
            for g in range(2):
                mine = (to == s) & (g == c)
                src = qt.at[i * 2 + g, :, at]

                @pl.when(mine)
                def _():
                    act(remote(
                        src, qb.at[0, place, :, at], q_send.at[ph, i, g], q_recv.at[0, place, ph],
                        (s, partner),
                    ))

                @pl.when(jnp.logical_not(mine))
                def _():
                    act(remote(
                        src, qb.at[1, place, :, at], q_send.at[ph, i, g], q_recv.at[1, place, ph],
                        (to, y * 2 + g),
                    ))

    def start(one):
        one.start()

    def project(ph):
        yy = (y + ph) % 2
        for i in range(2):
            xn[i * rows : (i + 1) * rows, :] = modulate(lat[yy * 2 + i], 0)
        value = xn[...]
        at = column(yy)
        cos, sin = cos_ref[:, :, at], sin_ref[:, :, at]
        full = jnp.dot(value, wk[...], preferred_element_type=F32)
        for h in range(2):
            yh = full[:, h * head_dim : (h + 1) * head_dim]
            kk[h, at, :] = turn(unit(yh, kgain).T, cos, sin).T.astype(BF16)
        full = jnp.dot(value, wv[...], preferred_element_type=F32)
        for h in range(2):
            vt[h, :, at] = full[:, h * head_dim : (h + 1) * head_dim].T.astype(BF16)
        send_kv(ph, start)
        for h in range(4):
            if h % 2 == 0:
                full = jnp.dot(value, wq[:, h * head_dim : (h + 2) * head_dim], preferred_element_type=F32)
            yh = full[:, (h % 2) * head_dim : (h % 2 + 1) * head_dim]
            qt[h, :, at] = turn(unit(yh, qgain).T, cos, sin).astype(BF16)
        send_q(ph, start)

    def take_q(ph):
        at = column((y + ph) % 2)
        for j in range(1, 4):
            m = (place + j) % 4
            ref = qb.at[1, m, :, at]
            remote(ref, ref, relay_send.at[0, 0], q_recv.at[1, m, ph], (s, partner)).wait_recv()
            one = remote(ref, qb.at[0, m, :, at], relay_send.at[j, ph], q_recv.at[0, m, ph], (s, partner))
            one.start()
            sends.append(one)

    for one in loads[2:]:
        one.wait()
    remote(lat.at[partner], lat.at[partner], lat_send.at[0], lat_recv.at[2], (s, partner)).wait_recv()
    project(0)
    relay_rows(0)
    cn = modulate(ctx[...], 1)
    kc = jnp.dot(cn, wk[...], preferred_element_type=F32)
    vc = jnp.dot(cn, wv[...], preferred_element_type=F32)
    for h in range(2):
        ckv[h, 0] = unit(kc[:, h * head_dim : (h + 1) * head_dim], kgain).astype(BF16)
        ckv[h, 1] = vc[:, h * head_dim : (h + 1) * head_dim].astype(BF16)
    send_ctx(start)
    relay_rows(1)
    take_q(0)
    other = (1 - y) * 2 + 1 - c
    for i, at in enumerate(pieces):
        ref = lat.at[other, at]
        remote(ref, ref, lat_send.at[0], lat_recv.at[3 + i], (s, partner)).wait_recv()
    project(1)

    local = owner & (target == c)

    @pl.when(local)
    def _():
        kb[z] = kk[x]
        vb[z] = vt[x]
        cb[z] = ckv[x]

    @pl.when(owner)
    def _():
        qb[1, place] = qt[x * 2 + c]
        qb[0, place] = qt[x * 2 + 1 - c]

    take_q(1)
    for ph in range(2):
        at = column((y + ph) % 2)
        for j in range(4):
            m = (place + j) % 4
            for role in range(2) if j == 0 else range(1):
                ref = qb.at[role, m, :, at]
                one = remote(ref, ref, relay_send.at[0, 0], q_recv.at[role, m, ph], (s, partner))
                if j == 0:
                    pl.when(jnp.logical_not(owner))(one.wait_recv)
                else:
                    one.wait_recv()

    def sweep(role, keys, values, bias, begin):
        count = keys().shape[0]

        def stage_a(m):
            score[m % 2, :count] = jnp.dot(keys(), qb[role, m], preferred_element_type=F32)

        def stage_b(m):
            sc = score[m % 2, :count]
            new = jnp.max(sc, axis=0, keepdims=True) + bias
            if not begin:
                old = top[role, m]
                new = jnp.maximum(old, new)
                f = jnp.exp2(old - new)
                fade[m % 2] = f
            p = jnp.exp2(sc - (new - bias))
            line = jnp.sum(p, axis=0, keepdims=True)
            ttl[role, m] = line if begin else ttl[role, m] * f + line
            top[role, m] = new
            prob[m % 2, :count] = p.astype(BF16)

        def stage_c(m):
            value = jnp.dot(values(), prob[m % 2, :count], preferred_element_type=F32)
            acc[role, m] = value if begin else acc[role, m] * fade[m % 2] + value

        for n in range(6):
            if n < 4:
                stage_a(n)
            if 1 <= n <= 4:
                stage_b(n - 1)
            if n >= 2:
                stage_c(n - 2)

    for k in range(z_count):

        @pl.when(jnp.logical_not(local & (k == z)))
        def _():
            remote(cb.at[k], cb.at[k], c_send.at[0, 0], c_recv.at[k], (s, partner)).wait_recv()

    ctx_keys = jnp.concatenate([cb[k, 0] for k in range(z_count)], axis=0)
    ctx_values = jnp.concatenate([cb[k, 1] for k in range(z_count)], axis=0)
    ctx_values = ctx_values.astype(F32).T.astype(BF16)
    for role in range(2):
        sweep(role, lambda: ctx_keys, lambda: ctx_values, lift * math.log2(math.e), True)

    give = [
        remote(acc.at[0, m], acc_in.at[m], a_send.at[m], a_recv.at[m], (s, partner)) for m in range(4)
    ]
    give_stats = remote(stats, stats_in, s_sem.at[0], s_sem.at[1], (s, partner))

    def step(n, carry):
        k, role = n // 2, n % 2
        zz = ((quad + k // 2) % quads) * 2 + (low + k % 2) % 2

        @pl.when((role == 0) & jnp.logical_not(local & (zz == z)))
        def _():
            for ph in range(2):
                at = column((y + ph) % 2)
                for kind, ref in ((0, kb.at[zz, at]), (1, vb.at[zz, :, at])):
                    remote(ref, ref, kv_send.at[0, 0, 0, 0], kv_recv.at[kind, ph, zz], (s, partner)).wait_recv()

        sweep(role, lambda: kb[zz], lambda: vb[zz], 0.0, False)

        @pl.when(n == 2 * z_count - 2)
        def _():
            for m in range(4):
                stats[m, 0:1] = top[0, m]
                stats[m, 1:2] = ttl[0, m]
            for one in give + [give_stats]:
                one.start()

        return carry

    lax.fori_loop(0, 2 * z_count, step, 0)
    give_stats.wait_recv()
    for one in give:
        one.wait_recv()

    def return_o(m, half, act):
        to = (quad * 2 + m // 2) * 2 + m % 2
        yy = (1 - y + half) % 2
        at = column(yy)
        head = pl.ds(pl.multiple_of((x * 2 + c) * head_dim, head_dim), head_dim)
        here = (to == s) & owner

        @pl.when(jnp.logical_not(here))
        def _():
            act(remote(
                ob.at[m, at], att.at[at, head], o_send.at[m, half],
                o_recv.at[x * 2 + c, half], (to, y * 2 + low),
            ))

        if act is start:

            @pl.when(here)
            def _():
                att[at, head] = ob[m, at]

    for half in range(2):
        at = column((1 - y + half) % 2)
        for j in range(4):
            m = j
            a, b = top[1, m, :, at], stats_in[m, 0:1, at]
            peak = jnp.maximum(a, b)
            wa, wb = jnp.exp2(a - peak), jnp.exp2(b - peak)
            den = 1.0 / (ttl[1, m, :, at] * wa + stats_in[m, 1:2, at] * wb)
            done = acc[1, m, :, at] * (wa * den) + acc_in[m, :, at] * (wb * den)
            ob[m, at, :] = done.T.astype(BF16)
            return_o(m, half, start)

    step_cols = width // chunks

    def piece(n, yy, cc):
        at = pl.ds(pl.multiple_of((yy * 2 + cc) * rows, rows), rows)
        return jnp.dot(
            att[at, :], wo[:, n * step_cols : (n + 1) * step_cols], preferred_element_type=F32
        )

    units = [(half, n) for half in range(2) for n in range(chunks)]
    cores = [
        remote(core_out.at[h, n], core_in.at[h, n], core_send.at[h, n], core_recv.at[h, n], (s, partner))
        for h, n in units
    ]
    mesh = [
        remote(mesh_out.at[n], mesh_in.at[n], mesh_send.at[n], mesh_recv.at[n], (s, across))
        for n in range(chunks)
    ]
    for u in range(len(units) + 1):
        if u < len(units):
            half, n = units[u]
            yy = (1 - y + half) % 2
            if n == 0:
                for i in range(2):
                    for g in range(2):
                        ref = att.at[column(yy), pl.ds((i * 2 + g) * head_dim, head_dim)]
                        one = remote(ref, ref, o_send.at[0, 0], o_recv.at[i * 2 + g, half], (s, partner))
                        pl.when(jnp.logical_not(owner & (x == i) & (g == c)))(one.wait_recv)
            core_out[half, n] = piece(n, yy, 1 - c).astype(BF16)
            cores[u].start()
        if u > 0:
            half, n = units[u - 1]
            value = piece(n, (1 - y + half) % 2, c)
            cores[u - 1].wait_recv()
            value = value + core_in[half, n].astype(F32)
            if half == 0:
                mesh_out[n] = value.astype(BF16)
                mesh[n].start()
            else:
                mixed[n] = value
    square = jnp.zeros((rows, 1), F32)
    for n in range(chunks):
        mesh[n].wait_recv()
        value = mixed[n] + mesh_in[n].astype(F32)
        mixed[n] = value
        square = square + jnp.sum(value * value, axis=-1, keepdims=True)
    inv = lax.rsqrt(square / width + NORM_EPS)
    for n in range(chunks):
        at = slice(n * step_cols, (n + 1) * step_cols)
        gate = mod[0:1, 2 * width + n * step_cols : 2 * width + (n + 1) * step_cols]
        out_ref[:, at] = (lat[t, :, at].astype(F32) + gate * (mixed[n] * inv)).astype(BF16)

    def sent(one):
        one.wait_send()

    for one in sends + give + [give_stats] + cores + mesh:
        one.wait_send()
    for ph in range(2):
        send_kv(ph, sent)
        send_q(ph, sent)
    send_ctx(sent)
    for half in range(2):
        for m in range(4):
            return_o(m, half, sent)


def mix_kernel(
    tp_count, chunks,
    att_ref, wo_hbm, wo_ref, wo_sem, lat_ref, gate_ref,
    out_ref,
    core_out, core_in, mesh_out, mesh_in, mixed, core_send, core_recv, mesh_send, mesh_recv,
):
    s, t = lax.axis_index("sp"), lax.axis_index("tp")
    y, c = t // 2, t % 2
    y_count = tp_count // 2
    partner = y * 2 + 1 - c
    rows, width = lat_ref.shape
    step = width // chunks
    peers = [((y + j) % y_count) * 2 + c for j in range(1, y_count)]
    pltpu.make_async_copy(wo_hbm, wo_ref, wo_sem.at[0]).wait()

    def piece(n, j, cc):
        yy = (y + j) % y_count
        at = pl.ds(pl.multiple_of((yy * 2 + cc) * rows, rows), rows)
        return jnp.dot(
            att_ref[at, :], wo_ref[:, n * step : (n + 1) * step], preferred_element_type=F32
        )

    order = list(range(1, y_count)) + [0]
    cores = [
        remote(core_out.at[n], core_in.at[n], core_send.at[n], core_recv.at[n], (s, partner))
        for n in range(chunks)
    ]
    sent = []
    for n in range(chunks + 1):
        if n < chunks:
            for j in order:
                core_out[n, j] = piece(n, j, 1 - c).astype(BF16)
            cores[n].start()
        if n == 0:
            continue
        m = n - 1
        own = [piece(m, j, c) for j in order]
        cores[m].wait_recv()
        for j, value in zip(order, own):
            value = value + core_in[m, j].astype(F32)
            if j == 0:
                mixed[m] = value
            else:
                mesh_out[m, j - 1] = value.astype(BF16)
                one = remote(
                    mesh_out.at[m, j - 1], mesh_in.at[m, j - 1], mesh_send.at[m, j - 1],
                    mesh_recv.at[m, j - 1], (s, peers[j - 1]),
                )
                one.start()
                sent.append(one)
    for one in sent:
        one.wait_recv()
    square = jnp.zeros((rows, 1), F32)
    for n in range(chunks):
        value = mixed[n]
        for j in range(1, y_count):
            value = value + mesh_in[n, j - 1].astype(F32)
        mixed[n] = value
        square = square + jnp.sum(value * value, axis=-1, keepdims=True)
    inv = lax.rsqrt(square / width + NORM_EPS)
    for n in range(chunks):
        at = slice(n * step, (n + 1) * step)
        out_ref[:, at] = (
            lat_ref[:, at].astype(F32) + gate_ref[:, at] * (mixed[n] * inv)
        ).astype(BF16)
    for one in sent + cores:
        one.wait_send()


def whole_kernel(sp_count, tp_count, x_count, head_dim, group, lift, chunks, counts, *refs):
    (
        cond, cond_1, mw, lat, ctx, wq, wk, wv, qg, kg, cos, sin, wo, lat_rows,
        out, qt, k, vt, ckv, gate, att, wo_vm, wo_sem, *rest,
    ) = refs
    front, middle, last = counts
    front_scratch, middle_scratch = rest[:front], rest[front : front + middle]
    front_kernel(
        sp_count, tp_count, head_dim, cond, cond_1, mw, lat, ctx, wq, wk, wv, qg, kg, cos, sin,
        qt, k, vt, ckv, gate, *front_scratch, wo, wo_vm, wo_sem,
    )
    attend_kernel(sp_count, x_count, group, lift, k, vt, ckv, qt, att, *middle_scratch)
    mix_kernel(
        tp_count, chunks, att, wo, wo_vm, wo_sem, lat_rows, gate, out, *rest[front + middle :]
    )


ANY = pl.BlockSpec(memory_space=pl.ANY)
VM = pl.BlockSpec(memory_space=pltpu.VMEM)
DMA = pltpu.SemaphoreType.DMA


def grid_tables(all_rows, head_dim):
    quarter = head_dim // 4
    lines = all_rows // GRID_W
    row = lax.axis_index("sp") * lines + jnp.arange(lines, dtype=jnp.int32)
    where = jnp.concatenate([row, jnp.arange(GRID_W, dtype=jnp.int32)]).astype(F32)
    inv_freq = ROPE_BASE ** (-jnp.arange(quarter, dtype=F32) / quarter)
    angles = inv_freq[:, None] * where[None, :]
    small = lax.optimization_barrier((jnp.cos(angles), jnp.sin(angles)))
    return [
        jnp.stack([jnp.repeat(one[:, :lines], GRID_W, axis=1), jnp.tile(one[:, lines:], (1, lines))])
        for one in small
    ]


def quad_call(args, out_weight, sp_count, head_dim, lift):
    mod_weight, latents, context, query_weight, key_matrix, value_matrix = args[2:8]
    rows, width = latents.shape
    ctx_rows = context.shape[0]
    mod_cols = mod_weight.shape[1]
    all_rows, z_count, quads, chunks = 4 * rows, sp_count // 2, sp_count // 4, 4
    step = width // chunks
    cos, sin = grid_tables(all_rows, head_dim)
    block = max(all_rows, z_count * ctx_rows)
    scratch = [
        pltpu.VMEM(mod_weight.shape, F32),
        pltpu.VMEM((4, rows, width), BF16),
        pltpu.VMEM(context.shape, BF16),
        pltpu.VMEM(query_weight.shape, BF16),
        pltpu.VMEM(key_matrix.shape, BF16),
        pltpu.VMEM(value_matrix.shape, BF16),
        pltpu.VMEM(out_weight.shape, BF16),
        pltpu.VMEM(cos.shape, F32),
        pltpu.VMEM(sin.shape, F32),
        pltpu.VMEM((sp_count, 2, mod_cols), F32),
        pltpu.VMEM((4, 2, mod_cols), F32),
        pltpu.VMEM((2, 4 * mod_cols), F32),
        pltpu.VMEM((2 * rows, width), BF16),
        pltpu.VMEM((4, head_dim, all_rows), BF16),
        pltpu.VMEM((2, all_rows, head_dim), BF16),
        pltpu.VMEM((2, head_dim, all_rows), BF16),
        pltpu.VMEM((2, 2, ctx_rows, head_dim), BF16),
        pltpu.VMEM((2, 4, head_dim, all_rows), BF16),
        pltpu.VMEM((z_count, all_rows, head_dim), BF16),
        pltpu.VMEM((z_count, head_dim, all_rows), BF16),
        pltpu.VMEM((z_count, 2, ctx_rows, head_dim), BF16),
        pltpu.VMEM((2, 4, 1, all_rows), F32),
        pltpu.VMEM((2, 4, 1, all_rows), F32),
        pltpu.VMEM((2, 4, head_dim, all_rows), F32),
        pltpu.VMEM((4, 2, all_rows), F32),
        pltpu.VMEM((4, 2, all_rows), F32),
        pltpu.VMEM((4, head_dim, all_rows), F32),
        pltpu.VMEM((2, block, all_rows), F32),
        pltpu.VMEM((2, block, all_rows), BF16),
        pltpu.VMEM((2, 1, all_rows), F32),
        pltpu.VMEM((4, all_rows, head_dim), BF16),
        pltpu.VMEM((all_rows, 4 * head_dim), BF16),
        pltpu.VMEM((2, chunks, rows, step), BF16),
        pltpu.VMEM((2, chunks, rows, step), BF16),
        pltpu.VMEM((chunks, rows, step), BF16),
        pltpu.VMEM((chunks, rows, step), BF16),
        pltpu.VMEM((chunks, rows, step), F32),
        DMA((9,)),
        DMA((5,)),
        DMA((5,)),
        DMA((sp_count,)),
        DMA((sp_count,)),
        DMA((4,)),
        DMA((4,)),
        DMA((2, 2, quads, 2)),
        DMA((2, 2, z_count)),
        DMA((quads, 2)),
        DMA((z_count,)),
        DMA((2, 2, 2)),
        DMA((2, 4, 2)),
        DMA((4, 2)),
        DMA((4,)),
        DMA((4,)),
        DMA((2,)),
        DMA((4, 2)),
        DMA((4, 2)),
        DMA((2, chunks)),
        DMA((2, chunks)),
        DMA((chunks,)),
        DMA((chunks,)),
    ]
    return pl.pallas_call(
        functools.partial(quad_kernel, sp_count, head_dim, lift, chunks),
        out_shape=jax.ShapeDtypeStruct((rows, width), BF16),
        in_specs=[VM, VM, ANY, ANY, ANY, ANY, ANY, ANY, VM, VM, ANY, ANY, ANY],
        out_specs=VM,
        scratch_shapes=scratch,
        compiler_params=pltpu.CompilerParams(
            collective_id=0, has_side_effects=True, vmem_limit_bytes=VMEM_BYTES
        ),
        name="quad",
    )(*args, cos, sin, out_weight)


def body(
    latents,
    context,
    cond,
    ctx_cond,
    mod_weight,
    query_weight,
    key_matrix,
    value_matrix,
    out_weight,
    query_gain,
    key_gain,
):
    sp_count, tp_count = lax.axis_size("sp"), lax.axis_size("tp")
    x_count = row_size(sp_count)
    rows, width = latents.shape
    ctx_rows = context.shape[0]
    head_dim = query_gain.shape[0]
    heads = query_weight.shape[1] // head_dim
    kv_heads = key_matrix.shape[1] // head_dim
    all_rows = rows * tp_count
    mod_cols = mod_weight.shape[1]
    lift = math.log(sp_count * all_rows / (2.0 * sp_count * ctx_rows))
    group = heads // kv_heads
    args = (
        cond[None], ctx_cond[None], mod_weight, latents, context, query_weight, key_matrix, value_matrix,
        query_gain[None], key_gain[None],
    )
    wide = all_rows % GRID_W == 0 and all_rows == rows * 4 and rows % 128 == 0
    if wide and kv_heads == 2 and group == 2 and x_count == 2 and sp_count % 4 == 0:
        return quad_call(args, out_weight, sp_count, head_dim, lift)
    chunks = 4
    y_count = tp_count // 2
    step = width // chunks
    far = max(y_count - 1, 1)
    positions = lax.axis_index("sp") * all_rows + jnp.arange(all_rows, dtype=jnp.int32)
    cos, sin = tables(positions, head_dim)
    shared = [
        pltpu.VMEM((heads, head_dim, all_rows), BF16),
        pltpu.VMEM((kv_heads, all_rows, head_dim), BF16),
        pltpu.VMEM((kv_heads, head_dim, all_rows), BF16),
        pltpu.VMEM((kv_heads, 2, ctx_rows, head_dim), BF16),
        pltpu.VMEM((1, width), F32),
        pltpu.VMEM((all_rows, heads * head_dim), BF16),
        pltpu.VMEM(out_weight.shape, BF16),
        DMA((1,)),
    ]
    front = [
        pltpu.VMEM(mod_weight.shape, F32),
        pltpu.VMEM((tp_count, rows, width), BF16),
        pltpu.VMEM(query_weight.shape, BF16),
        pltpu.VMEM(key_matrix.shape, BF16),
        pltpu.VMEM(value_matrix.shape, BF16),
        pltpu.VMEM((sp_count, 2, mod_cols), F32),
        pltpu.VMEM((tp_count, 2, mod_cols), F32),
        pltpu.VMEM((2, mod_cols * tp_count), F32),
        pltpu.VMEM((2 * rows, width), BF16),
        DMA((5,)),
        DMA((tp_count,)),
        DMA((tp_count,)),
        DMA((sp_count,)),
        DMA((sp_count,)),
        DMA((tp_count,)),
        DMA((tp_count,)),
    ]
    middle = [
        pltpu.VMEM((sp_count, kv_heads, all_rows, head_dim), BF16),
        pltpu.VMEM((sp_count, kv_heads, head_dim, all_rows), BF16),
        pltpu.VMEM((sp_count, kv_heads, 2, ctx_rows, head_dim), BF16),
        pltpu.VMEM((heads, 1, all_rows), F32),
        pltpu.VMEM((heads, 1, all_rows), F32),
        pltpu.VMEM((heads, head_dim, all_rows), F32),
        DMA((3,)),
    ]
    middle += [DMA((3, sp_count, x_count + 1)), DMA((3, sp_count))]
    last = [
        pltpu.VMEM((chunks, y_count, rows, step), BF16),
        pltpu.VMEM((chunks, y_count, rows, step), BF16),
        pltpu.VMEM((chunks, far, rows, step), BF16),
        pltpu.VMEM((chunks, far, rows, step), BF16),
        pltpu.VMEM((chunks, rows, step), F32),
        DMA((chunks,)),
        DMA((chunks,)),
        DMA((chunks, far)),
        DMA((chunks, far)),
    ]
    counts = (len(front), len(middle), len(last))
    return pl.pallas_call(
        functools.partial(
            whole_kernel, sp_count, tp_count, x_count, head_dim, group, lift, chunks, counts
        ),
        out_shape=jax.ShapeDtypeStruct((rows, width), BF16),
        in_specs=[VM, VM, ANY, ANY, VM, ANY, ANY, ANY, VM, VM, VM, VM, ANY, VM],
        out_specs=VM,
        scratch_shapes=shared + front + middle + last,
        compiler_params=pltpu.CompilerParams(
            collective_id=0, has_side_effects=True, vmem_limit_bytes=VMEM_BYTES
        ),
        name="whole",
    )(
        *args, cos, sin, out_weight, latents,
    )


def solution(mesh):
    placed = (
        P(("sp", "tp"), None),
        P("sp", None),
        P("sp"),
        P("sp"),
        P("sp", "tp"),
        P(None, "tp"),
        P(None, "tp"),
        P(None, "tp"),
        P("tp", None),
        P(),
        P(),
    )
    return jax.shard_map(
        body, mesh=mesh, in_specs=placed, out_specs=P(("sp", "tp"), None), check_vma=False
    )
```

```python
import functools
import math

import jax
import jax.numpy as jnp
import numpy as np
from jax import lax
from jax.experimental import pallas as pl
from jax.experimental.pallas import tpu as pltpu
from jax.sharding import PartitionSpec as P

GRID_W = 64
NORM_EPS = 1e-06
ROPE_BASE = 10000.0
MESH = pl.DeviceIdType.MESH
BF16 = jnp.bfloat16
F32 = jnp.float32
VMEM_BYTES = 67043328


def row_size(sp_count):
    size = 1
    while 4 * size * size <= sp_count:
        size *= 2
    return size


def tables(positions, head_dim):
    quarter = head_dim // 4
    inv_freq = ROPE_BASE ** (-jnp.arange(quarter, dtype=F32) / quarter)
    where = jnp.stack([positions // GRID_W, positions % GRID_W]).astype(F32)
    angles = where[:, None, :] * inv_freq[None, :, None]
    return jnp.cos(angles), jnp.sin(angles)


def remote(src, dst, send, recv, dev):
    return pltpu.make_async_remote_copy(
        src_ref=src, dst_ref=dst, send_sem=send, recv_sem=recv, device_id=dev, device_id_type=MESH
    )


def front_kernel(
    sp_count, tp_count, head_dim,
    cond_ref, cond_1_ref, mw_hbm, lat_hbm, ctx_ref, wq_hbm, wk_hbm, wv_hbm, qg_ref, kg_ref, cos_ref, sin_ref,
    qt_ref, k_ref, vt_ref, ckv_ref, gate_ref,
    mw, lat, wq, wk, wv, part, tot, mod, xn, load_sem,
    lat_send, lat_recv, part_send, part_recv, tot_send, tot_recv,
    wo_hbm, wo_vm, wo_sem,
):
    s, t = lax.axis_index("sp"), lax.axis_index("tp")
    y, c = t // 2, t % 2
    y_count = tp_count // 2
    partner = y * 2 + 1 - c
    rows = lat.shape[1]
    width = lat.shape[2]
    model_cols = mod.shape[1]

    own = pltpu.make_async_copy(lat_hbm, lat.at[t], load_sem.at[0])
    own.start()
    loads = [
        pltpu.make_async_copy(a, b, load_sem.at[1 + i])
        for i, (a, b) in enumerate(((mw_hbm, mw), (wq_hbm, wq), (wk_hbm, wk), (wv_hbm, wv)))
    ]
    for one in loads:
        one.start()

    pltpu.make_async_copy(wo_hbm, wo_vm, wo_sem.at[0]).start()

    barrier = pltpu.get_barrier_semaphore()
    for j in range(1, sp_count):
        pl.semaphore_signal(barrier, inc=1, device_id=((s + j) % sp_count, t), device_id_type=MESH)
    for j in range(1, tp_count):
        pl.semaphore_signal(barrier, inc=1, device_id=(s, (t + j) % tp_count), device_id_type=MESH)
    pl.semaphore_wait(barrier, sp_count + tp_count - 2)

    own.wait()
    sends = []
    for j in range(1, y_count):
        peer = ((y + j) % y_count) * 2 + c
        sends.append(remote(lat.at[t], lat.at[t], lat_send.at[j], lat_recv.at[t], (s, peer)))
    sends.append(remote(lat.at[t], lat.at[t], lat_send.at[0], lat_recv.at[t], (s, partner)))
    for one in sends:
        one.start()

    loads[0].wait()
    lines = lax.broadcasted_iota(jnp.int32, (8, cond_ref.shape[1]), 0)
    cond = jnp.where(lines == 0, cond_ref[...], jnp.where(lines == 1, cond_1_ref[...], 0.0))
    cond = cond * jax.nn.sigmoid(cond)
    part[s] = jnp.dot(
        cond, mw[...], precision=lax.Precision.HIGHEST, preferred_element_type=F32
    )[:2]
    more = [
        remote(part.at[s], part.at[s], part_send.at[j], part_recv.at[s], ((s + j) % sp_count, t))
        for j in range(1, sp_count)
    ]
    for one in more:
        one.start()
    for j in range(1, sp_count):
        src = (s + j) % sp_count
        remote(part.at[src], part.at[src], part_send.at[0], part_recv.at[src], (s, t)).wait_recv()
    total = part[0]
    for j in range(1, sp_count):
        total = total + part[j]
    tot[t] = total
    last = [
        remote(tot.at[t], tot.at[t], tot_send.at[j], tot_recv.at[t], (s, (t + j) % tp_count))
        for j in range(1, tp_count)
    ]
    for one in last:
        one.start()
    for j in range(1, tp_count):
        src = (t + j) % tp_count
        remote(tot.at[src], tot.at[src], tot_send.at[0], tot_recv.at[src], (s, t)).wait_recv()
    cols = model_cols // tp_count
    for j in range(tp_count):
        mod[:, j * cols : (j + 1) * cols] = tot[j]
    gate_ref[...] = mod[0:1, 2 * width :]

    def modulate(x, r):
        x = x.astype(F32)
        scaled = x * lax.rsqrt(jnp.mean(x * x, axis=-1, keepdims=True) + NORM_EPS)
        shift, scale = mod[r : r + 1, :width], mod[r : r + 1, width : 2 * width]
        return (scaled * (1.0 + scale) + shift).astype(BF16)

    for one in loads[1:]:
        one.wait()

    cn = modulate(ctx_ref[...], 1)
    kc = jnp.dot(cn, wk[...], preferred_element_type=F32)
    vc = jnp.dot(cn, wv[...], preferred_element_type=F32)
    for h in range(kc.shape[1] // head_dim):
        kh = kc[:, h * head_dim : (h + 1) * head_dim]
        kh = kh * lax.rsqrt(jnp.mean(kh * kh, axis=-1, keepdims=True) + NORM_EPS) * kg_ref[...]
        ckv_ref[h, 0] = kh.astype(BF16)
        ckv_ref[h, 1] = vc[:, h * head_dim : (h + 1) * head_dim].astype(BF16)

    q4 = head_dim // 4
    qgain, kgain = qg_ref[...], kg_ref[...]

    def turn(yt, cos, sin):
        out = []
        for n in range(2):
            a = yt[2 * n * q4 : (2 * n + 1) * q4]
            b = yt[(2 * n + 1) * q4 : (2 * n + 2) * q4]
            out += [a * cos[n] - b * sin[n], b * cos[n] + a * sin[n]]
        return jnp.concatenate(out, axis=0)

    def unit(yh, gain):
        return yh * lax.rsqrt(jnp.mean(yh * yh, axis=-1, keepdims=True) + NORM_EPS) * gain

    span = 2 * rows
    relays = []
    for j in range(y_count):
        yy = (y + j) % y_count
        if j > 0:
            src = yy * 2 + c
            remote(lat.at[src], lat.at[src], lat_send.at[0], lat_recv.at[src], (s, t)).wait_recv()
            one = remote(
                lat.at[src], lat.at[src], lat_send.at[y_count - 1 + j], lat_recv.at[src], (s, partner)
            )
            one.start()
            relays.append(one)
        other = yy * 2 + 1 - c
        remote(lat.at[other], lat.at[other], lat_send.at[0], lat_recv.at[other], (s, t)).wait_recv()
        for i in range(2):
            xn[i * rows : (i + 1) * rows, :] = modulate(lat[yy * 2 + i], 0)
        x = xn[...]
        at = pl.ds(pl.multiple_of(yy * span, span), span)
        cos, sin = cos_ref[:, :, at], sin_ref[:, :, at]
        for w, kind in ((wq, 0), (wk, 1), (wv, 2)):
            step = min(2 * head_dim, w.shape[1])
            for n in range(0, w.shape[1], step):
                full = jnp.dot(x, w[:, n : n + step], preferred_element_type=F32)
                for m in range(0, step, head_dim):
                    h = (n + m) // head_dim
                    yh = full[:, m : m + head_dim]
                    if kind == 0:
                        qt_ref[h, :, at] = turn(unit(yh, qgain).T, cos, sin).astype(BF16)
                    elif kind == 1:
                        k_ref[h, at, :] = turn(unit(yh, kgain).T, cos, sin).T.astype(BF16)
                    else:
                        vt_ref[h, :, at] = yh.T.astype(BF16)
    for one in sends + more + last + relays:
        one.wait_send()


def attend_kernel(
    sp_count, x_count, group, lift,
    k_hbm, vt_hbm, ckv_hbm, qt_ref,
    out_ref,
    kb, vb, cb, top, tot, acc, load_sem, send_sem, recv_sem,
):
    s, t = lax.axis_index("sp"), lax.axis_index("tp")
    z, x = s // x_count, s % x_count
    z_count = sp_count // x_count
    heads, head_dim, rows = qt_ref.shape
    kv_heads = heads // group
    factor = head_dim ** (-0.5) * math.log2(math.e)

    loads = [
        pltpu.make_async_copy(a, b, load_sem.at[i])
        for i, (a, b) in enumerate(
            (
                (ckv_hbm, cb.at[s]),
                (k_hbm, kb.at[s]),
                (vt_hbm, vb.at[s]),
            )
        )
    ]
    for one in loads:
        one.start()
    targets = []
    for sign in (1, -1):
        ok = (z + sign >= 0) & (z + sign < z_count)
        peer = ((z + sign + z_count) % z_count) * x_count + x
        targets.append((ok, peer))

    top[...] = jnp.full_like(top, -1e30)
    tot[...] = jnp.zeros_like(tot)
    acc[...] = jnp.zeros_like(acc)
    for one in loads:
        one.wait()

    bufs = (cb, kb, vb)

    def copies(src, way, peer):
        return [
            remote(b.at[src], b.at[src], send_sem.at[i, src, way], recv_sem.at[i, src], (peer, t))
            for i, b in enumerate(bufs)
        ]

    def source(k):
        low = jnp.minimum(z, z_count - 1 - z)
        both = k <= 2 * low
        dist = jnp.where(both, (k + 1) // 2, k - low)
        up = jnp.where(both, k % 2 == 1, z < z_count - 1 - z)
        return jnp.where(up, z + dist, z - dist)

    def update(i, keys, values_t, bias):
        sc = jnp.dot(keys, qt_ref[i], preferred_element_type=F32) * factor
        if bias != 0.0:
            sc = sc + bias
        old = top[i]
        new = jnp.maximum(old, jnp.max(sc, axis=0, keepdims=True))
        p = jnp.exp2(sc - new)
        f = jnp.exp2(old - new)
        top[i] = new
        tot[i] = tot[i] * f + jnp.sum(p, axis=0, keepdims=True)
        acc[i] = acc[i] * f + jnp.dot(values_t, p.astype(BF16), preferred_element_type=F32)

    def block(src):
        def head(i, carry):
            h = i // group
            update(i, kb[src, h], vb[src, h], 0.0)
            return carry

        lax.fori_loop(0, heads, head, 0)

    def wait_from(src):
        for one in copies(src, 0, s):
            one.wait_recv()

    def step(k, carry):
        zz = source(k)
        src = zz * x_count + x

        @pl.when(k > 0)
        def _():
            wait_from(src)

        for way, (ok, peer) in enumerate(targets):
            mine = zz <= z if way == 0 else zz >= z

            @pl.when(ok & mine)
            def _():
                for one in copies(src, way, peer):
                    one.start()

        for j in range(1, x_count):
            for one in copies(src, 1 + j, z * x_count + (x + j) % x_count):
                one.start()
        block(src)

        @pl.when(k > 0)
        def _():
            before = source(k - 1)
            for j in range(1, x_count):
                old = before * x_count + (x + j) % x_count
                wait_from(old)
                block(old)

        return carry

    lax.fori_loop(0, z_count, step, 0)
    final = source(z_count - 1)
    ends = [final * x_count + (x + j) % x_count for j in range(1, x_count)]
    for src in ends:
        copies(src, 0, s)[0].wait_recv()
    for i in range(heads):
        h = i // group
        keys = jnp.concatenate([cb[j, h, 0] for j in range(sp_count)], axis=0)
        vals = jnp.concatenate([cb[j, h, 1] for j in range(sp_count)], axis=0)
        update(i, keys, vals.astype(F32).T.astype(BF16), lift * math.log2(math.e))
    for src in ends:
        for one in copies(src, 0, s)[1:]:
            one.wait_recv()
        block(src)
    for i in range(heads):
        out_ref[:, i * head_dim : (i + 1) * head_dim] = (acc[i] / tot[i]).T.astype(BF16)

    def drain(k, carry):
        zz = source(k)
        src = zz * x_count + x
        for way, (ok, peer) in enumerate(targets):
            mine = zz <= z if way == 0 else zz >= z

            @pl.when(ok & mine)
            def _():
                for one in copies(src, way, peer):
                    one.wait_send()

        for j in range(1, x_count):
            for one in copies(src, 1 + j, z * x_count + (x + j) % x_count):
                one.wait_send()
        return carry

    lax.fori_loop(0, z_count, drain, 0)


def quad_kernel(sp_count, head_dim, lift, chunks, *refs):
    (
        cond_hbm, cond_1_hbm, mw_hbm, lat_hbm, ctx_hbm, wq_hbm, wk_hbm, wv_hbm, qg_hbm, kg_hbm,
        cos_hbm, sin_hbm, wo_hbm,
        out_ref,
        cond_ref, cond_1_ref, qg_ref, kg_ref, cos_in, sin_in, small_sem,
        mw, lat, ctx, wq, wk, wv, wo, cos_ref, sin_ref, part, tot, mod, xn,
        qt, kk, vt, ckv, qb, kb, vb, cb, stat, acc, stat_in, acc_in,
        score, prob, fade, ob, att, core_out, core_in, mesh_out, mesh_in, mixed,
        load_sem, lat_send, lat_recv, part_send, part_recv, tot_send, tot_recv,
        kv_send, kv_recv, c_send, c_recv, q_send, q_recv, relay_send, pass_send,
        a_send, a_recv, s_send, s_recv, o_send, o_recv, core_send, core_recv, mesh_send, mesh_recv,
    ) = refs
    s, t = lax.axis_index("sp"), lax.axis_index("tp")
    y, c = t // 2, t % 2
    z, x = s // 2, s % 2
    z_count = sp_count // 2
    quads = z_count // 2
    quad, low = z // 2, z % 2
    place = low * 2 + x
    partner, across = y * 2 + 1 - c, (1 - y) * 2 + c
    target = (z + x) % 2
    owner = low == c
    rows, width = lat.shape[1], lat.shape[2]
    all_rows = 4 * rows
    span = 2 * rows
    first = rows // 64 * 16

    load_pairs = (
        (mw_hbm, mw), (lat_hbm, lat.at[t]), (wk_hbm, wk), (wv_hbm, wv), (wq_hbm, wq), (ctx_hbm, ctx),
        (wo_hbm, wo),
    )
    loads = [pltpu.make_async_copy(a, b, load_sem.at[i]) for i, (a, b) in enumerate(load_pairs)]
    small_pairs = (
        (cond_hbm, cond_ref), (cond_1_hbm, cond_1_ref), (cos_hbm.at[s], cos_in), (sin_hbm.at[s], sin_in),
        (qg_hbm, qg_ref), (kg_hbm, kg_ref),
    )
    smalls = [pltpu.make_async_copy(a, b, small_sem.at[i]) for i, (a, b) in enumerate(small_pairs)]
    for one in loads[:1] + smalls + loads[1:2]:
        one.start()

    barrier = pltpu.get_barrier_semaphore()
    for j in range(sp_count):
        for k in range(2):
            if j + k > 0:
                dev = ((s + j) % sp_count, y * 2 + (c + k) % 2)
                pl.semaphore_signal(barrier, inc=1, device_id=dev, device_id_type=MESH)
    for k in range(2):
        dev = (s, (1 - y) * 2 + (c + k) % 2)
        pl.semaphore_signal(barrier, inc=1, device_id=dev, device_id_type=MESH)

    for one in smalls:
        one.wait()
    for small, table in ((cos_in, cos_ref), (sin_in, sin_ref)):
        for n in range(all_rows // 128):
            at = slice(n * 128, (n + 1) * 128)
            parts = [
                jnp.broadcast_to(small[0, :, r : r + 1], (small.shape[1], GRID_W))
                for r in range(n * 128 // GRID_W, (n + 1) * 128 // GRID_W)
            ]
            table[0, :, at] = jnp.concatenate(parts, axis=1)
            table[1, :, at] = small[1]
    loads[0].wait()
    for one in loads[2:]:
        one.start()
    lines = lax.broadcasted_iota(jnp.int32, (8, cond_ref.shape[1]), 0)
    cond = jnp.where(lines == 0, cond_ref[...], jnp.where(lines == 1, cond_1_ref[...], 0.0))
    cond = cond * jax.nn.sigmoid(cond)
    part[s] = jnp.dot(
        cond, mw[...], precision=lax.Precision.HIGHEST, preferred_element_type=F32
    )[:2]
    loads[1].wait()
    pl.semaphore_wait(barrier, 2 * sp_count + 1)

    sends = [
        remote(part.at[s], part.at[s], part_send.at[j], part_recv.at[s], ((s + j) % sp_count, t))
        for j in range(1, sp_count)
    ]
    sends.append(remote(lat.at[t], lat.at[t], lat_send.at[2], lat_recv.at[2], (s, partner)))
    pieces = (pl.ds(0, first), pl.ds(first, rows - first))
    halves = [
        remote(lat.at[t, at], lat.at[t, at], lat_send.at[i], lat_recv.at[i], (s, across))
        for i, at in enumerate(pieces)
    ]
    for one in sends + halves[:1]:
        one.start()
    for j in range(1, sp_count):
        src = (s + j) % sp_count
        remote(part.at[src], part.at[src], part_send.at[0], part_recv.at[src], (s, partner)).wait_recv()
    total = part[0]
    for j in range(1, sp_count):
        total = total + part[j]
    tot[t] = total
    last = [
        remote(tot.at[t], tot.at[t], tot_send.at[j], tot_recv.at[t], (s, (t + j) % 4))
        for j in range(1, 4)
    ]
    for one in last + halves[1:]:
        one.start()
    sends += last + halves
    for j in range(1, 4):
        src = (t + j) % 4
        remote(tot.at[src], tot.at[src], tot_send.at[0], tot_recv.at[src], (s, partner)).wait_recv()
    cols = tot.shape[2]
    for j in range(4):
        mod[:, j * cols : (j + 1) * cols] = tot[j]

    def relay_rows(i):
        at = pieces[i]
        remote(lat.at[across, at], lat.at[across, at], lat_send.at[0], lat_recv.at[i], (s, partner)).wait_recv()
        one = remote(
            lat.at[across, at], lat.at[across, at], lat_send.at[3 + i], lat_recv.at[3 + i], (s, partner)
        )
        one.start()
        sends.append(one)

    def modulate(value, r):
        value = value.astype(F32)
        scaled = value * lax.rsqrt(jnp.mean(value * value, axis=-1, keepdims=True) + NORM_EPS)
        shift, scale = mod[r : r + 1, :width], mod[r : r + 1, width : 2 * width]
        return (scaled * (1.0 + scale) + shift).astype(BF16)

    q4 = head_dim // 4
    qgain = qg_ref[...] * (head_dim ** (-0.5) * math.log2(math.e))
    kgain = kg_ref[...]

    def turn(yt, cos, sin):
        out = []
        for n in range(2):
            a = yt[2 * n * q4 : (2 * n + 1) * q4]
            b = yt[(2 * n + 1) * q4 : (2 * n + 2) * q4]
            out += [a * cos[n] - b * sin[n], b * cos[n] + a * sin[n]]
        return jnp.concatenate(out, axis=0)

    def unit(yh, gain):
        return yh * lax.rsqrt(jnp.mean(yh * yh, axis=-1, keepdims=True) + NORM_EPS) * gain

    def column(yy):
        return pl.ds(pl.multiple_of(yy * span, span), span)

    def dest(i, n):
        to = (((quad + n) % quads) * 2 + c) * 2 + i
        here = (to == s) & (target == c)
        return to, here

    def free(n):
        return (low == 1) == ((quad + n) % quads > quad)

    def row_spot(lo):
        return pl.ds(pl.multiple_of(lo * span, span), span)

    def allowed(n, which):
        if n == 0:
            return which in ("own", "all")
        if which == "own":
            return False
        straight = {"early": free(n), "late": jnp.logical_not(free(n)) & (c == low)}
        return straight[which] if which in straight else free(n) | (c == low)

    def send_kv(ph, kinds, which, act):
        at, spot = column((y + ph) % 2), row_spot(low)
        for n in range(quads):
            ok = allowed(n, which)
            if ok is False:
                continue
            for i in range(2):
                to, here = dest(i, n)
                for kind in kinds:
                    src, dst = (
                        (kk.at[i, at], kb.at[quad, ph, spot]),
                        (vt.at[i, :, at], vb.at[quad, ph, :, spot]),
                    )[kind]

                    @pl.when(jnp.logical_not(here) & ok)
                    def _():
                        act(remote(
                            src, dst, kv_send.at[kind, ph, n, i], kv_recv.at[kind, ph, z],
                            (to, y * 2 + target),
                        ))

    def send_ctx(which, act):
        for n in range(quads):
            ok = allowed(n, which)
            if ok is False:
                continue
            for i in range(2):
                to, here = dest(i, n)

                @pl.when(jnp.logical_not(here) & ok)
                def _():
                    act(remote(
                        ckv.at[i], cb.at[z], c_send.at[n, i], c_recv.at[z], (to, y * 2 + target)
                    ))

    def pass_on(ph, act):
        spot = row_spot(1 - low)
        for n in range(1, quads):
            to = (((quad + n) % quads) * 2 + low) * 2 + x
            if ph is None:
                copies = [remote(cb.at[mate], cb.at[mate], pass_send.at[4, n], c_recv.at[mate], (to, t))]
            else:
                copies = [
                    remote(ref, ref, pass_send.at[2 * ph + kind, n], kv_recv.at[kind, ph, mate], (to, t))
                    for kind, ref in ((0, kb.at[quad, ph, spot]), (1, vb.at[quad, ph, :, spot]))
                ]

            @pl.when(free(n))
            def _():
                for one in copies:
                    act(one)

    def spot_of(m):
        return m // 2, pl.ds(pl.multiple_of(m % 2 * span, span), span)

    def send_q(ph, act):
        at = column((y + ph) % 2)
        pair, lanes = spot_of(place)
        for i in range(2):
            to = (quad * 2 + c) * 2 + i
            for g in range(2):
                mine = (to == s) & (g == c)
                src = qt.at[i * 2 + g, :, at]

                @pl.when(mine)
                def _():
                    act(remote(
                        src, qb.at[0, ph, pair, :, lanes], q_send.at[ph, i, g],
                        q_recv.at[0, place, ph], (s, partner),
                    ))

                @pl.when(jnp.logical_not(mine))
                def _():
                    act(remote(
                        src, qb.at[1, ph, pair, :, lanes], q_send.at[ph, i, g],
                        q_recv.at[1, place, ph], (to, y * 2 + g),
                    ))

    def start(one):
        one.start()

    def project(ph):
        yy = (y + ph) % 2
        for i in range(2):
            xn[i * rows : (i + 1) * rows, :] = modulate(lat[yy * 2 + i], 0)
        value = xn[...]
        at = column(yy)
        cos, sin = cos_ref[:, :, at], sin_ref[:, :, at]
        spot = row_spot(low)

        def keys():
            full = jnp.dot(value, wk[...], preferred_element_type=F32)
            for h in range(2):
                yh = full[:, h * head_dim : (h + 1) * head_dim]
                kk[h, at, :] = turn(unit(yh, kgain).T, cos, sin).T.astype(BF16)
            send_kv(ph, (0,), "early", start)
            send_kv(ph, (0,), "own", start)

        def values():
            full = jnp.dot(value, wv[...], preferred_element_type=F32)
            for h in range(2):
                vt[h, :, at] = full[:, h * head_dim : (h + 1) * head_dim].T.astype(BF16)
            send_kv(ph, (1,), "early", start)
            send_kv(ph, (1,), "own", start)

            @pl.when(local)
            def _():
                kb[quad, ph, spot] = kk[x, at]
                vb[quad, ph, :, spot] = vt[x, :, at]

        def queries():
            for h in range(4):
                if h % 2 == 0:
                    full = jnp.dot(
                        value, wq[:, h * head_dim : (h + 2) * head_dim], preferred_element_type=F32
                    )
                yh = full[:, (h % 2) * head_dim : (h % 2 + 1) * head_dim]
                qt[h, :, at] = turn(unit(yh, qgain).T, cos, sin).astype(BF16)
            send_q(ph, start)
            pair, lanes = spot_of(place)

            @pl.when(owner)
            def _():
                qb[1, ph, pair, :, lanes] = qt[x * 2 + c, :, at]
                qb[0, ph, pair, :, lanes] = qt[x * 2 + 1 - c, :, at]

        if ph == 1:
            queries()
            for which in ("early", "own", "late"):
                send_ctx(which, start)
        keys()
        values()
        if ph == 0:
            queries()
        send_kv(ph, (0, 1), "late", start)

    def take_q(ph):
        for j in range(1, 4):
            m = (place + j) % 4
            pair, lanes = spot_of(m)
            ref = qb.at[1, ph, pair, :, lanes]
            remote(ref, ref, relay_send.at[0, 0], q_recv.at[1, m, ph], (s, partner)).wait_recv()
            one = remote(
                ref, qb.at[0, ph, pair, :, lanes], relay_send.at[j, ph], q_recv.at[0, m, ph],
                (s, partner),
            )
            one.start()
            sends.append(one)

    def have_q(ph):
        for j in range(4):
            m = (place + j) % 4
            pair, lanes = spot_of(m)
            for role in range(2) if j == 0 else range(1):
                ref = qb.at[role, ph, pair, :, lanes]
                one = remote(ref, ref, relay_send.at[0, 0], q_recv.at[role, m, ph], (s, partner))
                if j == 0:
                    pl.when(jnp.logical_not(owner))(one.wait_recv)
                else:
                    one.wait_recv()

    def wait_kv(zz, ph):
        spot = row_spot(zz % 2)
        for kind, ref in ((0, kb.at[zz // 2, ph, spot]), (1, vb.at[zz // 2, ph, :, spot])):
            remote(ref, ref, kv_send.at[0, 0, 0, 0], kv_recv.at[kind, ph, zz], (s, partner)).wait_recv()

    def have_kv(goal, ph):
        for lo in range(2):
            wait_kv(goal * 2 + lo, ph)

    mate = quad * 2 + 1 - low
    inner = functools.reduce(jnp.logical_or, [free(n) for n in range(1, quads)], low < 0)

    def take_mate(ph):
        @pl.when(inner)
        def _():
            wait_kv(mate, ph)

        pass_on(ph, start)

    def have_own(ph):
        @pl.when(jnp.logical_not(inner))
        def _():
            wait_kv(mate, ph)

        @pl.when(jnp.logical_not(local))
        def _():
            wait_kv(z, ph)

    local = owner & (target == c)
    stat[...] = jnp.concatenate(
        [jnp.full(stat.shape[:3] + (1, all_rows), -1e30, F32), jnp.zeros(stat.shape[:3] + (1, all_rows), F32)],
        axis=3,
    )
    acc[...] = jnp.zeros_like(acc)
    for one in loads[2:]:
        one.wait()
    remote(lat.at[partner], lat.at[partner], lat_send.at[0], lat_recv.at[2], (s, partner)).wait_recv()
    project(0)
    relay_rows(0)
    cn = modulate(ctx[...], 1)
    kc = jnp.dot(cn, wk[...], preferred_element_type=F32)
    vc = jnp.dot(cn, wv[...], preferred_element_type=F32)
    for h in range(2):
        ckv[h, 0] = unit(kc[:, h * head_dim : (h + 1) * head_dim], kgain).astype(BF16)
        ckv[h, 1] = vc[:, h * head_dim : (h + 1) * head_dim].astype(BF16)

    @pl.when(local)
    def _():
        cb[z] = ckv[x]

    relay_rows(1)
    take_mate(0)
    other = (1 - y) * 2 + 1 - c
    for i, at in enumerate(pieces):
        ref = lat.at[other, at]
        remote(ref, ref, lat_send.at[0], lat_recv.at[3 + i], (s, partner)).wait_recv()
    project(1)

    def sweep(ph, keys, values, bias):
        count = keys().shape[0]

        def stage_a(n):
            score[n % 2, :count] = jnp.dot(keys(), qb[n // 2, ph, n % 2], preferred_element_type=F32)

        def stage_b(n):
            sc = score[n % 2, :count]
            old = stat[ph, n // 2, n % 2, 0:1]
            new = jnp.maximum(old, jnp.max(sc, axis=0, keepdims=True) + bias)
            f = jnp.exp2(old - new)
            fade[n % 2] = f
            p = jnp.exp2(sc - (new - bias))
            stat[ph, n // 2, n % 2, 1:2] = (
                stat[ph, n // 2, n % 2, 1:2] * f + jnp.sum(p, axis=0, keepdims=True)
            )
            stat[ph, n // 2, n % 2, 0:1] = new
            prob[n % 2, :count] = p.astype(BF16)

        def stage_c(n):
            value = jnp.dot(values(), prob[n % 2, :count], preferred_element_type=F32)
            acc[ph, n // 2, n % 2] = acc[ph, n // 2, n % 2] * fade[n % 2] + value

        for n in range(6):
            if n < 4:
                stage_a(n)
            if 1 <= n <= 4:
                stage_b(n - 1)
            if n >= 2:
                stage_c(n - 2)

    def give(ph):
        return [
            remote(acc.at[ph, 0], acc_in.at[ph], a_send.at[ph], a_recv.at[ph], (s, partner)),
            remote(stat.at[ph, 0], stat_in.at[ph], s_send.at[ph], s_recv.at[ph], (s, partner)),
        ]

    def have_ctx(goal):
        for lo in range(2):
            k = goal * 2 + lo

            @pl.when(jnp.logical_not(local & (k == z)))
            def _():
                remote(cb.at[k], cb.at[k], c_send.at[0, 0], c_recv.at[k], (s, partner)).wait_recv()

    def sweeps(ph, late, begin, end, wait):
        def one(j, carry):
            goal = (quad + j) % quads
            if wait:

                @pl.when(j > 0)
                def _():
                    have_kv(goal, late)

            sweep(ph, lambda: kb[goal, late], lambda: vb[goal, late], 0.0)
            return carry

        if end - begin == 1:
            one(begin, 0)
        elif end > begin:
            lax.fori_loop(begin, end, one, 0)

    def return_o(m, ph, cc, act):
        to = (quad * 2 + m // 2) * 2 + m % 2
        at = pl.ds(pl.multiple_of(((y + ph) % 2 * 2 + cc) * rows, rows), rows)
        mine = pl.ds(cc * rows, rows)
        head = pl.ds(pl.multiple_of((x * 2 + c) * head_dim, head_dim), head_dim)
        here = (to == s) & owner

        @pl.when(jnp.logical_not(here))
        def _():
            act(remote(
                ob.at[m, ph, mine], att.at[at, head], o_send.at[m, ph, cc],
                o_recv.at[x * 2 + c, ph, cc], (to, y * 2 + low),
            ))

        if act is start:

            @pl.when(here)
            def _():
                att[at, head] = ob[m, ph, mine]

    def merge(ph):
        for one in give(ph):
            one.wait_recv()
        for cc in range(2):
            for j in range(4):
                m = (place + 3 - j) % 4
                pair, half = m // 2, m % 2
                lanes = pl.ds(pl.multiple_of(half * span + cc * rows, rows), rows)
                a, b = stat[ph, 1, pair, 0:1, lanes], stat_in[ph, pair, 0:1, lanes]
                peak = jnp.maximum(a, b)
                wa, wb = jnp.exp2(a - peak), jnp.exp2(b - peak)
                den = 1.0 / (stat[ph, 1, pair, 1:2, lanes] * wa + stat_in[ph, pair, 1:2, lanes] * wb)
                done = acc[ph, 1, pair, :, lanes] * (wa * den) + acc_in[ph, pair, :, lanes] * (wb * den)
                ob[m, ph, cc * rows : (cc + 1) * rows] = done.T.astype(BF16)
            for j in range(4):
                return_o((place + 3 - j) % 4, ph, cc, start)

    step_cols = width // chunks

    def piece(n, yy, cc):
        at = pl.ds(pl.multiple_of((yy * 2 + cc) * rows, rows), rows)
        return jnp.dot(
            att[at, :], wo[:, n * step_cols : (n + 1) * step_cols], preferred_element_type=F32
        )

    cores = [
        [
            remote(core_out.at[h, n], core_in.at[h, n], core_send.at[h, n], core_recv.at[h, n], (s, partner))
            for n in range(chunks)
        ]
        for h in range(2)
    ]
    mesh = [
        remote(mesh_out.at[n], mesh_in.at[n], mesh_send.at[n], mesh_recv.at[n], (s, across))
        for n in range(chunks)
    ]

    def have_o(ph, cc):
        at = pl.ds(pl.multiple_of(((y + ph) % 2 * 2 + cc) * rows, rows), rows)
        for i in range(2):
            for g in range(2):
                ref = att.at[at, pl.ds((i * 2 + g) * head_dim, head_dim)]
                one = remote(ref, ref, o_send.at[0, 0, 0], o_recv.at[i * 2 + g, ph, cc], (s, partner))
                pl.when(jnp.logical_not(owner & (x == i) & (g == c)))(one.wait_recv)

    def mix(ph):
        yy = (y + ph) % 2

        def give_core(cc, n):
            core_out[ph, n] = piece(n, yy, cc).astype(BF16)
            cores[ph][n].start()

        def take_core(n, value):
            cores[ph][n].wait_recv()
            value = value + core_in[ph, n].astype(F32)
            if ph == 1:
                mesh_out[n] = value.astype(BF16)
                mesh[n].start()
            else:
                mixed[n] = value

        have_o(ph, 0)

        @pl.when(c == 1)
        def _():
            for n in range(chunks):
                give_core(0, n)
            have_o(ph, 1)
            for n in range(chunks):
                take_core(n, piece(n, yy, 1))

        @pl.when(c == 0)
        def _():
            for n in range(chunks):
                mixed[n] = piece(n, yy, 0)
            have_o(ph, 1)
            for n in range(chunks):
                give_core(1, n)
                take_core(n, mixed[n])

    take_q(0)
    have_q(0)
    have_own(0)
    sweeps(0, 0, 0, 1, False)
    sweeps(0, 0, 1, quads, True)
    take_q(1)
    have_q(1)
    sweeps(1, 0, 0, 1, False)
    have_ctx(quad)
    pass_on(None, start)
    take_mate(1)
    sweeps(1, 0, 1, quads, False)
    have_own(1)
    sweeps(1, 1, 0, 1, False)
    for n in range(1, quads):
        have_ctx((quad + n) % quads)
    ctx_keys = jnp.concatenate([cb[k, 0] for k in range(z_count)], axis=0)
    ctx_values = jnp.concatenate([cb[k, 1] for k in range(z_count)], axis=0)
    ctx_values = ctx_values.astype(F32).T.astype(BF16)

    def sweep_ctx(ph):
        sweep(ph, lambda: ctx_keys, lambda: ctx_values, lift * math.log2(math.e))

    sweep_ctx(1)
    sweeps(1, 1, 1, quads, True)
    for one in give(1):
        one.start()
    sweeps(0, 1, 0, 1, False)
    merge(1)
    sweeps(0, 1, 1, quads, False)
    sweep_ctx(0)
    for one in give(0):
        one.start()
    mix(1)
    merge(0)
    mix(0)
    square = jnp.zeros((rows, 1), F32)
    for n in range(chunks):
        mesh[n].wait_recv()
        value = mixed[n] + mesh_in[n].astype(F32)
        mixed[n] = value
        square = square + jnp.sum(value * value, axis=-1, keepdims=True)
    inv = lax.rsqrt(square / width + NORM_EPS)
    for n in range(chunks):
        at = slice(n * step_cols, (n + 1) * step_cols)
        gate = mod[0:1, 2 * width + n * step_cols : 2 * width + (n + 1) * step_cols]
        out_ref[:, at] = (lat[t, :, at].astype(F32) + gate * (mixed[n] * inv)).astype(BF16)

    def sent(one):
        one.wait_send()

    for one in sends + give(0) + give(1) + cores[0] + cores[1] + mesh:
        one.wait_send()
    for ph in range(2):
        send_kv(ph, (0, 1), "all", sent)
        pass_on(ph, sent)
        send_q(ph, sent)
        for m in range(4):
            for cc in range(2):
                return_o(m, ph, cc, sent)
    send_ctx("all", sent)
    pass_on(None, sent)


def mix_kernel(
    tp_count, chunks,
    att_ref, wo_hbm, wo_ref, wo_sem, lat_ref, gate_ref,
    out_ref,
    core_out, core_in, mesh_out, mesh_in, mixed, core_send, core_recv, mesh_send, mesh_recv,
):
    s, t = lax.axis_index("sp"), lax.axis_index("tp")
    y, c = t // 2, t % 2
    y_count = tp_count // 2
    partner = y * 2 + 1 - c
    rows, width = lat_ref.shape
    step = width // chunks
    peers = [((y + j) % y_count) * 2 + c for j in range(1, y_count)]
    pltpu.make_async_copy(wo_hbm, wo_ref, wo_sem.at[0]).wait()

    def piece(n, j, cc):
        yy = (y + j) % y_count
        at = pl.ds(pl.multiple_of((yy * 2 + cc) * rows, rows), rows)
        return jnp.dot(
            att_ref[at, :], wo_ref[:, n * step : (n + 1) * step], preferred_element_type=F32
        )

    order = list(range(1, y_count)) + [0]
    cores = [
        remote(core_out.at[n], core_in.at[n], core_send.at[n], core_recv.at[n], (s, partner))
        for n in range(chunks)
    ]
    sent = []
    for n in range(chunks + 1):
        if n < chunks:
            for j in order:
                core_out[n, j] = piece(n, j, 1 - c).astype(BF16)
            cores[n].start()
        if n == 0:
            continue
        m = n - 1
        own = [piece(m, j, c) for j in order]
        cores[m].wait_recv()
        for j, value in zip(order, own):
            value = value + core_in[m, j].astype(F32)
            if j == 0:
                mixed[m] = value
            else:
                mesh_out[m, j - 1] = value.astype(BF16)
                one = remote(
                    mesh_out.at[m, j - 1], mesh_in.at[m, j - 1], mesh_send.at[m, j - 1],
                    mesh_recv.at[m, j - 1], (s, peers[j - 1]),
                )
                one.start()
                sent.append(one)
    for one in sent:
        one.wait_recv()
    square = jnp.zeros((rows, 1), F32)
    for n in range(chunks):
        value = mixed[n]
        for j in range(1, y_count):
            value = value + mesh_in[n, j - 1].astype(F32)
        mixed[n] = value
        square = square + jnp.sum(value * value, axis=-1, keepdims=True)
    inv = lax.rsqrt(square / width + NORM_EPS)
    for n in range(chunks):
        at = slice(n * step, (n + 1) * step)
        out_ref[:, at] = (
            lat_ref[:, at].astype(F32) + gate_ref[:, at] * (mixed[n] * inv)
        ).astype(BF16)
    for one in sent + cores:
        one.wait_send()


def whole_kernel(sp_count, tp_count, x_count, head_dim, group, lift, chunks, counts, *refs):
    (
        cond, cond_1, mw, lat, ctx, wq, wk, wv, qg, kg, cos, sin, wo, lat_rows,
        out, qt, k, vt, ckv, gate, att, wo_vm, wo_sem, *rest,
    ) = refs
    front, middle, last = counts
    front_scratch, middle_scratch = rest[:front], rest[front : front + middle]
    front_kernel(
        sp_count, tp_count, head_dim, cond, cond_1, mw, lat, ctx, wq, wk, wv, qg, kg, cos, sin,
        qt, k, vt, ckv, gate, *front_scratch, wo, wo_vm, wo_sem,
    )
    attend_kernel(sp_count, x_count, group, lift, k, vt, ckv, qt, att, *middle_scratch)
    mix_kernel(
        tp_count, chunks, att, wo, wo_vm, wo_sem, lat_rows, gate, out, *rest[front + middle :]
    )


ANY = pl.BlockSpec(memory_space=pl.ANY)
VM = pl.BlockSpec(memory_space=pltpu.VMEM)
DMA = pltpu.SemaphoreType.DMA


def grid_tables(sp_count, all_rows, head_dim):
    quarter, lines, lane = head_dim // 4, all_rows // GRID_W, np.arange(128)
    inv_freq = np.float32(ROPE_BASE) ** (-np.arange(quarter, dtype=np.float32) / quarter)
    rows = np.arange(sp_count)[:, None] * lines + lane[None, :] % lines
    both = np.stack([rows, np.broadcast_to(lane % GRID_W, rows.shape)], axis=1).astype(np.float32)
    angles = (both[:, :, None, :] * inv_freq[None, None, :, None]).astype(np.float32)
    return jnp.asarray(np.cos(angles)), jnp.asarray(np.sin(angles))


def quad_call(args, out_weight, sp_count, head_dim, lift):
    mod_weight, latents, context, query_weight, key_matrix, value_matrix = args[2:8]
    rows, width = latents.shape
    ctx_rows = context.shape[0]
    mod_cols = mod_weight.shape[1]
    all_rows, z_count, quads, chunks = 4 * rows, sp_count // 2, sp_count // 4, 4
    step = width // chunks
    cos, sin = grid_tables(sp_count, all_rows, head_dim)
    block = max(all_rows, z_count * ctx_rows)
    scratch = [
        pltpu.VMEM(args[0].shape, F32),
        pltpu.VMEM(args[1].shape, F32),
        pltpu.VMEM(args[8].shape, F32),
        pltpu.VMEM(args[9].shape, F32),
        pltpu.VMEM(cos.shape[1:], F32),
        pltpu.VMEM(sin.shape[1:], F32),
        DMA((6,)),
        pltpu.VMEM(mod_weight.shape, F32),
        pltpu.VMEM((4, rows, width), BF16),
        pltpu.VMEM(context.shape, BF16),
        pltpu.VMEM(query_weight.shape, BF16),
        pltpu.VMEM(key_matrix.shape, BF16),
        pltpu.VMEM(value_matrix.shape, BF16),
        pltpu.VMEM(out_weight.shape, BF16),
        pltpu.VMEM((2, head_dim // 4, all_rows), F32),
        pltpu.VMEM((2, head_dim // 4, all_rows), F32),
        pltpu.VMEM((sp_count, 2, mod_cols), F32),
        pltpu.VMEM((4, 2, mod_cols), F32),
        pltpu.VMEM((2, 4 * mod_cols), F32),
        pltpu.VMEM((2 * rows, width), BF16),
        pltpu.VMEM((4, head_dim, all_rows), BF16),
        pltpu.VMEM((2, all_rows, head_dim), BF16),
        pltpu.VMEM((2, head_dim, all_rows), BF16),
        pltpu.VMEM((2, 2, ctx_rows, head_dim), BF16),
        pltpu.VMEM((2, 2, 2, head_dim, all_rows), BF16),
        pltpu.VMEM((quads, 2, all_rows, head_dim), BF16),
        pltpu.VMEM((quads, 2, head_dim, all_rows), BF16),
        pltpu.VMEM((z_count, 2, ctx_rows, head_dim), BF16),
        pltpu.VMEM((2, 2, 2, 2, all_rows), F32),
        pltpu.VMEM((2, 2, 2, head_dim, all_rows), F32),
        pltpu.VMEM((2, 2, 2, all_rows), F32),
        pltpu.VMEM((2, 2, head_dim, all_rows), F32),
        pltpu.VMEM((2, block, all_rows), F32),
        pltpu.VMEM((2, block, all_rows), BF16),
        pltpu.VMEM((2, 1, all_rows), F32),
        pltpu.VMEM((4, 2, 2 * rows, head_dim), BF16),
        pltpu.VMEM((all_rows, 4 * head_dim), BF16),
        pltpu.VMEM((2, chunks, rows, step), BF16),
        pltpu.VMEM((2, chunks, rows, step), BF16),
        pltpu.VMEM((chunks, rows, step), BF16),
        pltpu.VMEM((chunks, rows, step), BF16),
        pltpu.VMEM((chunks, rows, step), F32),
        DMA((7,)),
        DMA((5,)),
        DMA((5,)),
        DMA((sp_count,)),
        DMA((sp_count,)),
        DMA((4,)),
        DMA((4,)),
        DMA((2, 2, quads, 2)),
        DMA((2, 2, z_count)),
        DMA((quads, 2)),
        DMA((z_count,)),
        DMA((2, 2, 2)),
        DMA((2, 4, 2)),
        DMA((4, 2)),
        DMA((5, quads)),
        DMA((2,)),
        DMA((2,)),
        DMA((2,)),
        DMA((2,)),
        DMA((4, 2, 2)),
        DMA((4, 2, 2)),
        DMA((2, chunks)),
        DMA((2, chunks)),
        DMA((chunks,)),
        DMA((chunks,)),
    ]
    out = pl.pallas_call(
        functools.partial(quad_kernel, sp_count, head_dim, lift, chunks),
        out_shape=pltpu.VMEM((rows, width), BF16),
        in_specs=[pl.BlockSpec(memory_space=pltpu.HBM)] * 13,
        out_specs=VM,
        scratch_shapes=scratch,
        compiler_params=pltpu.CompilerParams(
            collective_id=0, has_side_effects=True, vmem_limit_bytes=VMEM_BYTES - 2 * rows * width * 2
        ),
        name="quad",
    )(*args, cos, sin, out_weight)
    return out


def body(
    latents,
    context,
    cond,
    ctx_cond,
    mod_weight,
    query_weight,
    key_matrix,
    value_matrix,
    out_weight,
    query_gain,
    key_gain,
):
    sp_count, tp_count = lax.axis_size("sp"), lax.axis_size("tp")
    x_count = row_size(sp_count)
    rows, width = latents.shape
    ctx_rows = context.shape[0]
    head_dim = query_gain.shape[0]
    heads = query_weight.shape[1] // head_dim
    kv_heads = key_matrix.shape[1] // head_dim
    all_rows = rows * tp_count
    mod_cols = mod_weight.shape[1]
    lift = math.log(sp_count * all_rows / (2.0 * sp_count * ctx_rows))
    group = heads // kv_heads
    args = (
        cond[None], ctx_cond[None], mod_weight, latents, context, query_weight, key_matrix, value_matrix,
        query_gain[None], key_gain[None],
    )
    wide = all_rows % GRID_W == 0 and all_rows == rows * 4 and rows % 128 == 0
    if wide and kv_heads == 2 and group == 2 and x_count == 2 and sp_count % 4 == 0:
        return quad_call(args, out_weight, sp_count, head_dim, lift)
    chunks = 4
    y_count = tp_count // 2
    step = width // chunks
    far = max(y_count - 1, 1)
    positions = lax.axis_index("sp") * all_rows + jnp.arange(all_rows, dtype=jnp.int32)
    cos, sin = tables(positions, head_dim)
    shared = [
        pltpu.VMEM((heads, head_dim, all_rows), BF16),
        pltpu.VMEM((kv_heads, all_rows, head_dim), BF16),
        pltpu.VMEM((kv_heads, head_dim, all_rows), BF16),
        pltpu.VMEM((kv_heads, 2, ctx_rows, head_dim), BF16),
        pltpu.VMEM((1, width), F32),
        pltpu.VMEM((all_rows, heads * head_dim), BF16),
        pltpu.VMEM(out_weight.shape, BF16),
        DMA((1,)),
    ]
    front = [
        pltpu.VMEM(mod_weight.shape, F32),
        pltpu.VMEM((tp_count, rows, width), BF16),
        pltpu.VMEM(query_weight.shape, BF16),
        pltpu.VMEM(key_matrix.shape, BF16),
        pltpu.VMEM(value_matrix.shape, BF16),
        pltpu.VMEM((sp_count, 2, mod_cols), F32),
        pltpu.VMEM((tp_count, 2, mod_cols), F32),
        pltpu.VMEM((2, mod_cols * tp_count), F32),
        pltpu.VMEM((2 * rows, width), BF16),
        DMA((5,)),
        DMA((tp_count,)),
        DMA((tp_count,)),
        DMA((sp_count,)),
        DMA((sp_count,)),
        DMA((tp_count,)),
        DMA((tp_count,)),
    ]
    middle = [
        pltpu.VMEM((sp_count, kv_heads, all_rows, head_dim), BF16),
        pltpu.VMEM((sp_count, kv_heads, head_dim, all_rows), BF16),
        pltpu.VMEM((sp_count, kv_heads, 2, ctx_rows, head_dim), BF16),
        pltpu.VMEM((heads, 1, all_rows), F32),
        pltpu.VMEM((heads, 1, all_rows), F32),
        pltpu.VMEM((heads, head_dim, all_rows), F32),
        DMA((3,)),
    ]
    middle += [DMA((3, sp_count, x_count + 1)), DMA((3, sp_count))]
    last = [
        pltpu.VMEM((chunks, y_count, rows, step), BF16),
        pltpu.VMEM((chunks, y_count, rows, step), BF16),
        pltpu.VMEM((chunks, far, rows, step), BF16),
        pltpu.VMEM((chunks, far, rows, step), BF16),
        pltpu.VMEM((chunks, rows, step), F32),
        DMA((chunks,)),
        DMA((chunks,)),
        DMA((chunks, far)),
        DMA((chunks, far)),
    ]
    counts = (len(front), len(middle), len(last))
    return pl.pallas_call(
        functools.partial(
            whole_kernel, sp_count, tp_count, x_count, head_dim, group, lift, chunks, counts
        ),
        out_shape=jax.ShapeDtypeStruct((rows, width), BF16),
        in_specs=[VM, VM, ANY, ANY, VM, ANY, ANY, ANY, VM, VM, VM, VM, ANY, VM],
        out_specs=VM,
        scratch_shapes=shared + front + middle + last,
        compiler_params=pltpu.CompilerParams(
            collective_id=0, has_side_effects=True, vmem_limit_bytes=VMEM_BYTES
        ),
        name="whole",
    )(
        *args, cos, sin, out_weight, latents,
    )


def solution(mesh):
    placed = (
        P(("sp", "tp"), None),
        P("sp", None),
        P("sp"),
        P("sp"),
        P("sp", "tp"),
        P(None, "tp"),
        P(None, "tp"),
        P(None, "tp"),
        P("tp", None),
        P(),
        P(),
    )
    return jax.shard_map(
        body, mesh=mesh, in_specs=placed, out_specs=P(("sp", "tp"), None), check_vma=False
    )
```

```python
import functools
import math

import jax
import jax.numpy as jnp
import numpy as np
from jax import lax
from jax.experimental import pallas as pl
from jax.experimental.pallas import tpu as pltpu
from jax.sharding import PartitionSpec as P

GRID_W = 64
NORM_EPS = 1e-06
ROPE_BASE = 10000.0
MESH = pl.DeviceIdType.MESH
BF16 = jnp.bfloat16
F32 = jnp.float32
VMEM_BYTES = 67043328


def row_size(sp_count):
    size = 1
    while 4 * size * size <= sp_count:
        size *= 2
    return size


def tables(positions, head_dim):
    quarter = head_dim // 4
    inv_freq = ROPE_BASE ** (-jnp.arange(quarter, dtype=F32) / quarter)
    where = jnp.stack([positions // GRID_W, positions % GRID_W]).astype(F32)
    angles = where[:, None, :] * inv_freq[None, :, None]
    return jnp.cos(angles), jnp.sin(angles)


def remote(src, dst, send, recv, dev):
    return pltpu.make_async_remote_copy(
        src_ref=src, dst_ref=dst, send_sem=send, recv_sem=recv, device_id=dev, device_id_type=MESH
    )


def front_kernel(
    sp_count, tp_count, head_dim,
    cond_ref, cond_1_ref, mw_hbm, lat_hbm, ctx_ref, wq_hbm, wk_hbm, wv_hbm, qg_ref, kg_ref, cos_ref, sin_ref,
    qt_ref, k_ref, vt_ref, ckv_ref, gate_ref,
    mw, lat, wq, wk, wv, part, tot, mod, xn, load_sem,
    lat_send, lat_recv, part_send, part_recv, tot_send, tot_recv,
    wo_hbm, wo_vm, wo_sem,
):
    s, t = lax.axis_index("sp"), lax.axis_index("tp")
    y, c = t // 2, t % 2
    y_count = tp_count // 2
    partner = y * 2 + 1 - c
    rows = lat.shape[1]
    width = lat.shape[2]
    model_cols = mod.shape[1]

    own = pltpu.make_async_copy(lat_hbm, lat.at[t], load_sem.at[0])
    own.start()
    loads = [
        pltpu.make_async_copy(a, b, load_sem.at[1 + i])
        for i, (a, b) in enumerate(((mw_hbm, mw), (wq_hbm, wq), (wk_hbm, wk), (wv_hbm, wv)))
    ]
    for one in loads:
        one.start()

    pltpu.make_async_copy(wo_hbm, wo_vm, wo_sem.at[0]).start()

    barrier = pltpu.get_barrier_semaphore()
    for j in range(1, sp_count):
        pl.semaphore_signal(barrier, inc=1, device_id=((s + j) % sp_count, t), device_id_type=MESH)
    for j in range(1, tp_count):
        pl.semaphore_signal(barrier, inc=1, device_id=(s, (t + j) % tp_count), device_id_type=MESH)
    pl.semaphore_wait(barrier, sp_count + tp_count - 2)

    own.wait()
    sends = []
    for j in range(1, y_count):
        peer = ((y + j) % y_count) * 2 + c
        sends.append(remote(lat.at[t], lat.at[t], lat_send.at[j], lat_recv.at[t], (s, peer)))
    sends.append(remote(lat.at[t], lat.at[t], lat_send.at[0], lat_recv.at[t], (s, partner)))
    for one in sends:
        one.start()

    loads[0].wait()
    lines = lax.broadcasted_iota(jnp.int32, (8, cond_ref.shape[1]), 0)
    cond = jnp.where(lines == 0, cond_ref[...], jnp.where(lines == 1, cond_1_ref[...], 0.0))
    cond = cond * jax.nn.sigmoid(cond)
    part[s] = jnp.dot(
        cond, mw[...], precision=lax.Precision.HIGHEST, preferred_element_type=F32
    )[:2]
    more = [
        remote(part.at[s], part.at[s], part_send.at[j], part_recv.at[s], ((s + j) % sp_count, t))
        for j in range(1, sp_count)
    ]
    for one in more:
        one.start()
    for j in range(1, sp_count):
        src = (s + j) % sp_count
        remote(part.at[src], part.at[src], part_send.at[0], part_recv.at[src], (s, t)).wait_recv()
    total = part[0]
    for j in range(1, sp_count):
        total = total + part[j]
    tot[t] = total
    last = [
        remote(tot.at[t], tot.at[t], tot_send.at[j], tot_recv.at[t], (s, (t + j) % tp_count))
        for j in range(1, tp_count)
    ]
    for one in last:
        one.start()
    for j in range(1, tp_count):
        src = (t + j) % tp_count
        remote(tot.at[src], tot.at[src], tot_send.at[0], tot_recv.at[src], (s, t)).wait_recv()
    cols = model_cols // tp_count
    for j in range(tp_count):
        mod[:, j * cols : (j + 1) * cols] = tot[j]
    gate_ref[...] = mod[0:1, 2 * width :]

    def modulate(x, r):
        x = x.astype(F32)
        scaled = x * lax.rsqrt(jnp.mean(x * x, axis=-1, keepdims=True) + NORM_EPS)
        shift, scale = mod[r : r + 1, :width], mod[r : r + 1, width : 2 * width]
        return (scaled * (1.0 + scale) + shift).astype(BF16)

    for one in loads[1:]:
        one.wait()

    cn = modulate(ctx_ref[...], 1)
    kc = jnp.dot(cn, wk[...], preferred_element_type=F32)
    vc = jnp.dot(cn, wv[...], preferred_element_type=F32)
    for h in range(kc.shape[1] // head_dim):
        kh = kc[:, h * head_dim : (h + 1) * head_dim]
        kh = kh * lax.rsqrt(jnp.mean(kh * kh, axis=-1, keepdims=True) + NORM_EPS) * kg_ref[...]
        ckv_ref[h, 0] = kh.astype(BF16)
        ckv_ref[h, 1] = vc[:, h * head_dim : (h + 1) * head_dim].astype(BF16)

    q4 = head_dim // 4
    qgain, kgain = qg_ref[...], kg_ref[...]

    def turn(yt, cos, sin):
        out = []
        for n in range(2):
            a = yt[2 * n * q4 : (2 * n + 1) * q4]
            b = yt[(2 * n + 1) * q4 : (2 * n + 2) * q4]
            out += [a * cos[n] - b * sin[n], b * cos[n] + a * sin[n]]
        return jnp.concatenate(out, axis=0)

    def unit(yh, gain):
        return yh * lax.rsqrt(jnp.mean(yh * yh, axis=-1, keepdims=True) + NORM_EPS) * gain

    span = 2 * rows
    relays = []
    for j in range(y_count):
        yy = (y + j) % y_count
        if j > 0:
            src = yy * 2 + c
            remote(lat.at[src], lat.at[src], lat_send.at[0], lat_recv.at[src], (s, t)).wait_recv()
            one = remote(
                lat.at[src], lat.at[src], lat_send.at[y_count - 1 + j], lat_recv.at[src], (s, partner)
            )
            one.start()
            relays.append(one)
        other = yy * 2 + 1 - c
        remote(lat.at[other], lat.at[other], lat_send.at[0], lat_recv.at[other], (s, t)).wait_recv()
        for i in range(2):
            xn[i * rows : (i + 1) * rows, :] = modulate(lat[yy * 2 + i], 0)
        x = xn[...]
        at = pl.ds(pl.multiple_of(yy * span, span), span)
        cos, sin = cos_ref[:, :, at], sin_ref[:, :, at]
        for w, kind in ((wq, 0), (wk, 1), (wv, 2)):
            step = min(2 * head_dim, w.shape[1])
            for n in range(0, w.shape[1], step):
                full = jnp.dot(x, w[:, n : n + step], preferred_element_type=F32)
                for m in range(0, step, head_dim):
                    h = (n + m) // head_dim
                    yh = full[:, m : m + head_dim]
                    if kind == 0:
                        qt_ref[h, :, at] = turn(unit(yh, qgain).T, cos, sin).astype(BF16)
                    elif kind == 1:
                        k_ref[h, at, :] = turn(unit(yh, kgain).T, cos, sin).T.astype(BF16)
                    else:
                        vt_ref[h, :, at] = yh.T.astype(BF16)
    for one in sends + more + last + relays:
        one.wait_send()


def attend_kernel(
    sp_count, x_count, group, lift,
    k_hbm, vt_hbm, ckv_hbm, qt_ref,
    out_ref,
    kb, vb, cb, top, tot, acc, load_sem, send_sem, recv_sem,
):
    s, t = lax.axis_index("sp"), lax.axis_index("tp")
    z, x = s // x_count, s % x_count
    z_count = sp_count // x_count
    heads, head_dim, rows = qt_ref.shape
    kv_heads = heads // group
    factor = head_dim ** (-0.5) * math.log2(math.e)

    loads = [
        pltpu.make_async_copy(a, b, load_sem.at[i])
        for i, (a, b) in enumerate(
            (
                (ckv_hbm, cb.at[s]),
                (k_hbm, kb.at[s]),
                (vt_hbm, vb.at[s]),
            )
        )
    ]
    for one in loads:
        one.start()
    targets = []
    for sign in (1, -1):
        ok = (z + sign >= 0) & (z + sign < z_count)
        peer = ((z + sign + z_count) % z_count) * x_count + x
        targets.append((ok, peer))

    top[...] = jnp.full_like(top, -1e30)
    tot[...] = jnp.zeros_like(tot)
    acc[...] = jnp.zeros_like(acc)
    for one in loads:
        one.wait()

    bufs = (cb, kb, vb)

    def copies(src, way, peer):
        return [
            remote(b.at[src], b.at[src], send_sem.at[i, src, way], recv_sem.at[i, src], (peer, t))
            for i, b in enumerate(bufs)
        ]

    def source(k):
        low = jnp.minimum(z, z_count - 1 - z)
        both = k <= 2 * low
        dist = jnp.where(both, (k + 1) // 2, k - low)
        up = jnp.where(both, k % 2 == 1, z < z_count - 1 - z)
        return jnp.where(up, z + dist, z - dist)

    def update(i, keys, values_t, bias):
        sc = jnp.dot(keys, qt_ref[i], preferred_element_type=F32) * factor
        if bias != 0.0:
            sc = sc + bias
        old = top[i]
        new = jnp.maximum(old, jnp.max(sc, axis=0, keepdims=True))
        p = jnp.exp2(sc - new)
        f = jnp.exp2(old - new)
        top[i] = new
        tot[i] = tot[i] * f + jnp.sum(p, axis=0, keepdims=True)
        acc[i] = acc[i] * f + jnp.dot(values_t, p.astype(BF16), preferred_element_type=F32)

    def block(src):
        def head(i, carry):
            h = i // group
            update(i, kb[src, h], vb[src, h], 0.0)
            return carry

        lax.fori_loop(0, heads, head, 0)

    def wait_from(src):
        for one in copies(src, 0, s):
            one.wait_recv()

    def step(k, carry):
        zz = source(k)
        src = zz * x_count + x

        @pl.when(k > 0)
        def _():
            wait_from(src)

        for way, (ok, peer) in enumerate(targets):
            mine = zz <= z if way == 0 else zz >= z

            @pl.when(ok & mine)
            def _():
                for one in copies(src, way, peer):
                    one.start()

        for j in range(1, x_count):
            for one in copies(src, 1 + j, z * x_count + (x + j) % x_count):
                one.start()
        block(src)

        @pl.when(k > 0)
        def _():
            before = source(k - 1)
            for j in range(1, x_count):
                old = before * x_count + (x + j) % x_count
                wait_from(old)
                block(old)

        return carry

    lax.fori_loop(0, z_count, step, 0)
    final = source(z_count - 1)
    ends = [final * x_count + (x + j) % x_count for j in range(1, x_count)]
    for src in ends:
        copies(src, 0, s)[0].wait_recv()
    for i in range(heads):
        h = i // group
        keys = jnp.concatenate([cb[j, h, 0] for j in range(sp_count)], axis=0)
        vals = jnp.concatenate([cb[j, h, 1] for j in range(sp_count)], axis=0)
        update(i, keys, vals.astype(F32).T.astype(BF16), lift * math.log2(math.e))
    for src in ends:
        for one in copies(src, 0, s)[1:]:
            one.wait_recv()
        block(src)
    for i in range(heads):
        out_ref[:, i * head_dim : (i + 1) * head_dim] = (acc[i] / tot[i]).T.astype(BF16)

    def drain(k, carry):
        zz = source(k)
        src = zz * x_count + x
        for way, (ok, peer) in enumerate(targets):
            mine = zz <= z if way == 0 else zz >= z

            @pl.when(ok & mine)
            def _():
                for one in copies(src, way, peer):
                    one.wait_send()

        for j in range(1, x_count):
            for one in copies(src, 1 + j, z * x_count + (x + j) % x_count):
                one.wait_send()
        return carry

    lax.fori_loop(0, z_count, drain, 0)


def quad_kernel(sp_count, head_dim, lift, chunks, *refs):
    (
        cond_hbm, cond_1_hbm, mw_hbm, lat_hbm, ctx_hbm, wq_hbm, wk_hbm, wv_hbm, qg_hbm, kg_hbm,
        cos_hbm, sin_hbm, wo_hbm,
        out_ref,
        cond_ref, cond_1_ref, qg_ref, kg_ref, cos_in, sin_in, small_sem,
        mw, lat, ctx, wq, wk, wv, wo, cos_ref, sin_ref, part, tot, mod, xn, xs,
        qt, kk, vt, ckv, qb, kb, vb, cb, stat, acc, stat_in, acc_in,
        score, prob, fade, ob, att, core_out, core_in, mesh_out, mesh_in, mixed,
        load_sem, lat_send, lat_recv, part_send, part_recv, tot_send, tot_recv,
        kv_send, kv_recv, c_send, c_recv, q_send, q_recv, relay_send, pass_send, raw_send, raw_recv,
        a_send, a_recv, s_send, s_recv, o_recv, core_recv, mesh_send, mesh_recv,
    ) = refs
    s, t = lax.axis_index("sp"), lax.axis_index("tp")
    y, c = t // 2, t % 2
    z, x = s // 2, s % 2
    z_count = sp_count // 2
    quads = z_count // 2
    quad, low = z // 2, z % 2
    place = low * 2 + x
    partner, across = y * 2 + 1 - c, (1 - y) * 2 + c
    target = (z + x) % 2
    owner = low == c
    rows, width = lat.shape[1], lat.shape[2]
    all_rows = 4 * rows
    span = 2 * rows
    cuts = (0, rows * 3 // 8 // 16 * 16, rows * 3 // 4 // 16 * 16, rows)

    load_pairs = (
        (mw_hbm, mw), (lat_hbm, lat.at[t]), (wk_hbm, wk), (wv_hbm, wv), (wq_hbm, wq), (ctx_hbm, ctx.at[quad]),
        (wo_hbm, wo),
    )
    loads = [pltpu.make_async_copy(a, b, load_sem.at[i]) for i, (a, b) in enumerate(load_pairs)]
    small_pairs = (
        (cond_hbm, cond_ref), (cond_1_hbm, cond_1_ref), (cos_hbm.at[s], cos_in), (sin_hbm.at[s], sin_in),
        (qg_hbm, qg_ref), (kg_hbm, kg_ref),
    )
    smalls = [pltpu.make_async_copy(a, b, small_sem.at[i]) for i, (a, b) in enumerate(small_pairs)]
    for one in smalls[:2] + loads[:1] + smalls[2:] + loads[1:2]:
        one.start()

    barrier = pltpu.get_barrier_semaphore()
    for j in range(sp_count):
        for k in range(2):
            if j + k > 0:
                dev = ((s + j) % sp_count, y * 2 + (c + k) % 2)
                pl.semaphore_signal(barrier, inc=1, device_id=dev, device_id_type=MESH)
    for k in range(2):
        dev = (s, (1 - y) * 2 + (c + k) % 2)
        pl.semaphore_signal(barrier, inc=1, device_id=dev, device_id_type=MESH)

    for one in smalls:
        one.wait()
    lines = lax.broadcasted_iota(jnp.int32, (8, cond_ref.shape[1]), 0)
    cond = jnp.where(lines == 0, cond_ref[...], jnp.where(lines == 1, cond_1_ref[...], 0.0))
    cond = (cond * jax.nn.sigmoid(cond)).T
    for small, table in ((cos_in, cos_ref), (sin_in, sin_ref)):
        for n in range(all_rows // 128):
            at = slice(n * 128, (n + 1) * 128)
            parts = [
                jnp.broadcast_to(small[0, :, r : r + 1], (small.shape[1], GRID_W))
                for r in range(n * 128 // GRID_W, (n + 1) * 128 // GRID_W)
            ]
            table[0, :, at] = jnp.concatenate(parts, axis=1)
            table[1, :, at] = small[1]
    loads[0].wait()
    for one in loads[2:]:
        one.start()
    for r in range(2):
        part[s, r : r + 1, :] = jnp.sum(mw[...] * cond[:, r : r + 1], axis=0, keepdims=True)
    loads[1].wait()
    pl.semaphore_wait(barrier, 2 * sp_count + 1)

    sends = [
        remote(part.at[s], part.at[s], part_send.at[j], part_recv.at[s], ((s + j) % sp_count, t))
        for j in range(1, sp_count)
    ]
    sends.append(remote(lat.at[t], lat.at[t], lat_send.at[6], lat_recv.at[6], (s, partner)))
    pieces = [pl.ds(a, b - a) for a, b in zip(cuts, cuts[1:])]
    halves = [
        remote(lat.at[t, at], lat.at[t, at], lat_send.at[i], lat_recv.at[i], (s, across))
        for i, at in enumerate(pieces)
    ]
    for one in sends + halves[:1]:
        one.start()
    def unit_rows(value):
        value = value.astype(F32)
        return value * lax.rsqrt(jnp.mean(value * value, axis=-1, keepdims=True) + NORM_EPS)

    remote(lat.at[partner], lat.at[partner], lat_send.at[0], lat_recv.at[6], (s, partner)).wait_recv()
    for i in range(2):
        xs[i * rows : (i + 1) * rows, :] = unit_rows(lat[y * 2 + i])
    for j in range(1, sp_count):
        src = (s + j) % sp_count
        remote(part.at[src], part.at[src], part_send.at[0], part_recv.at[src], (s, partner)).wait_recv()
    total = part[0]
    for j in range(1, sp_count):
        total = total + part[j]
    tot[t] = total
    last = [
        remote(tot.at[t], tot.at[t], tot_send.at[j], tot_recv.at[t], (s, (t + j) % 4))
        for j in range(1, 4)
    ]
    ctx_rows = ctx.shape[1]
    half = ctx_rows // 2
    mine = pl.ds(pl.multiple_of(c * half, half), half)
    yours = pl.ds(pl.multiple_of((1 - c) * half, half), half)
    loads[5].wait()
    raw = [
        remote(
            ctx.at[quad, mine], ctx.at[quad, mine], raw_send.at[0, n], raw_recv.at[0, quad],
            ((((quad + n) % quads) * 2 + low) * 2 + x, t),
        )
        for n in range(1, quads)
    ]
    for one in last + halves[1:] + raw:
        one.start()
    sends += last + halves + raw
    for j in range(1, 4):
        src = (t + j) % 4
        remote(tot.at[src], tot.at[src], tot_send.at[0], tot_recv.at[src], (s, partner)).wait_recv()
    cols = tot.shape[2]
    for j in range(4):
        mod[:, j * cols : (j + 1) * cols] = tot[j]

    def relay_rows(i):
        at = pieces[i]
        remote(lat.at[across, at], lat.at[across, at], lat_send.at[0], lat_recv.at[i], (s, partner)).wait_recv()
        one = remote(
            lat.at[across, at], lat.at[across, at], lat_send.at[3 + i], lat_recv.at[3 + i], (s, partner)
        )
        one.start()
        sends.append(one)

    def modulate(scaled, r):
        shift, scale = mod[r : r + 1, :width], mod[r : r + 1, width : 2 * width]
        return (scaled * (1.0 + scale) + shift).astype(BF16)

    q4 = head_dim // 4
    qgain = qg_ref[...] * (head_dim ** (-0.5) * math.log2(math.e))
    kgain = kg_ref[...]

    def turn(yt, cos, sin):
        out = []
        for n in range(2):
            a = yt[2 * n * q4 : (2 * n + 1) * q4]
            b = yt[(2 * n + 1) * q4 : (2 * n + 2) * q4]
            out += [a * cos[n] - b * sin[n], b * cos[n] + a * sin[n]]
        return jnp.concatenate(out, axis=0)

    def unit(yh, gain):
        return yh * lax.rsqrt(jnp.mean(yh * yh, axis=-1, keepdims=True) + NORM_EPS) * gain

    def column(yy):
        return pl.ds(pl.multiple_of(yy * span, span), span)

    def dest(i, n):
        to = (((quad + n) % quads) * 2 + c) * 2 + i
        here = (to == s) & (target == c)
        return to, here

    def free(n):
        return (low == 1) == ((quad + n) % quads > quad)

    def row_spot(lo):
        return pl.ds(pl.multiple_of(lo * span, span), span)

    def allowed(n, which):
        if n == 0:
            return which in ("own", "all")
        if which == "own":
            return False
        straight = {"early": free(n), "late": jnp.logical_not(free(n)) & (c == low)}
        return straight[which] if which in straight else free(n) | (c == low)

    def send_kv(ph, kinds, which, act):
        at, spot = column((y + ph) % 2), row_spot(low)
        for n in range(quads):
            ok = allowed(n, which)
            if ok is False:
                continue
            for i in range(2):
                to, here = dest(i, n)
                for kind in kinds:
                    src, dst = (
                        (kk.at[i, at], kb.at[quad, ph, spot]),
                        (vt.at[i, :, at], vb.at[quad, ph, :, spot]),
                    )[kind]

                    @pl.when(jnp.logical_not(here) & ok)
                    def _():
                        act(remote(
                            src, dst, kv_send.at[kind, ph, n, i], kv_recv.at[kind, ph, z],
                            (to, y * 2 + target),
                        ))

    def send_ctx(act):
        for i in range(2):
            to, here = dest(i, 0)

            @pl.when(jnp.logical_not(here))
            def _():
                act(remote(ckv.at[i], cb.at[low], c_send.at[i], c_recv.at[low], (to, y * 2 + target)))

    def pass_on(ph, act):
        spot = row_spot(1 - low)
        for n in range(1, quads):
            to = (((quad + n) % quads) * 2 + low) * 2 + x
            copies = [
                remote(ref, ref, pass_send.at[2 * ph + kind, n], kv_recv.at[kind, ph, mate], (to, t))
                for kind, ref in ((0, kb.at[quad, ph, spot]), (1, vb.at[quad, ph, :, spot]))
            ]

            @pl.when(free(n))
            def _():
                for one in copies:
                    act(one)

    def spot_of(m):
        return m // 2, pl.ds(pl.multiple_of(m % 2 * span, span), span)

    def send_q(ph, act):
        at = column((y + ph) % 2)
        pair, lanes = spot_of(place)
        for i in range(2):
            to = (quad * 2 + c) * 2 + i
            for g in range(2):
                mine = (to == s) & (g == c)
                src = qt.at[i * 2 + g, :, at]

                @pl.when(mine)
                def _():
                    act(remote(
                        src, qb.at[0, ph, pair, :, lanes], q_send.at[ph, i, g],
                        q_recv.at[0, place, ph], (s, partner),
                    ))

                @pl.when(jnp.logical_not(mine))
                def _():
                    act(remote(
                        src, qb.at[1, ph, pair, :, lanes], q_send.at[ph, i, g],
                        q_recv.at[1, place, ph], (to, y * 2 + g),
                    ))

    def start(one):
        one.start()

    def sent(one):
        one.wait_send()

    def project(ph):
        yy = (y + ph) % 2
        for i in range(2):
            at = slice(i * rows, (i + 1) * rows)
            xn[at, :] = modulate(xs[at, :] if ph == 0 else unit_rows(lat[yy * 2 + i]), 0)
        value = xn[...]
        at = column(yy)
        cos, sin = cos_ref[:, :, at], sin_ref[:, :, at]
        spot = row_spot(low)

        def keys():
            full = jnp.dot(value, wk[...], preferred_element_type=F32)
            for h in range(2):
                yh = full[:, h * head_dim : (h + 1) * head_dim]
                kk[h, at, :] = turn(unit(yh, kgain).T, cos, sin).T.astype(BF16)
            send_kv(ph, (0,), "early", start)
            send_kv(ph, (0,), "own", start)

        def values():
            full = jnp.dot(value, wv[...], preferred_element_type=F32)
            for h in range(2):
                vt[h, :, at] = full[:, h * head_dim : (h + 1) * head_dim].T.astype(BF16)
            send_kv(ph, (1,), "early", start)
            send_kv(ph, (1,), "own", start)

            @pl.when(local)
            def _():
                kb[quad, ph, spot] = kk[x, at]
                vb[quad, ph, :, spot] = vt[x, :, at]

        def queries():
            for h in range(4):
                if h % 2 == 0:
                    full = jnp.dot(
                        value, wq[:, h * head_dim : (h + 2) * head_dim], preferred_element_type=F32
                    )
                yh = full[:, (h % 2) * head_dim : (h % 2 + 1) * head_dim]
                qt[h, :, at] = turn(unit(yh, qgain).T, cos, sin).astype(BF16)
            send_q(ph, start)
            pair, lanes = spot_of(place)

            @pl.when(owner)
            def _():
                qb[1, ph, pair, :, lanes] = qt[x * 2 + c, :, at]
                qb[0, ph, pair, :, lanes] = qt[x * 2 + 1 - c, :, at]

        if ph == 1:
            queries()
            take_mate(0)
        keys()
        values()
        if ph == 0:
            queries()
        send_kv(ph, (0, 1), "late", start)

    def take_q(ph):
        for j in range(1, 4):
            m = (place + j) % 4
            pair, lanes = spot_of(m)
            ref = qb.at[1, ph, pair, :, lanes]
            remote(ref, ref, relay_send.at[0, 0], q_recv.at[1, m, ph], (s, partner)).wait_recv()
            one = remote(
                ref, qb.at[0, ph, pair, :, lanes], relay_send.at[j, ph], q_recv.at[0, m, ph],
                (s, partner),
            )
            one.start()
            sends.append(one)

    def have_q(ph):
        for j in range(4):
            m = (place + j) % 4
            pair, lanes = spot_of(m)
            for role in range(2) if j == 0 else range(1):
                ref = qb.at[role, ph, pair, :, lanes]
                one = remote(ref, ref, relay_send.at[0, 0], q_recv.at[role, m, ph], (s, partner))
                if j == 0:
                    pl.when(jnp.logical_not(owner))(one.wait_recv)
                else:
                    one.wait_recv()

    def wait_kv(zz, ph):
        spot = row_spot(zz % 2)
        for kind, ref in ((0, kb.at[zz // 2, ph, spot]), (1, vb.at[zz // 2, ph, :, spot])):
            remote(ref, ref, kv_send.at[0, 0, 0, 0], kv_recv.at[kind, ph, zz], (s, partner)).wait_recv()

    def have_kv(goal, ph):
        for lo in range(2):
            wait_kv(goal * 2 + lo, ph)

    mate = quad * 2 + 1 - low
    inner = functools.reduce(jnp.logical_or, [free(n) for n in range(1, quads)], low < 0)

    def take_mate(ph):
        @pl.when(inner)
        def _():
            wait_kv(mate, ph)

        pass_on(ph, start)

    def have_own(ph):
        @pl.when(jnp.logical_not(inner))
        def _():
            wait_kv(mate, ph)

        @pl.when(jnp.logical_not(local))
        def _():
            wait_kv(z, ph)

    local = owner & (target == c)
    stat[...] = jnp.concatenate(
        [jnp.full(stat.shape[:3] + (1, all_rows), -1e30, F32), jnp.zeros(stat.shape[:3] + (1, all_rows), F32)],
        axis=3,
    )
    acc[...] = jnp.zeros_like(acc)
    for one in loads[2:5] + loads[6:]:
        one.wait()
    project(0)
    relay_rows(0)
    for n in range(1, quads):
        ref = ctx.at[(quad + n) % quads, mine]
        remote(ref, ref, raw_send.at[0, 0], raw_recv.at[0, (quad + n) % quads], (s, partner)).wait_recv()
        one = remote(ref, ref, raw_send.at[1, n], raw_recv.at[1, (quad + n) % quads], (s, partner))
        one.start()
        sends.append(one)
    relay_rows(1)
    relay_rows(2)
    other = (1 - y) * 2 + 1 - c
    for i, at in enumerate(pieces):
        ref = lat.at[other, at]
        remote(ref, ref, lat_send.at[0], lat_recv.at[3 + i], (s, partner)).wait_recv()
    project(1)

    def sweep(ph, blocks, send=False):
        tiles = [(block, n) for block in blocks for n in range(4)]

        def stage_a(i):
            (keys, _, _), n = tiles[i]
            count = keys().shape[0]
            score[i % 2, :count] = jnp.dot(keys(), qb[n // 2, ph, n % 2], preferred_element_type=F32)

        def stage_b(i):
            (keys, _, bias), n = tiles[i]
            count = keys().shape[0]
            sc = score[i % 2, :count]
            old = stat[ph, n // 2, n % 2, 0:1]
            new = jnp.maximum(old, jnp.max(sc, axis=0, keepdims=True) + bias)
            f = jnp.exp2(old - new)
            fade[i % 2] = f
            p = jnp.exp2(sc - (new - bias))
            stat[ph, n // 2, n % 2, 1:2] = (
                stat[ph, n // 2, n % 2, 1:2] * f + jnp.sum(p, axis=0, keepdims=True)
            )
            stat[ph, n // 2, n % 2, 0:1] = new
            prob[i % 2, :count] = p.astype(BF16)

        def stage_c(i):
            (keys, values, _), n = tiles[i]
            count = keys().shape[0]
            value = jnp.dot(values(), prob[i % 2, :count], preferred_element_type=F32)
            acc[ph, n // 2, n % 2] = acc[ph, n // 2, n % 2] * fade[i % 2] + value

        for i in range(len(tiles) + 2):
            if i < len(tiles):
                stage_a(i)
            if 1 <= i <= len(tiles):
                stage_b(i - 1)
            if i >= 2:
                stage_c(i - 2)
            if send and i == len(tiles) - 1:
                for one in give(ph):
                    one.start()

    def latent(goal, late):
        return (lambda: kb[goal, late], lambda: vb[goal, late], 0.0)

    def give(ph):
        return [
            remote(acc.at[ph, 0], acc_in.at[ph], a_send.at[ph], a_recv.at[ph], (s, partner)),
            remote(stat.at[ph, 0], stat_in.at[ph], s_send.at[ph], s_recv.at[ph], (s, partner)),
        ]

    def prefix():
        for n in range(1, quads):
            ref = ctx.at[(quad + n) % quads, yours]
            remote(ref, ref, raw_send.at[0, 0], raw_recv.at[1, (quad + n) % quads], (s, partner)).wait_recv()
        cn = jnp.concatenate([modulate(unit_rows(ctx[n]), 1) for n in range(quads)], axis=0)
        kc = jnp.dot(cn, wk[...], preferred_element_type=F32)
        vc = jnp.dot(cn, wv[...], preferred_element_type=F32)
        for h in range(2):
            ckv[h, 0] = unit(kc[:, h * head_dim : (h + 1) * head_dim], kgain).astype(BF16)
            ckv[h, 1] = vc[:, h * head_dim : (h + 1) * head_dim].astype(BF16)
        send_ctx(start)

        @pl.when(local)
        def _():
            cb[low] = ckv[x]

    def have_ctx():
        for lo in range(2):

            @pl.when(jnp.logical_not(local & (lo == low)))
            def _():
                remote(cb.at[lo], cb.at[lo], c_send.at[0], c_recv.at[lo], (s, partner)).wait_recv()

    def sweeps(ph, late, begin, end, wait):
        def one(j, carry):
            goal = (quad + j) % quads
            if wait:

                @pl.when(j > 0)
                def _():
                    have_kv(goal, late)

            sweep(ph, [latent(goal, late)])
            return carry

        if end - begin == 1:
            one(begin, 0)
        elif end > begin:
            lax.fori_loop(begin, end, one, 0)

    def return_o(m, ph, cc, act):
        to = (quad * 2 + m // 2) * 2 + m % 2
        at = pl.ds(pl.multiple_of(((y + ph) % 2 * 2 + cc) * rows, rows), rows)
        mine = pl.ds(cc * rows, rows)
        head = pl.ds(pl.multiple_of((x * 2 + c) * head_dim, head_dim), head_dim)
        here = (to == s) & owner

        @pl.when(jnp.logical_not(here))
        def _():
            act(remote(
                ob.at[m, ph, mine], att.at[at, head], kv_send.at[m // 2, m % 2, ph, cc],
                o_recv.at[x * 2 + c, ph, cc], (to, y * 2 + low),
            ))

        if act is start:

            @pl.when(here)
            def _():
                att[at, head] = ob[m, ph, mine]

    def merge(ph):
        for one in give(ph):
            one.wait_recv()
        for cc in range(2):
            for j in range(4):
                m = (place + 3 - j) % 4
                pair, half = m // 2, m % 2
                lanes = pl.ds(pl.multiple_of(half * span + cc * rows, rows), rows)
                a, b = stat[ph, 1, pair, 0:1, lanes], stat_in[ph, pair, 0:1, lanes]
                peak = jnp.maximum(a, b)
                wa, wb = jnp.exp2(a - peak), jnp.exp2(b - peak)
                den = 1.0 / (stat[ph, 1, pair, 1:2, lanes] * wa + stat_in[ph, pair, 1:2, lanes] * wb)
                done = acc[ph, 1, pair, :, lanes] * (wa * den) + acc_in[ph, pair, :, lanes] * (wb * den)
                ob[m, ph, cc * rows : (cc + 1) * rows] = done.T.astype(BF16)
            for m in (3 - place, (place + 2) % 4, place + 1 - 2 * x, place):
                return_o(m, ph, cc, start)

    step_cols = width // chunks

    def piece(n, yy, cc):
        at = pl.ds(pl.multiple_of((yy * 2 + cc) * rows, rows), rows)
        return jnp.dot(
            att[at, :], wo[:, n * step_cols : (n + 1) * step_cols], preferred_element_type=F32
        )

    cores = [
        [
            remote(core_out.at[h, n], core_in.at[h, n], q_send.at[h, n // 2, n % 2], core_recv.at[h, n], (s, partner))
            for n in range(chunks)
        ]
        for h in range(2)
    ]
    mesh = [
        remote(mesh_out.at[n], mesh_in.at[n], mesh_send.at[n], mesh_recv.at[n], (s, across))
        for n in range(chunks)
    ]

    def have_o(ph, cc):
        at = pl.ds(pl.multiple_of(((y + ph) % 2 * 2 + cc) * rows, rows), rows)
        for i in range(2):
            for g in range(2):
                ref = att.at[at, pl.ds((i * 2 + g) * head_dim, head_dim)]
                one = remote(ref, ref, kv_send.at[0, 0, 0, 0], o_recv.at[i * 2 + g, ph, cc], (s, partner))
                pl.when(jnp.logical_not(owner & (x == i) & (g == c)))(one.wait_recv)

    def mix(ph):
        yy = (y + ph) % 2

        def give_core(cc, n):
            core_out[ph, n] = piece(n, yy, cc).astype(BF16)
            cores[ph][n].start()

        def take_core(n, value):
            cores[ph][n].wait_recv()
            value = value + core_in[ph, n].astype(F32)
            if ph == 1:
                mesh_out[n] = value.astype(BF16)
                mesh[n].start()
            else:
                mixed[n] = value

        have_o(ph, 0)

        @pl.when(c == 1)
        def _():
            for n in range(chunks):
                give_core(0, n)
            have_o(ph, 1)
            for n in range(chunks):
                take_core(n, piece(n, yy, 1))

        @pl.when(c == 0)
        def _():
            for n in range(chunks):
                mixed[n] = piece(n, yy, 0)
            have_o(ph, 1)
            for n in range(chunks):
                give_core(1, n)
                take_core(n, mixed[n])

    take_q(0)
    prefix()
    have_q(0)
    have_own(0)
    sweeps(0, 0, 0, 1, False)
    sweeps(0, 0, 1, quads, True)
    take_q(1)
    have_q(1)
    take_mate(1)
    sweep(1, [latent((quad + n) % quads, 0) for n in range(quads)])
    have_own(1)
    sweep(1, [latent(quad, 1)])
    have_ctx()
    ctx_keys = jnp.concatenate([cb[k, 0] for k in range(2)], axis=0)
    ctx_values = jnp.concatenate([cb[k, 1] for k in range(2)], axis=0)
    ctx_values = ctx_values.astype(F32).T.astype(BF16)
    ctx_block = (lambda: ctx_keys, lambda: ctx_values, lift * math.log2(math.e))
    others = [(quad + n) % quads for n in range(1, quads)]
    for goal in others:
        have_kv(goal, 1)
    sweep(1, [ctx_block] + [latent(goal, 1) for goal in others], send=True)
    for ph in range(2):
        send_kv(ph, (0, 1), "all", sent)
        send_q(ph, sent)
    merge(1)
    sweep(0, [latent(quad, 1), ctx_block])
    mix(1)
    sweep(0, [latent(goal, 1) for goal in others], send=True)
    merge(0)
    mix(0)
    square = jnp.zeros((rows, 1), F32)
    for n in range(chunks):
        mesh[n].wait_recv()
        value = mixed[n] + mesh_in[n].astype(F32)
        mixed[n] = value
        square = square + jnp.sum(value * value, axis=-1, keepdims=True)
    inv = lax.rsqrt(square / width + NORM_EPS)
    for n in range(chunks):
        at = slice(n * step_cols, (n + 1) * step_cols)
        gate = mod[0:1, 2 * width + n * step_cols : 2 * width + (n + 1) * step_cols]
        out_ref[:, at] = (lat[t, :, at].astype(F32) + gate * (mixed[n] * inv)).astype(BF16)

    for one in sends + give(0) + give(1) + cores[0] + cores[1] + mesh:
        one.wait_send()
    for ph in range(2):
        pass_on(ph, sent)
        for m in range(4):
            for cc in range(2):
                return_o(m, ph, cc, sent)
    send_ctx(sent)


def mix_kernel(
    tp_count, chunks,
    att_ref, wo_hbm, wo_ref, wo_sem, lat_ref, gate_ref,
    out_ref,
    core_out, core_in, mesh_out, mesh_in, mixed, core_send, core_recv, mesh_send, mesh_recv,
):
    s, t = lax.axis_index("sp"), lax.axis_index("tp")
    y, c = t // 2, t % 2
    y_count = tp_count // 2
    partner = y * 2 + 1 - c
    rows, width = lat_ref.shape
    step = width // chunks
    peers = [((y + j) % y_count) * 2 + c for j in range(1, y_count)]
    pltpu.make_async_copy(wo_hbm, wo_ref, wo_sem.at[0]).wait()

    def piece(n, j, cc):
        yy = (y + j) % y_count
        at = pl.ds(pl.multiple_of((yy * 2 + cc) * rows, rows), rows)
        return jnp.dot(
            att_ref[at, :], wo_ref[:, n * step : (n + 1) * step], preferred_element_type=F32
        )

    order = list(range(1, y_count)) + [0]
    cores = [
        remote(core_out.at[n], core_in.at[n], core_send.at[n], core_recv.at[n], (s, partner))
        for n in range(chunks)
    ]
    sent = []
    for n in range(chunks + 1):
        if n < chunks:
            for j in order:
                core_out[n, j] = piece(n, j, 1 - c).astype(BF16)
            cores[n].start()
        if n == 0:
            continue
        m = n - 1
        own = [piece(m, j, c) for j in order]
        cores[m].wait_recv()
        for j, value in zip(order, own):
            value = value + core_in[m, j].astype(F32)
            if j == 0:
                mixed[m] = value
            else:
                mesh_out[m, j - 1] = value.astype(BF16)
                one = remote(
                    mesh_out.at[m, j - 1], mesh_in.at[m, j - 1], mesh_send.at[m, j - 1],
                    mesh_recv.at[m, j - 1], (s, peers[j - 1]),
                )
                one.start()
                sent.append(one)
    for one in sent:
        one.wait_recv()
    square = jnp.zeros((rows, 1), F32)
    for n in range(chunks):
        value = mixed[n]
        for j in range(1, y_count):
            value = value + mesh_in[n, j - 1].astype(F32)
        mixed[n] = value
        square = square + jnp.sum(value * value, axis=-1, keepdims=True)
    inv = lax.rsqrt(square / width + NORM_EPS)
    for n in range(chunks):
        at = slice(n * step, (n + 1) * step)
        out_ref[:, at] = (
            lat_ref[:, at].astype(F32) + gate_ref[:, at] * (mixed[n] * inv)
        ).astype(BF16)
    for one in sent + cores:
        one.wait_send()


def whole_kernel(sp_count, tp_count, x_count, head_dim, group, lift, chunks, counts, *refs):
    (
        cond, cond_1, mw, lat, ctx, wq, wk, wv, qg, kg, cos, sin, wo, lat_rows,
        out, qt, k, vt, ckv, gate, att, wo_vm, wo_sem, *rest,
    ) = refs
    front, middle, last = counts
    front_scratch, middle_scratch = rest[:front], rest[front : front + middle]
    front_kernel(
        sp_count, tp_count, head_dim, cond, cond_1, mw, lat, ctx, wq, wk, wv, qg, kg, cos, sin,
        qt, k, vt, ckv, gate, *front_scratch, wo, wo_vm, wo_sem,
    )
    attend_kernel(sp_count, x_count, group, lift, k, vt, ckv, qt, att, *middle_scratch)
    mix_kernel(
        tp_count, chunks, att, wo, wo_vm, wo_sem, lat_rows, gate, out, *rest[front + middle :]
    )


ANY = pl.BlockSpec(memory_space=pl.ANY)
VM = pl.BlockSpec(memory_space=pltpu.VMEM)
DMA = pltpu.SemaphoreType.DMA


def grid_tables(sp_count, all_rows, head_dim):
    quarter, lines, lane = head_dim // 4, all_rows // GRID_W, np.arange(128)
    inv_freq = np.float32(ROPE_BASE) ** (-np.arange(quarter, dtype=np.float32) / quarter)
    rows = np.arange(sp_count)[:, None] * lines + lane[None, :] % lines
    both = np.stack([rows, np.broadcast_to(lane % GRID_W, rows.shape)], axis=1).astype(np.float32)
    angles = (both[:, :, None, :] * inv_freq[None, None, :, None]).astype(np.float32)
    return jnp.asarray(np.cos(angles)), jnp.asarray(np.sin(angles))


def quad_call(args, out_weight, sp_count, head_dim, lift):
    mod_weight, latents, context, query_weight, key_matrix, value_matrix = args[2:8]
    rows, width = latents.shape
    ctx_rows = context.shape[0]
    mod_cols = mod_weight.shape[1]
    all_rows, z_count, quads, chunks = 4 * rows, sp_count // 2, sp_count // 4, 4
    step = width // chunks
    cos, sin = grid_tables(sp_count, all_rows, head_dim)
    block = max(all_rows, z_count * ctx_rows)
    scratch = [
        pltpu.VMEM(args[0].shape, F32),
        pltpu.VMEM(args[1].shape, F32),
        pltpu.VMEM(args[8].shape, F32),
        pltpu.VMEM(args[9].shape, F32),
        pltpu.VMEM(cos.shape[1:], F32),
        pltpu.VMEM(sin.shape[1:], F32),
        DMA((6,)),
        pltpu.VMEM(mod_weight.shape, F32),
        pltpu.VMEM((4, rows, width), BF16),
        pltpu.VMEM((quads, ctx_rows, width), BF16),
        pltpu.VMEM(query_weight.shape, BF16),
        pltpu.VMEM(key_matrix.shape, BF16),
        pltpu.VMEM(value_matrix.shape, BF16),
        pltpu.VMEM(out_weight.shape, BF16),
        pltpu.VMEM((2, head_dim // 4, all_rows), F32),
        pltpu.VMEM((2, head_dim // 4, all_rows), F32),
        pltpu.VMEM((sp_count, 2, mod_cols), F32),
        pltpu.VMEM((4, 2, mod_cols), F32),
        pltpu.VMEM((2, 4 * mod_cols), F32),
        pltpu.VMEM((2 * rows, width), BF16),
        pltpu.VMEM((2 * rows, width), F32),
        pltpu.VMEM((4, head_dim, all_rows), BF16),
        pltpu.VMEM((2, all_rows, head_dim), BF16),
        pltpu.VMEM((2, head_dim, all_rows), BF16),
        pltpu.VMEM((2, 2, quads * ctx_rows, head_dim), BF16),
        pltpu.VMEM((2, 2, 2, head_dim, all_rows), BF16),
        pltpu.VMEM((quads, 2, all_rows, head_dim), BF16),
        pltpu.VMEM((quads, 2, head_dim, all_rows), BF16),
        pltpu.VMEM((2, 2, quads * ctx_rows, head_dim), BF16),
        pltpu.VMEM((2, 2, 2, 2, all_rows), F32),
        pltpu.VMEM((2, 2, 2, head_dim, all_rows), F32),
        pltpu.VMEM((2, 2, 2, all_rows), F32),
        pltpu.VMEM((2, 2, head_dim, all_rows), F32),
        pltpu.VMEM((2, block, all_rows), F32),
        pltpu.VMEM((2, block, all_rows), BF16),
        pltpu.VMEM((2, 1, all_rows), F32),
        pltpu.VMEM((4, 2, 2 * rows, head_dim), BF16),
        pltpu.VMEM((all_rows, 4 * head_dim), BF16),
        pltpu.VMEM((2, chunks, rows, step), BF16),
        pltpu.VMEM((2, chunks, rows, step), BF16),
        pltpu.VMEM((chunks, rows, step), BF16),
        pltpu.VMEM((chunks, rows, step), BF16),
        pltpu.VMEM((chunks, rows, step), F32),
        DMA((7,)),
        DMA((7,)),
        DMA((7,)),
        DMA((sp_count,)),
        DMA((sp_count,)),
        DMA((4,)),
        DMA((4,)),
        DMA((2, 2, quads, 2)),
        DMA((2, 2, z_count)),
        DMA((2,)),
        DMA((2,)),
        DMA((2, 2, 2)),
        DMA((2, 4, 2)),
        DMA((4, 2)),
        DMA((4, quads)),
        DMA((2, quads)),
        DMA((2, quads)),
        DMA((2,)),
        DMA((2,)),
        DMA((2,)),
        DMA((2,)),
        DMA((4, 2, 2)),
        DMA((2, chunks)),
        DMA((chunks,)),
        DMA((chunks,)),
    ]
    out = pl.pallas_call(
        functools.partial(quad_kernel, sp_count, head_dim, lift, chunks),
        out_shape=pltpu.VMEM((rows, width), BF16),
        in_specs=[pl.BlockSpec(memory_space=pltpu.HBM)] * 13,
        out_specs=VM,
        scratch_shapes=scratch,
        compiler_params=pltpu.CompilerParams(
            collective_id=0, has_side_effects=True, vmem_limit_bytes=VMEM_BYTES - 2 * rows * width * 2
        ),
        name="quad",
    )(*args, cos, sin, out_weight)
    return out


def body(
    latents,
    context,
    cond,
    ctx_cond,
    mod_weight,
    query_weight,
    key_matrix,
    value_matrix,
    out_weight,
    query_gain,
    key_gain,
):
    sp_count, tp_count = lax.axis_size("sp"), lax.axis_size("tp")
    x_count = row_size(sp_count)
    rows, width = latents.shape
    ctx_rows = context.shape[0]
    head_dim = query_gain.shape[0]
    heads = query_weight.shape[1] // head_dim
    kv_heads = key_matrix.shape[1] // head_dim
    all_rows = rows * tp_count
    mod_cols = mod_weight.shape[1]
    lift = math.log(sp_count * all_rows / (2.0 * sp_count * ctx_rows))
    group = heads // kv_heads
    args = (
        cond[None], ctx_cond[None], mod_weight, latents, context, query_weight, key_matrix, value_matrix,
        query_gain[None], key_gain[None],
    )
    wide = all_rows % GRID_W == 0 and all_rows == rows * 4 and rows % 128 == 0
    if wide and kv_heads == 2 and group == 2 and x_count == 2 and sp_count % 4 == 0 and ctx_rows % 32 == 0:
        return quad_call(args, out_weight, sp_count, head_dim, lift)
    chunks = 4
    y_count = tp_count // 2
    step = width // chunks
    far = max(y_count - 1, 1)
    positions = lax.axis_index("sp") * all_rows + jnp.arange(all_rows, dtype=jnp.int32)
    cos, sin = tables(positions, head_dim)
    shared = [
        pltpu.VMEM((heads, head_dim, all_rows), BF16),
        pltpu.VMEM((kv_heads, all_rows, head_dim), BF16),
        pltpu.VMEM((kv_heads, head_dim, all_rows), BF16),
        pltpu.VMEM((kv_heads, 2, ctx_rows, head_dim), BF16),
        pltpu.VMEM((1, width), F32),
        pltpu.VMEM((all_rows, heads * head_dim), BF16),
        pltpu.VMEM(out_weight.shape, BF16),
        DMA((1,)),
    ]
    front = [
        pltpu.VMEM(mod_weight.shape, F32),
        pltpu.VMEM((tp_count, rows, width), BF16),
        pltpu.VMEM(query_weight.shape, BF16),
        pltpu.VMEM(key_matrix.shape, BF16),
        pltpu.VMEM(value_matrix.shape, BF16),
        pltpu.VMEM((sp_count, 2, mod_cols), F32),
        pltpu.VMEM((tp_count, 2, mod_cols), F32),
        pltpu.VMEM((2, mod_cols * tp_count), F32),
        pltpu.VMEM((2 * rows, width), BF16),
        DMA((5,)),
        DMA((tp_count,)),
        DMA((tp_count,)),
        DMA((sp_count,)),
        DMA((sp_count,)),
        DMA((tp_count,)),
        DMA((tp_count,)),
    ]
    middle = [
        pltpu.VMEM((sp_count, kv_heads, all_rows, head_dim), BF16),
        pltpu.VMEM((sp_count, kv_heads, head_dim, all_rows), BF16),
        pltpu.VMEM((sp_count, kv_heads, 2, ctx_rows, head_dim), BF16),
        pltpu.VMEM((heads, 1, all_rows), F32),
        pltpu.VMEM((heads, 1, all_rows), F32),
        pltpu.VMEM((heads, head_dim, all_rows), F32),
        DMA((3,)),
    ]
    middle += [DMA((3, sp_count, x_count + 1)), DMA((3, sp_count))]
    last = [
        pltpu.VMEM((chunks, y_count, rows, step), BF16),
        pltpu.VMEM((chunks, y_count, rows, step), BF16),
        pltpu.VMEM((chunks, far, rows, step), BF16),
        pltpu.VMEM((chunks, far, rows, step), BF16),
        pltpu.VMEM((chunks, rows, step), F32),
        DMA((chunks,)),
        DMA((chunks,)),
        DMA((chunks, far)),
        DMA((chunks, far)),
    ]
    counts = (len(front), len(middle), len(last))
    return pl.pallas_call(
        functools.partial(
            whole_kernel, sp_count, tp_count, x_count, head_dim, group, lift, chunks, counts
        ),
        out_shape=jax.ShapeDtypeStruct((rows, width), BF16),
        in_specs=[VM, VM, ANY, ANY, VM, ANY, ANY, ANY, VM, VM, VM, VM, ANY, VM],
        out_specs=VM,
        scratch_shapes=shared + front + middle + last,
        compiler_params=pltpu.CompilerParams(
            collective_id=0, has_side_effects=True, vmem_limit_bytes=VMEM_BYTES
        ),
        name="whole",
    )(
        *args, cos, sin, out_weight, latents,
    )


def solution(mesh):
    placed = (
        P(("sp", "tp"), None),
        P("sp", None),
        P("sp"),
        P("sp"),
        P("sp", "tp"),
        P(None, "tp"),
        P(None, "tp"),
        P(None, "tp"),
        P("tp", None),
        P(),
        P(),
    )
    return jax.shard_map(
        body, mesh=mesh, in_specs=placed, out_specs=P(("sp", "tp"), None), check_vma=False
    )
```

```python
import functools
import math

import jax
import jax.numpy as jnp
import numpy as np
from jax import lax
from jax.experimental import pallas as pl
from jax.experimental.pallas import tpu as pltpu
from jax.sharding import PartitionSpec as P

GRID_W = 64
NORM_EPS = 1e-06
ROPE_BASE = 10000.0
MESH = pl.DeviceIdType.MESH
BF16 = jnp.bfloat16
F32 = jnp.float32
VMEM_BYTES = 67043328


def row_size(sp_count):
    size = 1
    while 4 * size * size <= sp_count:
        size *= 2
    return size


def tables(positions, head_dim):
    quarter = head_dim // 4
    inv_freq = ROPE_BASE ** (-jnp.arange(quarter, dtype=F32) / quarter)
    where = jnp.stack([positions // GRID_W, positions % GRID_W]).astype(F32)
    angles = where[:, None, :] * inv_freq[None, :, None]
    return jnp.cos(angles), jnp.sin(angles)


def remote(src, dst, send, recv, dev):
    return pltpu.make_async_remote_copy(
        src_ref=src, dst_ref=dst, send_sem=send, recv_sem=recv, device_id=dev, device_id_type=MESH
    )


def front_kernel(
    sp_count, tp_count, head_dim,
    cond_ref, cond_1_ref, mw_hbm, lat_hbm, ctx_ref, wq_hbm, wk_hbm, wv_hbm, qg_ref, kg_ref, cos_ref, sin_ref,
    qt_ref, k_ref, vt_ref, ckv_ref, gate_ref,
    mw, lat, wq, wk, wv, part, tot, mod, xn, load_sem,
    lat_send, lat_recv, part_send, part_recv, tot_send, tot_recv,
    wo_hbm, wo_vm, wo_sem,
):
    s, t = lax.axis_index("sp"), lax.axis_index("tp")
    y, c = t // 2, t % 2
    y_count = tp_count // 2
    partner = y * 2 + 1 - c
    rows = lat.shape[1]
    width = lat.shape[2]
    model_cols = mod.shape[1]

    own = pltpu.make_async_copy(lat_hbm, lat.at[t], load_sem.at[0])
    own.start()
    loads = [
        pltpu.make_async_copy(a, b, load_sem.at[1 + i])
        for i, (a, b) in enumerate(((mw_hbm, mw), (wq_hbm, wq), (wk_hbm, wk), (wv_hbm, wv)))
    ]
    for one in loads:
        one.start()

    pltpu.make_async_copy(wo_hbm, wo_vm, wo_sem.at[0]).start()

    barrier = pltpu.get_barrier_semaphore()
    for j in range(1, sp_count):
        pl.semaphore_signal(barrier, inc=1, device_id=((s + j) % sp_count, t), device_id_type=MESH)
    for j in range(1, tp_count):
        pl.semaphore_signal(barrier, inc=1, device_id=(s, (t + j) % tp_count), device_id_type=MESH)
    pl.semaphore_wait(barrier, sp_count + tp_count - 2)

    own.wait()
    sends = []
    for j in range(1, y_count):
        peer = ((y + j) % y_count) * 2 + c
        sends.append(remote(lat.at[t], lat.at[t], lat_send.at[j], lat_recv.at[t], (s, peer)))
    sends.append(remote(lat.at[t], lat.at[t], lat_send.at[0], lat_recv.at[t], (s, partner)))
    for one in sends:
        one.start()

    loads[0].wait()
    lines = lax.broadcasted_iota(jnp.int32, (8, cond_ref.shape[1]), 0)
    cond = jnp.where(lines == 0, cond_ref[...], jnp.where(lines == 1, cond_1_ref[...], 0.0))
    cond = cond * jax.nn.sigmoid(cond)
    part[s] = jnp.dot(
        cond, mw[...], precision=lax.Precision.HIGHEST, preferred_element_type=F32
    )[:2]
    more = [
        remote(part.at[s], part.at[s], part_send.at[j], part_recv.at[s], ((s + j) % sp_count, t))
        for j in range(1, sp_count)
    ]
    for one in more:
        one.start()
    for j in range(1, sp_count):
        src = (s + j) % sp_count
        remote(part.at[src], part.at[src], part_send.at[0], part_recv.at[src], (s, t)).wait_recv()
    total = part[0]
    for j in range(1, sp_count):
        total = total + part[j]
    tot[t] = total
    last = [
        remote(tot.at[t], tot.at[t], tot_send.at[j], tot_recv.at[t], (s, (t + j) % tp_count))
        for j in range(1, tp_count)
    ]
    for one in last:
        one.start()
    for j in range(1, tp_count):
        src = (t + j) % tp_count
        remote(tot.at[src], tot.at[src], tot_send.at[0], tot_recv.at[src], (s, t)).wait_recv()
    cols = model_cols // tp_count
    for j in range(tp_count):
        mod[:, j * cols : (j + 1) * cols] = tot[j]
    gate_ref[...] = mod[0:1, 2 * width :]

    def modulate(x, r):
        x = x.astype(F32)
        scaled = x * lax.rsqrt(jnp.mean(x * x, axis=-1, keepdims=True) + NORM_EPS)
        shift, scale = mod[r : r + 1, :width], mod[r : r + 1, width : 2 * width]
        return (scaled * (1.0 + scale) + shift).astype(BF16)

    for one in loads[1:]:
        one.wait()

    cn = modulate(ctx_ref[...], 1)
    kc = jnp.dot(cn, wk[...], preferred_element_type=F32)
    vc = jnp.dot(cn, wv[...], preferred_element_type=F32)
    for h in range(kc.shape[1] // head_dim):
        kh = kc[:, h * head_dim : (h + 1) * head_dim]
        kh = kh * lax.rsqrt(jnp.mean(kh * kh, axis=-1, keepdims=True) + NORM_EPS) * kg_ref[...]
        ckv_ref[h, 0] = kh.astype(BF16)
        ckv_ref[h, 1] = vc[:, h * head_dim : (h + 1) * head_dim].astype(BF16)

    q4 = head_dim // 4
    qgain, kgain = qg_ref[...], kg_ref[...]

    def turn(yt, cos, sin):
        out = []
        for n in range(2):
            a = yt[2 * n * q4 : (2 * n + 1) * q4]
            b = yt[(2 * n + 1) * q4 : (2 * n + 2) * q4]
            out += [a * cos[n] - b * sin[n], b * cos[n] + a * sin[n]]
        return jnp.concatenate(out, axis=0)

    def unit(yh, gain):
        return yh * lax.rsqrt(jnp.mean(yh * yh, axis=-1, keepdims=True) + NORM_EPS) * gain

    span = 2 * rows
    relays = []
    for j in range(y_count):
        yy = (y + j) % y_count
        if j > 0:
            src = yy * 2 + c
            remote(lat.at[src], lat.at[src], lat_send.at[0], lat_recv.at[src], (s, t)).wait_recv()
            one = remote(
                lat.at[src], lat.at[src], lat_send.at[y_count - 1 + j], lat_recv.at[src], (s, partner)
            )
            one.start()
            relays.append(one)
        other = yy * 2 + 1 - c
        remote(lat.at[other], lat.at[other], lat_send.at[0], lat_recv.at[other], (s, t)).wait_recv()
        for i in range(2):
            xn[i * rows : (i + 1) * rows, :] = modulate(lat[yy * 2 + i], 0)
        x = xn[...]
        at = pl.ds(pl.multiple_of(yy * span, span), span)
        cos, sin = cos_ref[:, :, at], sin_ref[:, :, at]
        for w, kind in ((wq, 0), (wk, 1), (wv, 2)):
            step = min(2 * head_dim, w.shape[1])
            for n in range(0, w.shape[1], step):
                full = jnp.dot(x, w[:, n : n + step], preferred_element_type=F32)
                for m in range(0, step, head_dim):
                    h = (n + m) // head_dim
                    yh = full[:, m : m + head_dim]
                    if kind == 0:
                        qt_ref[h, :, at] = turn(unit(yh, qgain).T, cos, sin).astype(BF16)
                    elif kind == 1:
                        k_ref[h, at, :] = turn(unit(yh, kgain).T, cos, sin).T.astype(BF16)
                    else:
                        vt_ref[h, :, at] = yh.T.astype(BF16)
    for one in sends + more + last + relays:
        one.wait_send()


def attend_kernel(
    sp_count, x_count, group, lift,
    k_hbm, vt_hbm, ckv_hbm, qt_ref,
    out_ref,
    kb, vb, cb, top, tot, acc, load_sem, send_sem, recv_sem,
):
    s, t = lax.axis_index("sp"), lax.axis_index("tp")
    z, x = s // x_count, s % x_count
    z_count = sp_count // x_count
    heads, head_dim, rows = qt_ref.shape
    kv_heads = heads // group
    factor = head_dim ** (-0.5) * math.log2(math.e)

    loads = [
        pltpu.make_async_copy(a, b, load_sem.at[i])
        for i, (a, b) in enumerate(
            (
                (ckv_hbm, cb.at[s]),
                (k_hbm, kb.at[s]),
                (vt_hbm, vb.at[s]),
            )
        )
    ]
    for one in loads:
        one.start()
    targets = []
    for sign in (1, -1):
        ok = (z + sign >= 0) & (z + sign < z_count)
        peer = ((z + sign + z_count) % z_count) * x_count + x
        targets.append((ok, peer))

    top[...] = jnp.full_like(top, -1e30)
    tot[...] = jnp.zeros_like(tot)
    acc[...] = jnp.zeros_like(acc)
    for one in loads:
        one.wait()

    bufs = (cb, kb, vb)

    def copies(src, way, peer):
        return [
            remote(b.at[src], b.at[src], send_sem.at[i, src, way], recv_sem.at[i, src], (peer, t))
            for i, b in enumerate(bufs)
        ]

    def source(k):
        low = jnp.minimum(z, z_count - 1 - z)
        both = k <= 2 * low
        dist = jnp.where(both, (k + 1) // 2, k - low)
        up = jnp.where(both, k % 2 == 1, z < z_count - 1 - z)
        return jnp.where(up, z + dist, z - dist)

    def update(i, keys, values_t, bias):
        sc = jnp.dot(keys, qt_ref[i], preferred_element_type=F32) * factor
        if bias != 0.0:
            sc = sc + bias
        old = top[i]
        new = jnp.maximum(old, jnp.max(sc, axis=0, keepdims=True))
        p = jnp.exp2(sc - new)
        f = jnp.exp2(old - new)
        top[i] = new
        tot[i] = tot[i] * f + jnp.sum(p, axis=0, keepdims=True)
        acc[i] = acc[i] * f + jnp.dot(values_t, p.astype(BF16), preferred_element_type=F32)

    def block(src):
        def head(i, carry):
            h = i // group
            update(i, kb[src, h], vb[src, h], 0.0)
            return carry

        lax.fori_loop(0, heads, head, 0)

    def wait_from(src):
        for one in copies(src, 0, s):
            one.wait_recv()

    def step(k, carry):
        zz = source(k)
        src = zz * x_count + x

        @pl.when(k > 0)
        def _():
            wait_from(src)

        for way, (ok, peer) in enumerate(targets):
            mine = zz <= z if way == 0 else zz >= z

            @pl.when(ok & mine)
            def _():
                for one in copies(src, way, peer):
                    one.start()

        for j in range(1, x_count):
            for one in copies(src, 1 + j, z * x_count + (x + j) % x_count):
                one.start()
        block(src)

        @pl.when(k > 0)
        def _():
            before = source(k - 1)
            for j in range(1, x_count):
                old = before * x_count + (x + j) % x_count
                wait_from(old)
                block(old)

        return carry

    lax.fori_loop(0, z_count, step, 0)
    final = source(z_count - 1)
    ends = [final * x_count + (x + j) % x_count for j in range(1, x_count)]
    for src in ends:
        copies(src, 0, s)[0].wait_recv()
    for i in range(heads):
        h = i // group
        keys = jnp.concatenate([cb[j, h, 0] for j in range(sp_count)], axis=0)
        vals = jnp.concatenate([cb[j, h, 1] for j in range(sp_count)], axis=0)
        update(i, keys, vals.astype(F32).T.astype(BF16), lift * math.log2(math.e))
    for src in ends:
        for one in copies(src, 0, s)[1:]:
            one.wait_recv()
        block(src)
    for i in range(heads):
        out_ref[:, i * head_dim : (i + 1) * head_dim] = (acc[i] / tot[i]).T.astype(BF16)

    def drain(k, carry):
        zz = source(k)
        src = zz * x_count + x
        for way, (ok, peer) in enumerate(targets):
            mine = zz <= z if way == 0 else zz >= z

            @pl.when(ok & mine)
            def _():
                for one in copies(src, way, peer):
                    one.wait_send()

        for j in range(1, x_count):
            for one in copies(src, 1 + j, z * x_count + (x + j) % x_count):
                one.wait_send()
        return carry

    lax.fori_loop(0, z_count, drain, 0)


def quad_kernel(sp_count, head_dim, lift, chunks, *refs):
    (
        cond_hbm, cond_1_hbm, mw_hbm, lat_hbm, ctx_hbm, wq_hbm, wk_hbm, wv_hbm, qg_hbm, kg_hbm,
        cos_hbm, sin_hbm, wo_hbm,
        out_ref,
        cond_ref, cond_1_ref, qg_ref, kg_ref, cos_in, sin_in, small_sem,
        mw, lat, ctx, wq, wk, wv, wo, cos_ref, sin_ref, part, tot, mod, xn, xs,
        qt, kk, vt, ckv, qb, kb, vb, cb, stat, acc, stat_in, acc_in,
        score, prob, fade, ob, att, core_out, core_in, mesh_out, mesh_in, mixed,
        load_sem, lat_send, lat_recv, part_send, part_recv, tot_send, tot_recv,
        kv_send, kv_recv, c_send, c_recv, q_send, q_recv, relay_send, pass_send, raw_send, raw_recv,
        a_send, a_recv, s_send, s_recv, o_recv, core_recv, mesh_send, mesh_recv,
    ) = refs
    s, t = lax.axis_index("sp"), lax.axis_index("tp")
    y, c = t // 2, t % 2
    z, x = s // 2, s % 2
    z_count = sp_count // 2
    quads = z_count // 2
    quad, low = z // 2, z % 2
    place = low * 2 + x
    partner, across = y * 2 + 1 - c, (1 - y) * 2 + c
    target = (z + x) % 2
    owner = low == c
    rows, width = lat.shape[1], lat.shape[2]
    all_rows = 4 * rows
    span = 2 * rows
    cuts = (0, rows * 3 // 8 // 16 * 16, rows * 3 // 4 // 16 * 16, rows)

    load_pairs = (
        (mw_hbm, mw), (lat_hbm, lat.at[t]), (wk_hbm, wk), (wv_hbm, wv), (wq_hbm, wq), (ctx_hbm, ctx.at[quad]),
        (wo_hbm, wo),
    )
    loads = [pltpu.make_async_copy(a, b, load_sem.at[i]) for i, (a, b) in enumerate(load_pairs)]
    small_pairs = (
        (cond_hbm, cond_ref), (cond_1_hbm, cond_1_ref), (cos_hbm.at[s], cos_in), (sin_hbm.at[s], sin_in),
        (qg_hbm, qg_ref), (kg_hbm, kg_ref),
    )
    smalls = [pltpu.make_async_copy(a, b, small_sem.at[i]) for i, (a, b) in enumerate(small_pairs)]
    for one in smalls[:2] + loads[:1] + smalls[2:] + loads[1:2]:
        one.start()

    barrier = pltpu.get_barrier_semaphore()
    for j in range(sp_count):
        for k in range(2):
            if j + k > 0:
                dev = ((s + j) % sp_count, y * 2 + (c + k) % 2)
                pl.semaphore_signal(barrier, inc=1, device_id=dev, device_id_type=MESH)
    for k in range(2):
        dev = (s, (1 - y) * 2 + (c + k) % 2)
        pl.semaphore_signal(barrier, inc=1, device_id=dev, device_id_type=MESH)

    for one in smalls:
        one.wait()
    lines = lax.broadcasted_iota(jnp.int32, (8, cond_ref.shape[1]), 0)
    cond = jnp.where(lines == 0, cond_ref[...], jnp.where(lines == 1, cond_1_ref[...], 0.0))
    cond = (cond * jax.nn.sigmoid(cond)).T
    for small, table in ((cos_in, cos_ref), (sin_in, sin_ref)):
        for n in range(all_rows // 128):
            at = slice(n * 128, (n + 1) * 128)
            parts = [
                jnp.broadcast_to(small[0, :, r : r + 1], (small.shape[1], GRID_W))
                for r in range(n * 128 // GRID_W, (n + 1) * 128 // GRID_W)
            ]
            table[0, :, at] = jnp.concatenate(parts, axis=1)
            table[1, :, at] = small[1]
    loads[0].wait()
    for one in loads[2:]:
        one.start()
    for r in range(2):
        part[s, r : r + 1, :] = jnp.sum(mw[...] * cond[:, r : r + 1], axis=0, keepdims=True)
    loads[1].wait()
    pl.semaphore_wait(barrier, 2 * sp_count + 1)

    sends = [
        remote(part.at[s], part.at[s], part_send.at[j], part_recv.at[s], ((s + j) % sp_count, t))
        for j in range(1, sp_count)
    ]
    sends.append(remote(lat.at[t], lat.at[t], lat_send.at[6], lat_recv.at[6], (s, partner)))
    pieces = [pl.ds(a, b - a) for a, b in zip(cuts, cuts[1:])]
    halves = [
        remote(lat.at[t, at], lat.at[t, at], lat_send.at[i], lat_recv.at[i], (s, across))
        for i, at in enumerate(pieces)
    ]
    for one in sends + halves[:1]:
        one.start()
    def unit_rows(value):
        value = value.astype(F32)
        return value * lax.rsqrt(jnp.mean(value * value, axis=-1, keepdims=True) + NORM_EPS)

    remote(lat.at[partner], lat.at[partner], lat_send.at[0], lat_recv.at[6], (s, partner)).wait_recv()
    for i in range(2):
        xs[i * rows : (i + 1) * rows, :] = unit_rows(lat[y * 2 + i])
    for j in range(1, sp_count):
        src = (s + j) % sp_count
        remote(part.at[src], part.at[src], part_send.at[0], part_recv.at[src], (s, partner)).wait_recv()
    total = part[0]
    for j in range(1, sp_count):
        total = total + part[j]
    tot[t] = total
    last = [
        remote(tot.at[t], tot.at[t], tot_send.at[j], tot_recv.at[t], (s, (t + j) % 4))
        for j in range(1, 4)
    ]
    ctx_rows = ctx.shape[1]
    half = ctx_rows // 2
    mine = pl.ds(pl.multiple_of(c * half, half), half)
    yours = pl.ds(pl.multiple_of((1 - c) * half, half), half)
    loads[5].wait()
    raw = [
        remote(
            ctx.at[quad, mine], ctx.at[quad, mine], raw_send.at[0, n], raw_recv.at[0, quad],
            ((((quad + n) % quads) * 2 + low) * 2 + x, t),
        )
        for n in range(1, quads)
    ]
    for one in last + halves[1:] + raw:
        one.start()
    sends += last + halves + raw
    for j in range(1, 4):
        src = (t + j) % 4
        remote(tot.at[src], tot.at[src], tot_send.at[0], tot_recv.at[src], (s, partner)).wait_recv()
    cols = tot.shape[2]
    for j in range(4):
        mod[:, j * cols : (j + 1) * cols] = tot[j]

    def relay_rows(i):
        at = pieces[i]
        remote(lat.at[across, at], lat.at[across, at], lat_send.at[0], lat_recv.at[i], (s, partner)).wait_recv()
        one = remote(
            lat.at[across, at], lat.at[across, at], lat_send.at[3 + i], lat_recv.at[3 + i], (s, partner)
        )
        one.start()
        sends.append(one)

    def modulate(scaled, r):
        shift, scale = mod[r : r + 1, :width], mod[r : r + 1, width : 2 * width]
        return (scaled * (1.0 + scale) + shift).astype(BF16)

    q4 = head_dim // 4
    qgain = qg_ref[...] * (head_dim ** (-0.5) * math.log2(math.e))
    kgain = kg_ref[...]

    def turn(yt, cos, sin):
        out = []
        for n in range(2):
            a = yt[2 * n * q4 : (2 * n + 1) * q4]
            b = yt[(2 * n + 1) * q4 : (2 * n + 2) * q4]
            out += [a * cos[n] - b * sin[n], b * cos[n] + a * sin[n]]
        return jnp.concatenate(out, axis=0)

    def unit(yh, gain):
        return yh * lax.rsqrt(jnp.mean(yh * yh, axis=-1, keepdims=True) + NORM_EPS) * gain

    def column(yy):
        return pl.ds(pl.multiple_of(yy * span, span), span)

    def dest(i, n):
        to = (((quad + n) % quads) * 2 + c) * 2 + i
        here = (to == s) & (target == c)
        return to, here

    def free(n):
        return (low == 1) == ((quad + n) % quads > quad)

    def row_spot(lo):
        return pl.ds(pl.multiple_of(lo * span, span), span)

    def allowed(n, which):
        if n == 0:
            return which in ("own", "all")
        if which == "own":
            return False
        straight = {"early": free(n), "late": jnp.logical_not(free(n)) & (c == low)}
        return straight[which] if which in straight else free(n) | (c == low)

    def send_kv(ph, kinds, which, act):
        at, spot = column((y + ph) % 2), row_spot(low)
        for n in range(quads):
            ok = allowed(n, which)
            if ok is False:
                continue
            for i in range(2):
                to, here = dest(i, n)
                for kind in kinds:
                    src, dst = (
                        (kk.at[i, at], kb.at[quad, ph, spot]),
                        (vt.at[i, :, at], vb.at[quad, ph, :, spot]),
                    )[kind]

                    @pl.when(jnp.logical_not(here) & ok)
                    def _():
                        act(remote(
                            src, dst, kv_send.at[kind, ph, n, i], kv_recv.at[kind, ph, z],
                            (to, y * 2 + target),
                        ))

    def send_ctx(act):
        for i in range(2):
            to, here = dest(i, 0)

            @pl.when(jnp.logical_not(here))
            def _():
                act(remote(ckv.at[i], cb.at[low], c_send.at[i], c_recv.at[low], (to, y * 2 + target)))

    def pass_on(ph, act):
        spot = row_spot(1 - low)
        for n in range(1, quads):
            to = (((quad + n) % quads) * 2 + low) * 2 + x
            copies = [
                remote(ref, ref, pass_send.at[2 * ph + kind, n], kv_recv.at[kind, ph, mate], (to, t))
                for kind, ref in ((0, kb.at[quad, ph, spot]), (1, vb.at[quad, ph, :, spot]))
            ]

            @pl.when(free(n))
            def _():
                for one in copies:
                    act(one)

    def spot_of(m):
        return pl.ds(pl.multiple_of(m * rows, rows), rows)

    def send_q(ph, act):
        blocks = pl.ds((y + ph) % 2 * 2, 2)
        lanes = spot_of(place)
        for i in range(2):
            to = (quad * 2 + c) * 2 + i
            for g in range(2):
                mine = (to == s) & (g == c)
                src = qt.at[i * 2 + g, blocks]

                @pl.when(mine)
                def _():
                    act(remote(
                        src, qb.at[0, ph, :, :, lanes], q_send.at[ph, i, g],
                        q_recv.at[0, place, ph], (s, partner),
                    ))

                @pl.when(jnp.logical_not(mine))
                def _():
                    act(remote(
                        src, qb.at[1, ph, :, :, lanes], q_send.at[ph, i, g],
                        q_recv.at[1, place, ph], (to, y * 2 + g),
                    ))

    def start(one):
        one.start()

    def sent(one):
        one.wait_send()

    def project(ph):
        yy = (y + ph) % 2
        for i in range(2):
            at = slice(i * rows, (i + 1) * rows)
            xn[at, :] = modulate(xs[at, :] if ph == 0 else unit_rows(lat[yy * 2 + i]), 0)
        value = xn[...]
        at = column(yy)
        cos, sin = cos_ref[:, :, at], sin_ref[:, :, at]
        spot = row_spot(low)

        def keys():
            full = jnp.dot(value, wk[...], preferred_element_type=F32)
            for h in range(2):
                yh = full[:, h * head_dim : (h + 1) * head_dim]
                kk[h, at, :] = turn(unit(yh, kgain).T, cos, sin).T.astype(BF16)
            send_kv(ph, (0,), "early", start)
            send_kv(ph, (0,), "own", start)

        def values():
            full = jnp.dot(value, wv[...], preferred_element_type=F32)
            for h in range(2):
                vt[h, :, at] = full[:, h * head_dim : (h + 1) * head_dim].T.astype(BF16)
            send_kv(ph, (1,), "early", start)
            send_kv(ph, (1,), "own", start)

            @pl.when(local)
            def _():
                kb[quad, ph, spot] = kk[x, at]
                vb[quad, ph, :, spot] = vt[x, :, at]

        def queries():
            for h in range(4):
                if h % 2 == 0:
                    full = jnp.dot(
                        value, wq[:, h * head_dim : (h + 2) * head_dim], preferred_element_type=F32
                    )
                yh = full[:, (h % 2) * head_dim : (h % 2 + 1) * head_dim]
                turned = turn(unit(yh, qgain).T, cos, sin).astype(BF16)
                for cc in range(2):
                    qt[h, yy * 2 + cc] = turned[:, cc * rows : (cc + 1) * rows]
            send_q(ph, start)
            lanes = spot_of(place)

            @pl.when(owner)
            def _():
                for cc in range(2):
                    qb[1, ph, cc, :, lanes] = qt[x * 2 + c, yy * 2 + cc]
                    qb[0, ph, cc, :, lanes] = qt[x * 2 + 1 - c, yy * 2 + cc]

        if ph == 1:
            queries()
            take_mate(0)
        keys()
        values()
        if ph == 0:
            queries()
        send_kv(ph, (0, 1), "late", start)

    def take_q(ph):
        for j in range(1, 4):
            m = (place + j) % 4
            lanes = spot_of(m)
            ref = qb.at[1, ph, :, :, lanes]
            remote(ref, ref, relay_send.at[0, 0], q_recv.at[1, m, ph], (s, partner)).wait_recv()
            one = remote(
                ref, qb.at[0, ph, :, :, lanes], relay_send.at[j, ph], q_recv.at[0, m, ph],
                (s, partner),
            )
            one.start()
            sends.append(one)

    def have_q(ph):
        for j in range(4):
            m = (place + j) % 4
            lanes = spot_of(m)
            for role in range(2) if j == 0 else range(1):
                ref = qb.at[role, ph, :, :, lanes]
                one = remote(ref, ref, relay_send.at[0, 0], q_recv.at[role, m, ph], (s, partner))
                if j == 0:
                    pl.when(jnp.logical_not(owner))(one.wait_recv)
                else:
                    one.wait_recv()

    def wait_kv(zz, ph):
        spot = row_spot(zz % 2)
        for kind, ref in ((0, kb.at[zz // 2, ph, spot]), (1, vb.at[zz // 2, ph, :, spot])):
            remote(ref, ref, kv_send.at[0, 0, 0, 0], kv_recv.at[kind, ph, zz], (s, partner)).wait_recv()

    def have_kv(goal, ph):
        for lo in range(2):
            wait_kv(goal * 2 + lo, ph)

    mate = quad * 2 + 1 - low
    inner = functools.reduce(jnp.logical_or, [free(n) for n in range(1, quads)], low < 0)

    def take_mate(ph):
        @pl.when(inner)
        def _():
            wait_kv(mate, ph)

        pass_on(ph, start)

    def have_own(ph):
        @pl.when(jnp.logical_not(inner))
        def _():
            wait_kv(mate, ph)

        @pl.when(jnp.logical_not(local))
        def _():
            wait_kv(z, ph)

    local = owner & (target == c)
    stat[...] = jnp.concatenate(
        [jnp.full(stat.shape[:3] + (1, all_rows), -1e30, F32), jnp.zeros(stat.shape[:3] + (1, all_rows), F32)],
        axis=3,
    )
    acc[...] = jnp.zeros_like(acc)
    for one in loads[2:5] + loads[6:]:
        one.wait()
    project(0)
    relay_rows(0)
    for n in range(1, quads):
        ref = ctx.at[(quad + n) % quads, mine]
        remote(ref, ref, raw_send.at[0, 0], raw_recv.at[0, (quad + n) % quads], (s, partner)).wait_recv()
        one = remote(ref, ref, raw_send.at[1, n], raw_recv.at[1, (quad + n) % quads], (s, partner))
        one.start()
        sends.append(one)
    relay_rows(1)
    relay_rows(2)
    other = (1 - y) * 2 + 1 - c
    for i, at in enumerate(pieces):
        ref = lat.at[other, at]
        remote(ref, ref, lat_send.at[0], lat_recv.at[3 + i], (s, partner)).wait_recv()
    project(1)

    def sweep(ph, blocks, send=False):
        tiles = [(block, n) for block in blocks for n in range(4)]

        def stage_a(i):
            (keys, _, _), n = tiles[i]
            count = keys().shape[0]
            score[i % 2, :count] = jnp.dot(keys(), qb[n % 2, ph, n // 2], preferred_element_type=F32)

        def stage_b(i):
            (keys, _, bias), n = tiles[i]
            count = keys().shape[0]
            sc = score[i % 2, :count]
            old = stat[ph, n % 2, n // 2, 0:1]
            new = jnp.maximum(old, jnp.max(sc, axis=0, keepdims=True) + bias)
            f = jnp.exp2(old - new)
            fade[i % 2] = f
            p = jnp.exp2(sc - (new - bias))
            stat[ph, n % 2, n // 2, 1:2] = (
                stat[ph, n % 2, n // 2, 1:2] * f + jnp.sum(p, axis=0, keepdims=True)
            )
            stat[ph, n % 2, n // 2, 0:1] = new
            prob[i % 2, :count] = p.astype(BF16)

        def stage_c(i):
            (keys, values, _), n = tiles[i]
            count = keys().shape[0]
            value = jnp.dot(values(), prob[i % 2, :count], preferred_element_type=F32)
            acc[ph, n % 2, n // 2] = acc[ph, n % 2, n // 2] * fade[i % 2] + value

        for i in range(len(tiles) + 2):
            if i < len(tiles):
                stage_a(i)
            if 1 <= i <= len(tiles):
                stage_b(i - 1)
            if i >= 2:
                stage_c(i - 2)
            if send and i >= len(tiles) - 2 and (len(tiles) - i) % 2 == 0:
                for one in give(ph, 0 if i < len(tiles) else 1):
                    one.start()

    def latent(goal, late):
        return (lambda: kb[goal, late], lambda: vb[goal, late], 0.0)

    def give(ph, cc):
        return [
            remote(acc.at[ph, 0, cc], acc_in.at[ph, cc], a_send.at[ph, cc], a_recv.at[ph, cc], (s, partner)),
            remote(stat.at[ph, 0, cc], stat_in.at[ph, cc], s_send.at[ph, cc], s_recv.at[ph, cc], (s, partner)),
        ]

    def prefix():
        for n in range(1, quads):
            ref = ctx.at[(quad + n) % quads, yours]
            remote(ref, ref, raw_send.at[0, 0], raw_recv.at[1, (quad + n) % quads], (s, partner)).wait_recv()
        cn = jnp.concatenate([modulate(unit_rows(ctx[n]), 1) for n in range(quads)], axis=0)
        kc = jnp.dot(cn, wk[...], preferred_element_type=F32)
        vc = jnp.dot(cn, wv[...], preferred_element_type=F32)
        for h in range(2):
            ckv[h, 0] = unit(kc[:, h * head_dim : (h + 1) * head_dim], kgain).astype(BF16)
            ckv[h, 1] = vc[:, h * head_dim : (h + 1) * head_dim].astype(BF16)
        send_ctx(start)

        @pl.when(local)
        def _():
            cb[low] = ckv[x]

    def have_ctx():
        for lo in range(2):

            @pl.when(jnp.logical_not(local & (lo == low)))
            def _():
                remote(cb.at[lo], cb.at[lo], c_send.at[0], c_recv.at[lo], (s, partner)).wait_recv()

    def sweeps(ph, late, begin, end, wait):
        def one(j, carry):
            goal = (quad + j) % quads
            if wait:

                @pl.when(j > 0)
                def _():
                    have_kv(goal, late)

            sweep(ph, [latent(goal, late)])
            return carry

        if end - begin == 1:
            one(begin, 0)
        elif end > begin:
            lax.fori_loop(begin, end, one, 0)

    def return_o(m, ph, cc, act):
        to = (quad * 2 + m // 2) * 2 + m % 2
        at = pl.ds(pl.multiple_of(((y + ph) % 2 * 2 + cc) * rows, rows), rows)
        mine = pl.ds(cc * rows, rows)
        head = pl.ds(pl.multiple_of((x * 2 + c) * head_dim, head_dim), head_dim)
        here = (to == s) & owner

        @pl.when(jnp.logical_not(here))
        def _():
            act(remote(
                ob.at[m, ph, mine], att.at[at, head], kv_send.at[m // 2, m % 2, ph, cc],
                o_recv.at[x * 2 + c, ph, cc], (to, y * 2 + low),
            ))

        if act is start:

            @pl.when(here)
            def _():
                att[at, head] = ob[m, ph, mine]

    def merge(ph):
        for cc in range(2):
            for one in give(ph, cc):
                one.wait_recv()
            for m in range(4):
                lanes = slice(m * rows, (m + 1) * rows)
                a, b = stat[ph, 1, cc, 0:1, lanes], stat_in[ph, cc, 0:1, lanes]
                peak = jnp.maximum(a, b)
                wa, wb = jnp.exp2(a - peak), jnp.exp2(b - peak)
                den = 1.0 / (stat[ph, 1, cc, 1:2, lanes] * wa + stat_in[ph, cc, 1:2, lanes] * wb)
                done = acc[ph, 1, cc, :, lanes] * (wa * den) + acc_in[ph, cc, :, lanes] * (wb * den)
                ob[m, ph, cc * rows : (cc + 1) * rows] = done.T.astype(BF16)
            for m in (3 - place, (place + 2) % 4, place + 1 - 2 * x, place):
                return_o(m, ph, cc, start)

    step_cols = width // chunks

    def piece(n, yy, cc):
        at = pl.ds(pl.multiple_of((yy * 2 + cc) * rows, rows), rows)
        return jnp.dot(
            att[at, :], wo[:, n * step_cols : (n + 1) * step_cols], preferred_element_type=F32
        )

    cores = [
        [
            remote(core_out.at[h, n], core_in.at[h, n], q_send.at[h, n // 2, n % 2], core_recv.at[h, n], (s, partner))
            for n in range(chunks)
        ]
        for h in range(2)
    ]
    mesh = [
        remote(mesh_out.at[n], mesh_in.at[n], mesh_send.at[n], mesh_recv.at[n], (s, across))
        for n in range(chunks)
    ]

    def have_o(ph, cc):
        at = pl.ds(pl.multiple_of(((y + ph) % 2 * 2 + cc) * rows, rows), rows)
        for i in range(2):
            for g in range(2):
                ref = att.at[at, pl.ds((i * 2 + g) * head_dim, head_dim)]
                one = remote(ref, ref, kv_send.at[0, 0, 0, 0], o_recv.at[i * 2 + g, ph, cc], (s, partner))
                pl.when(jnp.logical_not(owner & (x == i) & (g == c)))(one.wait_recv)

    def mix(ph, cc):
        yy = (y + ph) % 2

        def give_core(block, n):
            core_out[ph, n] = piece(n, yy, block).astype(BF16)
            cores[ph][n].start()

        def take_core(n, value):
            cores[ph][n].wait_recv()
            value = value + core_in[ph, n].astype(F32)
            if ph == 1:
                mesh_out[n] = value.astype(BF16)
                mesh[n].start()
            else:
                mixed[n] = value

        if cc == 0:
            have_o(ph, 0)

            @pl.when(c == 1)
            def _():
                for n in range(chunks):
                    give_core(0, n)

            @pl.when(c == 0)
            def _():
                for n in range(chunks):
                    mixed[n] = piece(n, yy, 0)
                for n in range(chunks):
                    take_core(n, mixed[n])

            return

        @pl.when(c == (0 if cc == 1 else 1))
        def _():
            have_o(ph, 1)
            for n in range(chunks):
                if cc == 1:
                    give_core(1, n)
                    continue
                take_core(n, piece(n, yy, 1))

    take_q(0)
    prefix()
    have_q(0)
    have_own(0)
    sweeps(0, 0, 0, 1, False)
    sweeps(0, 0, 1, quads, True)
    take_q(1)
    have_q(1)
    take_mate(1)
    sweep(1, [latent((quad + n) % quads, 0) for n in range(quads)])
    have_own(1)
    sweep(1, [latent(quad, 1)])
    others = [(quad + n) % quads for n in range(1, quads)]
    for goal in others:
        have_kv(goal, 1)
    sweep(1, [latent(goal, 1) for goal in others])
    have_ctx()
    ctx_keys = jnp.concatenate([cb[k, 0] for k in range(2)], axis=0)
    ctx_values = jnp.concatenate([cb[k, 1] for k in range(2)], axis=0)
    ctx_values = ctx_values.astype(F32).T.astype(BF16)
    ctx_block = (lambda: ctx_keys, lambda: ctx_values, lift * math.log2(math.e))
    sweep(1, [ctx_block], send=True)
    for ph in range(2):
        send_kv(ph, (0, 1), "all", sent)
        send_q(ph, sent)
    merge(1)
    sweep(0, [latent(quad, 1), ctx_block])
    mix(1, 0)
    mix(1, 1)
    sweep(0, [latent(goal, 1) for goal in others], send=True)
    mix(1, 2)
    merge(0)
    mix(0, 0)
    mix(0, 1)
    mix(0, 2)
    square = jnp.zeros((rows, 1), F32)
    for n in range(chunks):
        mesh[n].wait_recv()
        value = mixed[n] + mesh_in[n].astype(F32)
        mixed[n] = value
        square = square + jnp.sum(value * value, axis=-1, keepdims=True)
    inv = lax.rsqrt(square / width + NORM_EPS)
    for n in range(chunks):
        at = slice(n * step_cols, (n + 1) * step_cols)
        gate = mod[0:1, 2 * width + n * step_cols : 2 * width + (n + 1) * step_cols]
        out_ref[:, at] = (lat[t, :, at].astype(F32) + gate * (mixed[n] * inv)).astype(BF16)

    given = [one for ph in range(2) for cc in range(2) for one in give(ph, cc)]
    for one in sends + given + cores[0] + cores[1] + mesh:
        one.wait_send()
    for ph in range(2):
        pass_on(ph, sent)
        for m in range(4):
            for cc in range(2):
                return_o(m, ph, cc, sent)
    send_ctx(sent)


def mix_kernel(
    tp_count, chunks,
    att_ref, wo_hbm, wo_ref, wo_sem, lat_ref, gate_ref,
    out_ref,
    core_out, core_in, mesh_out, mesh_in, mixed, core_send, core_recv, mesh_send, mesh_recv,
):
    s, t = lax.axis_index("sp"), lax.axis_index("tp")
    y, c = t // 2, t % 2
    y_count = tp_count // 2
    partner = y * 2 + 1 - c
    rows, width = lat_ref.shape
    step = width // chunks
    peers = [((y + j) % y_count) * 2 + c for j in range(1, y_count)]
    pltpu.make_async_copy(wo_hbm, wo_ref, wo_sem.at[0]).wait()

    def piece(n, j, cc):
        yy = (y + j) % y_count
        at = pl.ds(pl.multiple_of((yy * 2 + cc) * rows, rows), rows)
        return jnp.dot(
            att_ref[at, :], wo_ref[:, n * step : (n + 1) * step], preferred_element_type=F32
        )

    order = list(range(1, y_count)) + [0]
    cores = [
        remote(core_out.at[n], core_in.at[n], core_send.at[n], core_recv.at[n], (s, partner))
        for n in range(chunks)
    ]
    sent = []
    for n in range(chunks + 1):
        if n < chunks:
            for j in order:
                core_out[n, j] = piece(n, j, 1 - c).astype(BF16)
            cores[n].start()
        if n == 0:
            continue
        m = n - 1
        own = [piece(m, j, c) for j in order]
        cores[m].wait_recv()
        for j, value in zip(order, own):
            value = value + core_in[m, j].astype(F32)
            if j == 0:
                mixed[m] = value
            else:
                mesh_out[m, j - 1] = value.astype(BF16)
                one = remote(
                    mesh_out.at[m, j - 1], mesh_in.at[m, j - 1], mesh_send.at[m, j - 1],
                    mesh_recv.at[m, j - 1], (s, peers[j - 1]),
                )
                one.start()
                sent.append(one)
    for one in sent:
        one.wait_recv()
    square = jnp.zeros((rows, 1), F32)
    for n in range(chunks):
        value = mixed[n]
        for j in range(1, y_count):
            value = value + mesh_in[n, j - 1].astype(F32)
        mixed[n] = value
        square = square + jnp.sum(value * value, axis=-1, keepdims=True)
    inv = lax.rsqrt(square / width + NORM_EPS)
    for n in range(chunks):
        at = slice(n * step, (n + 1) * step)
        out_ref[:, at] = (
            lat_ref[:, at].astype(F32) + gate_ref[:, at] * (mixed[n] * inv)
        ).astype(BF16)
    for one in sent + cores:
        one.wait_send()


def whole_kernel(sp_count, tp_count, x_count, head_dim, group, lift, chunks, counts, *refs):
    (
        cond, cond_1, mw, lat, ctx, wq, wk, wv, qg, kg, cos, sin, wo, lat_rows,
        out, qt, k, vt, ckv, gate, att, wo_vm, wo_sem, *rest,
    ) = refs
    front, middle, last = counts
    front_scratch, middle_scratch = rest[:front], rest[front : front + middle]
    front_kernel(
        sp_count, tp_count, head_dim, cond, cond_1, mw, lat, ctx, wq, wk, wv, qg, kg, cos, sin,
        qt, k, vt, ckv, gate, *front_scratch, wo, wo_vm, wo_sem,
    )
    attend_kernel(sp_count, x_count, group, lift, k, vt, ckv, qt, att, *middle_scratch)
    mix_kernel(
        tp_count, chunks, att, wo, wo_vm, wo_sem, lat_rows, gate, out, *rest[front + middle :]
    )


ANY = pl.BlockSpec(memory_space=pl.ANY)
VM = pl.BlockSpec(memory_space=pltpu.VMEM)
DMA = pltpu.SemaphoreType.DMA


def grid_tables(sp_count, all_rows, head_dim):
    quarter, lines, lane = head_dim // 4, all_rows // GRID_W, np.arange(128)
    inv_freq = np.float32(ROPE_BASE) ** (-np.arange(quarter, dtype=np.float32) / quarter)
    rows = np.arange(sp_count)[:, None] * lines + lane[None, :] % lines
    both = np.stack([rows, np.broadcast_to(lane % GRID_W, rows.shape)], axis=1).astype(np.float32)
    angles = (both[:, :, None, :] * inv_freq[None, None, :, None]).astype(np.float32)
    return jnp.asarray(np.cos(angles)), jnp.asarray(np.sin(angles))


def quad_call(args, out_weight, sp_count, head_dim, lift):
    mod_weight, latents, context, query_weight, key_matrix, value_matrix = args[2:8]
    rows, width = latents.shape
    ctx_rows = context.shape[0]
    mod_cols = mod_weight.shape[1]
    all_rows, z_count, quads, chunks = 4 * rows, sp_count // 2, sp_count // 4, 4
    step = width // chunks
    cos, sin = grid_tables(sp_count, all_rows, head_dim)
    block = max(all_rows, z_count * ctx_rows)
    scratch = [
        pltpu.VMEM(args[0].shape, F32),
        pltpu.VMEM(args[1].shape, F32),
        pltpu.VMEM(args[8].shape, F32),
        pltpu.VMEM(args[9].shape, F32),
        pltpu.VMEM(cos.shape[1:], F32),
        pltpu.VMEM(sin.shape[1:], F32),
        DMA((6,)),
        pltpu.VMEM(mod_weight.shape, F32),
        pltpu.VMEM((4, rows, width), BF16),
        pltpu.VMEM((quads, ctx_rows, width), BF16),
        pltpu.VMEM(query_weight.shape, BF16),
        pltpu.VMEM(key_matrix.shape, BF16),
        pltpu.VMEM(value_matrix.shape, BF16),
        pltpu.VMEM(out_weight.shape, BF16),
        pltpu.VMEM((2, head_dim // 4, all_rows), F32),
        pltpu.VMEM((2, head_dim // 4, all_rows), F32),
        pltpu.VMEM((sp_count, 2, mod_cols), F32),
        pltpu.VMEM((4, 2, mod_cols), F32),
        pltpu.VMEM((2, 4 * mod_cols), F32),
        pltpu.VMEM((2 * rows, width), BF16),
        pltpu.VMEM((2 * rows, width), F32),
        pltpu.VMEM((4, 4, head_dim, rows), BF16),
        pltpu.VMEM((2, all_rows, head_dim), BF16),
        pltpu.VMEM((2, head_dim, all_rows), BF16),
        pltpu.VMEM((2, 2, quads * ctx_rows, head_dim), BF16),
        pltpu.VMEM((2, 2, 2, head_dim, all_rows), BF16),
        pltpu.VMEM((quads, 2, all_rows, head_dim), BF16),
        pltpu.VMEM((quads, 2, head_dim, all_rows), BF16),
        pltpu.VMEM((2, 2, quads * ctx_rows, head_dim), BF16),
        pltpu.VMEM((2, 2, 2, 2, all_rows), F32),
        pltpu.VMEM((2, 2, 2, head_dim, all_rows), F32),
        pltpu.VMEM((2, 2, 2, all_rows), F32),
        pltpu.VMEM((2, 2, head_dim, all_rows), F32),
        pltpu.VMEM((2, block, all_rows), F32),
        pltpu.VMEM((2, block, all_rows), BF16),
        pltpu.VMEM((2, 1, all_rows), F32),
        pltpu.VMEM((4, 2, 2 * rows, head_dim), BF16),
        pltpu.VMEM((all_rows, 4 * head_dim), BF16),
        pltpu.VMEM((2, chunks, rows, step), BF16),
        pltpu.VMEM((2, chunks, rows, step), BF16),
        pltpu.VMEM((chunks, rows, step), BF16),
        pltpu.VMEM((chunks, rows, step), BF16),
        pltpu.VMEM((chunks, rows, step), F32),
        DMA((7,)),
        DMA((7,)),
        DMA((7,)),
        DMA((sp_count,)),
        DMA((sp_count,)),
        DMA((4,)),
        DMA((4,)),
        DMA((2, 2, quads, 2)),
        DMA((2, 2, z_count)),
        DMA((2,)),
        DMA((2,)),
        DMA((2, 2, 2)),
        DMA((2, 4, 2)),
        DMA((4, 2)),
        DMA((4, quads)),
        DMA((2, quads)),
        DMA((2, quads)),
        DMA((2, 2)),
        DMA((2, 2)),
        DMA((2, 2)),
        DMA((2, 2)),
        DMA((4, 2, 2)),
        DMA((2, chunks)),
        DMA((chunks,)),
        DMA((chunks,)),
    ]
    out = pl.pallas_call(
        functools.partial(quad_kernel, sp_count, head_dim, lift, chunks),
        out_shape=pltpu.VMEM((rows, width), BF16),
        in_specs=[pl.BlockSpec(memory_space=pltpu.HBM)] * 13,
        out_specs=VM,
        scratch_shapes=scratch,
        compiler_params=pltpu.CompilerParams(
            collective_id=0, has_side_effects=True, vmem_limit_bytes=VMEM_BYTES - 2 * rows * width * 2
        ),
        name="quad",
    )(*args, cos, sin, out_weight)
    return out


def body(
    latents,
    context,
    cond,
    ctx_cond,
    mod_weight,
    query_weight,
    key_matrix,
    value_matrix,
    out_weight,
    query_gain,
    key_gain,
):
    sp_count, tp_count = lax.axis_size("sp"), lax.axis_size("tp")
    x_count = row_size(sp_count)
    rows, width = latents.shape
    ctx_rows = context.shape[0]
    head_dim = query_gain.shape[0]
    heads = query_weight.shape[1] // head_dim
    kv_heads = key_matrix.shape[1] // head_dim
    all_rows = rows * tp_count
    mod_cols = mod_weight.shape[1]
    lift = math.log(sp_count * all_rows / (2.0 * sp_count * ctx_rows))
    group = heads // kv_heads
    args = (
        cond[None], ctx_cond[None], mod_weight, latents, context, query_weight, key_matrix, value_matrix,
        query_gain[None], key_gain[None],
    )
    wide = all_rows % GRID_W == 0 and all_rows == rows * 4 and rows % 128 == 0
    if wide and kv_heads == 2 and group == 2 and x_count == 2 and sp_count % 4 == 0 and ctx_rows % 32 == 0:
        return quad_call(args, out_weight, sp_count, head_dim, lift)
    chunks = 4
    y_count = tp_count // 2
    step = width // chunks
    far = max(y_count - 1, 1)
    positions = lax.axis_index("sp") * all_rows + jnp.arange(all_rows, dtype=jnp.int32)
    cos, sin = tables(positions, head_dim)
    shared = [
        pltpu.VMEM((heads, head_dim, all_rows), BF16),
        pltpu.VMEM((kv_heads, all_rows, head_dim), BF16),
        pltpu.VMEM((kv_heads, head_dim, all_rows), BF16),
        pltpu.VMEM((kv_heads, 2, ctx_rows, head_dim), BF16),
        pltpu.VMEM((1, width), F32),
        pltpu.VMEM((all_rows, heads * head_dim), BF16),
        pltpu.VMEM(out_weight.shape, BF16),
        DMA((1,)),
    ]
    front = [
        pltpu.VMEM(mod_weight.shape, F32),
        pltpu.VMEM((tp_count, rows, width), BF16),
        pltpu.VMEM(query_weight.shape, BF16),
        pltpu.VMEM(key_matrix.shape, BF16),
        pltpu.VMEM(value_matrix.shape, BF16),
        pltpu.VMEM((sp_count, 2, mod_cols), F32),
        pltpu.VMEM((tp_count, 2, mod_cols), F32),
        pltpu.VMEM((2, mod_cols * tp_count), F32),
        pltpu.VMEM((2 * rows, width), BF16),
        DMA((5,)),
        DMA((tp_count,)),
        DMA((tp_count,)),
        DMA((sp_count,)),
        DMA((sp_count,)),
        DMA((tp_count,)),
        DMA((tp_count,)),
    ]
    middle = [
        pltpu.VMEM((sp_count, kv_heads, all_rows, head_dim), BF16),
        pltpu.VMEM((sp_count, kv_heads, head_dim, all_rows), BF16),
        pltpu.VMEM((sp_count, kv_heads, 2, ctx_rows, head_dim), BF16),
        pltpu.VMEM((heads, 1, all_rows), F32),
        pltpu.VMEM((heads, 1, all_rows), F32),
        pltpu.VMEM((heads, head_dim, all_rows), F32),
        DMA((3,)),
    ]
    middle += [DMA((3, sp_count, x_count + 1)), DMA((3, sp_count))]
    last = [
        pltpu.VMEM((chunks, y_count, rows, step), BF16),
        pltpu.VMEM((chunks, y_count, rows, step), BF16),
        pltpu.VMEM((chunks, far, rows, step), BF16),
        pltpu.VMEM((chunks, far, rows, step), BF16),
        pltpu.VMEM((chunks, rows, step), F32),
        DMA((chunks,)),
        DMA((chunks,)),
        DMA((chunks, far)),
        DMA((chunks, far)),
    ]
    counts = (len(front), len(middle), len(last))
    return pl.pallas_call(
        functools.partial(
            whole_kernel, sp_count, tp_count, x_count, head_dim, group, lift, chunks, counts
        ),
        out_shape=jax.ShapeDtypeStruct((rows, width), BF16),
        in_specs=[VM, VM, ANY, ANY, VM, ANY, ANY, ANY, VM, VM, VM, VM, ANY, VM],
        out_specs=VM,
        scratch_shapes=shared + front + middle + last,
        compiler_params=pltpu.CompilerParams(
            collective_id=0, has_side_effects=True, vmem_limit_bytes=VMEM_BYTES
        ),
        name="whole",
    )(
        *args, cos, sin, out_weight, latents,
    )


def solution(mesh):
    placed = (
        P(("sp", "tp"), None),
        P("sp", None),
        P("sp"),
        P("sp"),
        P("sp", "tp"),
        P(None, "tp"),
        P(None, "tp"),
        P(None, "tp"),
        P("tp", None),
        P(),
        P(),
    )
    return jax.shard_map(
        body, mesh=mesh, in_specs=placed, out_specs=P(("sp", "tp"), None), check_vma=False
    )
```

```python
import functools
import math

import jax
import jax.numpy as jnp
import numpy as np
from jax import lax
from jax.experimental import pallas as pl
from jax.experimental.pallas import tpu as pltpu
from jax.sharding import PartitionSpec as P

GRID_W = 64
NORM_EPS = 1e-06
ROPE_BASE = 10000.0
MESH = pl.DeviceIdType.MESH
BF16 = jnp.bfloat16
F32 = jnp.float32
VMEM_BYTES = 67043328


def row_size(sp_count):
    size = 1
    while 4 * size * size <= sp_count:
        size *= 2
    return size


def tables(positions, head_dim):
    quarter = head_dim // 4
    inv_freq = ROPE_BASE ** (-jnp.arange(quarter, dtype=F32) / quarter)
    where = jnp.stack([positions // GRID_W, positions % GRID_W]).astype(F32)
    angles = where[:, None, :] * inv_freq[None, :, None]
    return jnp.cos(angles), jnp.sin(angles)


def remote(src, dst, send, recv, dev):
    return pltpu.make_async_remote_copy(
        src_ref=src, dst_ref=dst, send_sem=send, recv_sem=recv, device_id=dev, device_id_type=MESH
    )


def front_kernel(
    sp_count, tp_count, head_dim,
    cond_ref, cond_1_ref, mw_hbm, lat_hbm, ctx_ref, wq_hbm, wk_hbm, wv_hbm, qg_ref, kg_ref, cos_ref, sin_ref,
    qt_ref, k_ref, vt_ref, ckv_ref, gate_ref,
    mw, lat, wq, wk, wv, part, tot, mod, xn, load_sem,
    lat_send, lat_recv, part_send, part_recv, tot_send, tot_recv,
    wo_hbm, wo_vm, wo_sem,
):
    s, t = lax.axis_index("sp"), lax.axis_index("tp")
    y, c = t // 2, t % 2
    y_count = tp_count // 2
    partner = y * 2 + 1 - c
    rows = lat.shape[1]
    width = lat.shape[2]
    model_cols = mod.shape[1]

    own = pltpu.make_async_copy(lat_hbm, lat.at[t], load_sem.at[0])
    own.start()
    loads = [
        pltpu.make_async_copy(a, b, load_sem.at[1 + i])
        for i, (a, b) in enumerate(((mw_hbm, mw), (wq_hbm, wq), (wk_hbm, wk), (wv_hbm, wv)))
    ]
    for one in loads:
        one.start()

    pltpu.make_async_copy(wo_hbm, wo_vm, wo_sem.at[0]).start()

    barrier = pltpu.get_barrier_semaphore()
    for j in range(1, sp_count):
        pl.semaphore_signal(barrier, inc=1, device_id=((s + j) % sp_count, t), device_id_type=MESH)
    for j in range(1, tp_count):
        pl.semaphore_signal(barrier, inc=1, device_id=(s, (t + j) % tp_count), device_id_type=MESH)
    pl.semaphore_wait(barrier, sp_count + tp_count - 2)

    own.wait()
    sends = []
    for j in range(1, y_count):
        peer = ((y + j) % y_count) * 2 + c
        sends.append(remote(lat.at[t], lat.at[t], lat_send.at[j], lat_recv.at[t], (s, peer)))
    sends.append(remote(lat.at[t], lat.at[t], lat_send.at[0], lat_recv.at[t], (s, partner)))
    for one in sends:
        one.start()

    loads[0].wait()
    lines = lax.broadcasted_iota(jnp.int32, (8, cond_ref.shape[1]), 0)
    cond = jnp.where(lines == 0, cond_ref[...], jnp.where(lines == 1, cond_1_ref[...], 0.0))
    cond = cond * jax.nn.sigmoid(cond)
    part[s] = jnp.dot(
        cond, mw[...], precision=lax.Precision.HIGHEST, preferred_element_type=F32
    )[:2]
    more = [
        remote(part.at[s], part.at[s], part_send.at[j], part_recv.at[s], ((s + j) % sp_count, t))
        for j in range(1, sp_count)
    ]
    for one in more:
        one.start()
    for j in range(1, sp_count):
        src = (s + j) % sp_count
        remote(part.at[src], part.at[src], part_send.at[0], part_recv.at[src], (s, t)).wait_recv()
    total = part[0]
    for j in range(1, sp_count):
        total = total + part[j]
    tot[t] = total
    last = [
        remote(tot.at[t], tot.at[t], tot_send.at[j], tot_recv.at[t], (s, (t + j) % tp_count))
        for j in range(1, tp_count)
    ]
    for one in last:
        one.start()
    for j in range(1, tp_count):
        src = (t + j) % tp_count
        remote(tot.at[src], tot.at[src], tot_send.at[0], tot_recv.at[src], (s, t)).wait_recv()
    cols = model_cols // tp_count
    for j in range(tp_count):
        mod[:, j * cols : (j + 1) * cols] = tot[j]
    gate_ref[...] = mod[0:1, 2 * width :]

    def modulate(x, r):
        x = x.astype(F32)
        scaled = x * lax.rsqrt(jnp.mean(x * x, axis=-1, keepdims=True) + NORM_EPS)
        shift, scale = mod[r : r + 1, :width], mod[r : r + 1, width : 2 * width]
        return (scaled * (1.0 + scale) + shift).astype(BF16)

    for one in loads[1:]:
        one.wait()

    cn = modulate(ctx_ref[...], 1)
    kc = jnp.dot(cn, wk[...], preferred_element_type=F32)
    vc = jnp.dot(cn, wv[...], preferred_element_type=F32)
    for h in range(kc.shape[1] // head_dim):
        kh = kc[:, h * head_dim : (h + 1) * head_dim]
        kh = kh * lax.rsqrt(jnp.mean(kh * kh, axis=-1, keepdims=True) + NORM_EPS) * kg_ref[...]
        ckv_ref[h, 0] = kh.astype(BF16)
        ckv_ref[h, 1] = vc[:, h * head_dim : (h + 1) * head_dim].astype(BF16)

    q4 = head_dim // 4
    qgain, kgain = qg_ref[...], kg_ref[...]

    def turn(yt, cos, sin):
        out = []
        for n in range(2):
            a = yt[2 * n * q4 : (2 * n + 1) * q4]
            b = yt[(2 * n + 1) * q4 : (2 * n + 2) * q4]
            out += [a * cos[n] - b * sin[n], b * cos[n] + a * sin[n]]
        return jnp.concatenate(out, axis=0)

    def unit(yh, gain):
        return yh * lax.rsqrt(jnp.mean(yh * yh, axis=-1, keepdims=True) + NORM_EPS) * gain

    span = 2 * rows
    relays = []
    for j in range(y_count):
        yy = (y + j) % y_count
        if j > 0:
            src = yy * 2 + c
            remote(lat.at[src], lat.at[src], lat_send.at[0], lat_recv.at[src], (s, t)).wait_recv()
            one = remote(
                lat.at[src], lat.at[src], lat_send.at[y_count - 1 + j], lat_recv.at[src], (s, partner)
            )
            one.start()
            relays.append(one)
        other = yy * 2 + 1 - c
        remote(lat.at[other], lat.at[other], lat_send.at[0], lat_recv.at[other], (s, t)).wait_recv()
        for i in range(2):
            xn[i * rows : (i + 1) * rows, :] = modulate(lat[yy * 2 + i], 0)
        x = xn[...]
        at = pl.ds(pl.multiple_of(yy * span, span), span)
        cos, sin = cos_ref[:, :, at], sin_ref[:, :, at]
        for w, kind in ((wq, 0), (wk, 1), (wv, 2)):
            step = min(2 * head_dim, w.shape[1])
            for n in range(0, w.shape[1], step):
                full = jnp.dot(x, w[:, n : n + step], preferred_element_type=F32)
                for m in range(0, step, head_dim):
                    h = (n + m) // head_dim
                    yh = full[:, m : m + head_dim]
                    if kind == 0:
                        qt_ref[h, :, at] = turn(unit(yh, qgain).T, cos, sin).astype(BF16)
                    elif kind == 1:
                        k_ref[h, at, :] = turn(unit(yh, kgain).T, cos, sin).T.astype(BF16)
                    else:
                        vt_ref[h, :, at] = yh.T.astype(BF16)
    for one in sends + more + last + relays:
        one.wait_send()


def attend_kernel(
    sp_count, x_count, group, lift,
    k_hbm, vt_hbm, ckv_hbm, qt_ref,
    out_ref,
    kb, vb, cb, top, tot, acc, load_sem, send_sem, recv_sem,
):
    s, t = lax.axis_index("sp"), lax.axis_index("tp")
    z, x = s // x_count, s % x_count
    z_count = sp_count // x_count
    heads, head_dim, rows = qt_ref.shape
    kv_heads = heads // group
    factor = head_dim ** (-0.5) * math.log2(math.e)

    loads = [
        pltpu.make_async_copy(a, b, load_sem.at[i])
        for i, (a, b) in enumerate(
            (
                (ckv_hbm, cb.at[s]),
                (k_hbm, kb.at[s]),
                (vt_hbm, vb.at[s]),
            )
        )
    ]
    for one in loads:
        one.start()
    targets = []
    for sign in (1, -1):
        ok = (z + sign >= 0) & (z + sign < z_count)
        peer = ((z + sign + z_count) % z_count) * x_count + x
        targets.append((ok, peer))

    top[...] = jnp.full_like(top, -1e30)
    tot[...] = jnp.zeros_like(tot)
    acc[...] = jnp.zeros_like(acc)
    for one in loads:
        one.wait()

    bufs = (cb, kb, vb)

    def copies(src, way, peer):
        return [
            remote(b.at[src], b.at[src], send_sem.at[i, src, way], recv_sem.at[i, src], (peer, t))
            for i, b in enumerate(bufs)
        ]

    def source(k):
        low = jnp.minimum(z, z_count - 1 - z)
        both = k <= 2 * low
        dist = jnp.where(both, (k + 1) // 2, k - low)
        up = jnp.where(both, k % 2 == 1, z < z_count - 1 - z)
        return jnp.where(up, z + dist, z - dist)

    def update(i, keys, values_t, bias):
        sc = jnp.dot(keys, qt_ref[i], preferred_element_type=F32) * factor
        if bias != 0.0:
            sc = sc + bias
        old = top[i]
        new = jnp.maximum(old, jnp.max(sc, axis=0, keepdims=True))
        p = jnp.exp2(sc - new)
        f = jnp.exp2(old - new)
        top[i] = new
        tot[i] = tot[i] * f + jnp.sum(p, axis=0, keepdims=True)
        acc[i] = acc[i] * f + jnp.dot(values_t, p.astype(BF16), preferred_element_type=F32)

    def block(src):
        def head(i, carry):
            h = i // group
            update(i, kb[src, h], vb[src, h], 0.0)
            return carry

        lax.fori_loop(0, heads, head, 0)

    def wait_from(src):
        for one in copies(src, 0, s):
            one.wait_recv()

    def step(k, carry):
        zz = source(k)
        src = zz * x_count + x

        @pl.when(k > 0)
        def _():
            wait_from(src)

        for way, (ok, peer) in enumerate(targets):
            mine = zz <= z if way == 0 else zz >= z

            @pl.when(ok & mine)
            def _():
                for one in copies(src, way, peer):
                    one.start()

        for j in range(1, x_count):
            for one in copies(src, 1 + j, z * x_count + (x + j) % x_count):
                one.start()
        block(src)

        @pl.when(k > 0)
        def _():
            before = source(k - 1)
            for j in range(1, x_count):
                old = before * x_count + (x + j) % x_count
                wait_from(old)
                block(old)

        return carry

    lax.fori_loop(0, z_count, step, 0)
    final = source(z_count - 1)
    ends = [final * x_count + (x + j) % x_count for j in range(1, x_count)]
    for src in ends:
        copies(src, 0, s)[0].wait_recv()
    for i in range(heads):
        h = i // group
        keys = jnp.concatenate([cb[j, h, 0] for j in range(sp_count)], axis=0)
        vals = jnp.concatenate([cb[j, h, 1] for j in range(sp_count)], axis=0)
        update(i, keys, vals.astype(F32).T.astype(BF16), lift * math.log2(math.e))
    for src in ends:
        for one in copies(src, 0, s)[1:]:
            one.wait_recv()
        block(src)
    for i in range(heads):
        out_ref[:, i * head_dim : (i + 1) * head_dim] = (acc[i] / tot[i]).T.astype(BF16)

    def drain(k, carry):
        zz = source(k)
        src = zz * x_count + x
        for way, (ok, peer) in enumerate(targets):
            mine = zz <= z if way == 0 else zz >= z

            @pl.when(ok & mine)
            def _():
                for one in copies(src, way, peer):
                    one.wait_send()

        for j in range(1, x_count):
            for one in copies(src, 1 + j, z * x_count + (x + j) % x_count):
                one.wait_send()
        return carry

    lax.fori_loop(0, z_count, drain, 0)


def quad_kernel(sp_count, head_dim, lift, chunks, *refs):
    (
        cond_hbm, cond_1_hbm, mw_hbm, lat_hbm, ctx_hbm, wq_hbm, wk_hbm, wv_hbm, qg_hbm, kg_hbm,
        cos_hbm, sin_hbm, wo_hbm,
        out_ref,
        cond_ref, cond_1_ref, qg_ref, kg_ref, cos_in, sin_in, small_sem,
        mw, lat, ctx, wq, wk, wv, wo, cos_ref, sin_ref, part, tot, mod, xn, xs,
        qt, kk, vt, ckv, qb, kb, vb, cb, stat, acc, stat_in, acc_in,
        score, prob, fade, ob, att, core_out, core_in, mesh_out, mesh_in, mixed,
        load_sem, lat_send, lat_recv, part_send, part_recv, tot_send, tot_recv,
        kv_send, kv_recv, c_send, c_recv, q_send, q_recv, relay_send, pass_send, raw_send, raw_recv,
        a_send, a_recv, s_send, s_recv, o_recv, core_recv, mesh_send, mesh_recv,
    ) = refs
    s, t = lax.axis_index("sp"), lax.axis_index("tp")
    y, c = t // 2, t % 2
    z, x = s // 2, s % 2
    z_count = sp_count // 2
    quads = z_count // 2
    quad, low = z // 2, z % 2
    place = low * 2 + x
    partner, across = y * 2 + 1 - c, (1 - y) * 2 + c
    target = (z + x) % 2
    owner = low == c
    rows, width = lat.shape[1], lat.shape[2]
    all_rows = 4 * rows
    span = 2 * rows
    cuts = (0, rows * 3 // 8 // 16 * 16, rows * 3 // 4 // 16 * 16, rows)

    load_pairs = (
        (mw_hbm, mw), (lat_hbm, lat.at[t]), (wk_hbm, wk), (wv_hbm, wv), (wq_hbm, wq), (ctx_hbm, ctx.at[quad]),
        (wo_hbm, wo),
    )
    loads = [pltpu.make_async_copy(a, b, load_sem.at[i]) for i, (a, b) in enumerate(load_pairs)]
    small_pairs = (
        (cond_hbm, cond_ref), (cond_1_hbm, cond_1_ref), (cos_hbm.at[s], cos_in), (sin_hbm.at[s], sin_in),
        (qg_hbm, qg_ref), (kg_hbm, kg_ref),
    )
    smalls = [pltpu.make_async_copy(a, b, small_sem.at[i]) for i, (a, b) in enumerate(small_pairs)]
    for one in smalls[:2] + loads[:1] + smalls[2:] + loads[1:2]:
        one.start()

    barrier = pltpu.get_barrier_semaphore()
    for j in range(sp_count):
        for k in range(2):
            if j + k > 0:
                dev = ((s + j) % sp_count, y * 2 + (c + k) % 2)
                pl.semaphore_signal(barrier, inc=1, device_id=dev, device_id_type=MESH)
    for k in range(2):
        dev = (s, (1 - y) * 2 + (c + k) % 2)
        pl.semaphore_signal(barrier, inc=1, device_id=dev, device_id_type=MESH)

    for one in smalls:
        one.wait()
    lines = lax.broadcasted_iota(jnp.int32, (8, cond_ref.shape[1]), 0)
    cond = jnp.where(lines == 0, cond_ref[...], jnp.where(lines == 1, cond_1_ref[...], 0.0))
    cond = (cond * jax.nn.sigmoid(cond)).T
    for small, table in ((cos_in, cos_ref), (sin_in, sin_ref)):
        for n in range(all_rows // 128):
            at = slice(n * 128, (n + 1) * 128)
            parts = [
                jnp.broadcast_to(small[0, :, r : r + 1], (small.shape[1], GRID_W))
                for r in range(n * 128 // GRID_W, (n + 1) * 128 // GRID_W)
            ]
            table[0, :, at] = jnp.concatenate(parts, axis=1)
            table[1, :, at] = small[1]
    loads[0].wait()
    for one in loads[2:]:
        one.start()
    for r in range(2):
        part[s, r : r + 1, :] = jnp.sum(mw[...] * cond[:, r : r + 1], axis=0, keepdims=True)
    loads[1].wait()
    pl.semaphore_wait(barrier, 2 * sp_count + 1)

    sends = [
        remote(part.at[s], part.at[s], part_send.at[j], part_recv.at[s], ((s + j) % sp_count, t))
        for j in range(1, sp_count)
    ]
    sends.append(remote(lat.at[t], lat.at[t], lat_send.at[6], lat_recv.at[6], (s, partner)))
    pieces = [pl.ds(a, b - a) for a, b in zip(cuts, cuts[1:])]
    halves = [
        remote(lat.at[t, at], lat.at[t, at], lat_send.at[i], lat_recv.at[i], (s, across))
        for i, at in enumerate(pieces)
    ]
    for one in sends + halves[:1]:
        one.start()
    def unit_rows(value):
        value = value.astype(F32)
        return value * lax.rsqrt(jnp.mean(value * value, axis=-1, keepdims=True) + NORM_EPS)

    remote(lat.at[partner], lat.at[partner], lat_send.at[0], lat_recv.at[6], (s, partner)).wait_recv()
    for i in range(2):
        xs[i * rows : (i + 1) * rows, :] = unit_rows(lat[y * 2 + i])
    for j in range(1, sp_count):
        src = (s + j) % sp_count
        remote(part.at[src], part.at[src], part_send.at[0], part_recv.at[src], (s, partner)).wait_recv()
    total = part[0]
    for j in range(1, sp_count):
        total = total + part[j]
    tot[t] = total
    last = [
        remote(tot.at[t], tot.at[t], tot_send.at[j], tot_recv.at[t], (s, (t + j) % 4))
        for j in range(1, 4)
    ]
    ctx_rows = ctx.shape[1]
    half = ctx_rows // 2
    mine = pl.ds(pl.multiple_of(c * half, half), half)
    yours = pl.ds(pl.multiple_of((1 - c) * half, half), half)
    loads[5].wait()
    raw = [
        remote(
            ctx.at[quad, mine], ctx.at[quad, mine], raw_send.at[0, n], raw_recv.at[0, quad],
            ((((quad + n) % quads) * 2 + low) * 2 + x, t),
        )
        for n in range(1, quads)
    ]
    for one in last + halves[1:] + raw:
        one.start()
    sends += last + halves + raw
    for j in range(1, 4):
        src = (t + j) % 4
        remote(tot.at[src], tot.at[src], tot_send.at[0], tot_recv.at[src], (s, partner)).wait_recv()
    cols = tot.shape[2]
    for j in range(4):
        mod[:, j * cols : (j + 1) * cols] = tot[j]

    def relay_rows(i):
        at = pieces[i]
        remote(lat.at[across, at], lat.at[across, at], lat_send.at[0], lat_recv.at[i], (s, partner)).wait_recv()
        one = remote(
            lat.at[across, at], lat.at[across, at], lat_send.at[3 + i], lat_recv.at[3 + i], (s, partner)
        )
        one.start()
        sends.append(one)

    def modulate(scaled, r):
        shift, scale = mod[r : r + 1, :width], mod[r : r + 1, width : 2 * width]
        return (scaled * (1.0 + scale) + shift).astype(BF16)

    q4 = head_dim // 4
    qgain = qg_ref[...] * (head_dim ** (-0.5) * math.log2(math.e))
    kgain = kg_ref[...]

    def turn(yt, cos, sin):
        out = []
        for n in range(2):
            a = yt[2 * n * q4 : (2 * n + 1) * q4]
            b = yt[(2 * n + 1) * q4 : (2 * n + 2) * q4]
            out += [a * cos[n] - b * sin[n], b * cos[n] + a * sin[n]]
        return jnp.concatenate(out, axis=0)

    def unit(yh, gain):
        return yh * lax.rsqrt(jnp.mean(yh * yh, axis=-1, keepdims=True) + NORM_EPS) * gain

    def column(yy):
        return pl.ds(pl.multiple_of(yy * span, span), span)

    def dest(i, n):
        to = (((quad + n) % quads) * 2 + c) * 2 + i
        here = (to == s) & (target == c)
        return to, here

    def free(n):
        return (low == 1) == ((quad + n) % quads > quad)

    def row_spot(lo):
        return pl.ds(pl.multiple_of(lo * span, span), span)

    def allowed(n, which):
        if n == 0:
            return which in ("own", "all")
        if which == "own":
            return False
        straight = {"early": free(n), "late": jnp.logical_not(free(n)) & (c == low)}
        return straight[which] if which in straight else free(n) | (c == low)

    def send_kv(ph, kinds, which, act):
        at, spot = column((y + ph) % 2), row_spot(low)
        for n in range(quads):
            ok = allowed(n, which)
            if ok is False:
                continue
            for i in range(2):
                to, here = dest(i, n)
                for kind in kinds:
                    src, dst = (
                        (kk.at[i, at], kb.at[quad, ph, spot]),
                        (vt.at[i, :, at], vb.at[quad, ph, :, spot]),
                    )[kind]

                    @pl.when(jnp.logical_not(here) & ok)
                    def _():
                        act(remote(
                            src, dst, kv_send.at[kind, ph, n, i], kv_recv.at[kind, ph, z],
                            (to, y * 2 + target),
                        ))

    def send_ctx(act):
        for i in range(2):
            to, here = dest(i, 0)

            @pl.when(jnp.logical_not(here))
            def _():
                act(remote(ckv.at[i], cb.at[low], c_send.at[i], c_recv.at[low], (to, y * 2 + target)))

    def pass_on(ph, act):
        spot = row_spot(1 - low)
        for n in range(1, quads):
            to = (((quad + n) % quads) * 2 + low) * 2 + x
            copies = [
                remote(ref, ref, pass_send.at[2 * ph + kind, n], kv_recv.at[kind, ph, mate], (to, t))
                for kind, ref in ((0, kb.at[quad, ph, spot]), (1, vb.at[quad, ph, :, spot]))
            ]

            @pl.when(free(n))
            def _():
                for one in copies:
                    act(one)

    def spot_of(m):
        return pl.ds(pl.multiple_of(m * rows, rows), rows)

    def send_q(ph, act):
        blocks = pl.ds((y + ph) % 2 * 2, 2)
        lanes = spot_of(place)
        for i in range(2):
            to = (quad * 2 + c) * 2 + i
            for g in range(2):
                mine = (to == s) & (g == c)
                src = qt.at[i * 2 + g, blocks]

                @pl.when(mine)
                def _():
                    act(remote(
                        src, qb.at[0, ph, :, :, lanes], q_send.at[ph, i, g],
                        q_recv.at[0, place, ph], (s, partner),
                    ))

                @pl.when(jnp.logical_not(mine))
                def _():
                    act(remote(
                        src, qb.at[1, ph, :, :, lanes], q_send.at[ph, i, g],
                        q_recv.at[1, place, ph], (to, y * 2 + g),
                    ))

    def start(one):
        one.start()

    def sent(one):
        one.wait_send()

    def project(ph):
        yy = (y + ph) % 2
        for i in range(2):
            at = slice(i * rows, (i + 1) * rows)
            xn[at, :] = modulate(xs[at, :] if ph == 0 else unit_rows(lat[yy * 2 + i]), 0)
        value = xn[...]
        at = column(yy)
        cos, sin = cos_ref[:, :, at], sin_ref[:, :, at]
        spot = row_spot(low)

        def keys():
            full = jnp.dot(value, wk[...], preferred_element_type=F32)
            for h in range(2):
                yh = full[:, h * head_dim : (h + 1) * head_dim]
                kk[h, at, :] = turn(unit(yh, kgain).T, cos, sin).T.astype(BF16)
            send_kv(ph, (0,), "early", start)
            send_kv(ph, (0,), "own", start)

        def values():
            full = jnp.dot(value, wv[...], preferred_element_type=F32)
            for h in range(2):
                vt[h, :, at] = full[:, h * head_dim : (h + 1) * head_dim].T.astype(BF16)
            send_kv(ph, (1,), "early", start)
            send_kv(ph, (1,), "own", start)

            @pl.when(local)
            def _():
                kb[quad, ph, spot] = kk[x, at]
                vb[quad, ph, :, spot] = vt[x, :, at]

        def queries():
            for h in range(4):
                if h % 2 == 0:
                    full = jnp.dot(
                        value, wq[:, h * head_dim : (h + 2) * head_dim], preferred_element_type=F32
                    )
                yh = full[:, (h % 2) * head_dim : (h % 2 + 1) * head_dim]
                turned = turn(unit(yh, qgain).T, cos, sin).astype(BF16)
                for cc in range(2):
                    qt[h, yy * 2 + cc] = turned[:, cc * rows : (cc + 1) * rows]
            send_q(ph, start)
            lanes = spot_of(place)

            @pl.when(owner)
            def _():
                for cc in range(2):
                    qb[1, ph, cc, :, lanes] = qt[x * 2 + c, yy * 2 + cc]
                    qb[0, ph, cc, :, lanes] = qt[x * 2 + 1 - c, yy * 2 + cc]

        if ph == 1:
            queries()
            take_mate(0)
        keys()
        values()
        if ph == 0:
            queries()
        send_kv(ph, (0, 1), "late", start)

    def take_q(ph):
        for j in range(1, 4):
            m = (place + j) % 4
            lanes = spot_of(m)
            ref = qb.at[1, ph, :, :, lanes]
            remote(ref, ref, relay_send.at[0, 0], q_recv.at[1, m, ph], (s, partner)).wait_recv()
            one = remote(
                ref, qb.at[0, ph, :, :, lanes], relay_send.at[j, ph], q_recv.at[0, m, ph],
                (s, partner),
            )
            one.start()
            sends.append(one)

    def have_q(ph):
        for j in range(4):
            m = (place + j) % 4
            lanes = spot_of(m)
            for role in range(2) if j == 0 else range(1):
                ref = qb.at[role, ph, :, :, lanes]
                one = remote(ref, ref, relay_send.at[0, 0], q_recv.at[role, m, ph], (s, partner))
                if j == 0:
                    pl.when(jnp.logical_not(owner))(one.wait_recv)
                else:
                    one.wait_recv()

    def wait_kv(zz, ph):
        spot = row_spot(zz % 2)
        for kind, ref in ((0, kb.at[zz // 2, ph, spot]), (1, vb.at[zz // 2, ph, :, spot])):
            remote(ref, ref, kv_send.at[0, 0, 0, 0], kv_recv.at[kind, ph, zz], (s, partner)).wait_recv()

    def have_kv(goal, ph):
        for lo in range(2):
            wait_kv(goal * 2 + lo, ph)

    mate = quad * 2 + 1 - low
    inner = functools.reduce(jnp.logical_or, [free(n) for n in range(1, quads)], low < 0)

    def take_mate(ph):
        @pl.when(inner)
        def _():
            wait_kv(mate, ph)

        pass_on(ph, start)

    def have_own(ph):
        @pl.when(jnp.logical_not(inner))
        def _():
            wait_kv(mate, ph)

        @pl.when(jnp.logical_not(local))
        def _():
            wait_kv(z, ph)

    local = owner & (target == c)
    stat[...] = jnp.concatenate(
        [jnp.full(stat.shape[:3] + (1, all_rows), -1e30, F32), jnp.zeros(stat.shape[:3] + (1, all_rows), F32)],
        axis=3,
    )
    acc[...] = jnp.zeros_like(acc)
    for one in loads[2:5] + loads[6:]:
        one.wait()
    project(0)
    relay_rows(0)
    for n in range(1, quads):
        ref = ctx.at[(quad + n) % quads, mine]
        remote(ref, ref, raw_send.at[0, 0], raw_recv.at[0, (quad + n) % quads], (s, partner)).wait_recv()
        one = remote(ref, ref, raw_send.at[1, n], raw_recv.at[1, (quad + n) % quads], (s, partner))
        one.start()
        sends.append(one)
    relay_rows(1)
    relay_rows(2)
    other = (1 - y) * 2 + 1 - c
    for i, at in enumerate(pieces):
        ref = lat.at[other, at]
        remote(ref, ref, lat_send.at[0], lat_recv.at[3 + i], (s, partner)).wait_recv()
    project(1)

    def sweep(ph, blocks, send=False):
        tiles = [(block, n) for block in blocks for n in range(4)]

        def stage_a(i):
            (keys, _, _), n = tiles[i]
            count = keys().shape[0]
            score[i % 2, :count] = jnp.dot(keys(), qb[n % 2, ph, n // 2], preferred_element_type=F32)

        def stage_b(i):
            (keys, _, bias), n = tiles[i]
            count = keys().shape[0]
            sc = score[i % 2, :count]
            old = stat[ph, n % 2, n // 2, 0:1]
            new = jnp.maximum(old, jnp.max(sc, axis=0, keepdims=True) + bias)
            f = jnp.exp2(old - new)
            fade[i % 2] = f
            p = jnp.exp2(sc - (new - bias))
            stat[ph, n % 2, n // 2, 1:2] = (
                stat[ph, n % 2, n // 2, 1:2] * f + jnp.sum(p, axis=0, keepdims=True)
            )
            stat[ph, n % 2, n // 2, 0:1] = new
            prob[i % 2, :count] = p.astype(BF16)

        def stage_c(i):
            (keys, values, _), n = tiles[i]
            count = keys().shape[0]
            value = jnp.dot(values(), prob[i % 2, :count], preferred_element_type=F32)
            acc[ph, n % 2, n // 2] = acc[ph, n % 2, n // 2] * fade[i % 2] + value

        for i in range(len(tiles) + 2):
            if i < len(tiles):
                stage_a(i)
            if 1 <= i <= len(tiles):
                stage_b(i - 1)
            if i >= 2:
                stage_c(i - 2)
            if send and i >= len(tiles) - 2 and (len(tiles) - i) % 2 == 0:
                for one in give(ph, 0 if i < len(tiles) else 1):
                    one.start()

    def latent(goal, late):
        return (lambda: kb[goal, late], lambda: vb[goal, late], 0.0)

    def give(ph, cc):
        return [
            remote(acc.at[ph, 0, cc], acc_in.at[ph, cc], a_send.at[ph, cc], a_recv.at[ph, cc], (s, partner)),
            remote(stat.at[ph, 0, cc], stat_in.at[ph, cc], s_send.at[ph, cc], s_recv.at[ph, cc], (s, partner)),
        ]

    def prefix():
        for n in range(1, quads):
            ref = ctx.at[(quad + n) % quads, yours]
            remote(ref, ref, raw_send.at[0, 0], raw_recv.at[1, (quad + n) % quads], (s, partner)).wait_recv()
        cn = jnp.concatenate([modulate(unit_rows(ctx[n]), 1) for n in range(quads)], axis=0)
        kc = jnp.dot(cn, wk[...], preferred_element_type=F32)
        vc = jnp.dot(cn, wv[...], preferred_element_type=F32)
        for h in range(2):
            ckv[h, 0] = unit(kc[:, h * head_dim : (h + 1) * head_dim], kgain).astype(BF16)
            ckv[h, 1] = vc[:, h * head_dim : (h + 1) * head_dim].astype(BF16)
        send_ctx(start)

        @pl.when(local)
        def _():
            cb[low] = ckv[x]

    def have_ctx():
        for lo in range(2):

            @pl.when(jnp.logical_not(local & (lo == low)))
            def _():
                remote(cb.at[lo], cb.at[lo], c_send.at[0], c_recv.at[lo], (s, partner)).wait_recv()

    def sweeps(ph, late, begin, end, wait):
        def one(j, carry):
            goal = (quad + j) % quads
            if wait:

                @pl.when(j > 0)
                def _():
                    have_kv(goal, late)

            sweep(ph, [latent(goal, late)])
            return carry

        if end - begin == 1:
            one(begin, 0)
        elif end > begin:
            lax.fori_loop(begin, end, one, 0)

    def return_o(m, ph, cc, act):
        to = (quad * 2 + m // 2) * 2 + m % 2
        at = pl.ds(pl.multiple_of(((y + ph) % 2 * 2 + cc) * rows, rows), rows)
        mine = pl.ds(cc * rows, rows)
        head = pl.ds(pl.multiple_of((x * 2 + c) * head_dim, head_dim), head_dim)
        here = (to == s) & owner

        @pl.when(jnp.logical_not(here))
        def _():
            act(remote(
                ob.at[m, ph, mine], att.at[at, head], kv_send.at[m // 2, m % 2, ph, cc],
                o_recv.at[x * 2 + c, ph, cc], (to, y * 2 + low),
            ))

        if act is start:

            @pl.when(here)
            def _():
                att[at, head] = ob[m, ph, mine]

    def merge(ph):
        for cc in range(2):
            for one in give(ph, cc):
                one.wait_recv()
            for m in range(4):
                lanes = slice(m * rows, (m + 1) * rows)
                a, b = stat[ph, 1, cc, 0:1, lanes], stat_in[ph, cc, 0:1, lanes]
                peak = jnp.maximum(a, b)
                wa, wb = jnp.exp2(a - peak), jnp.exp2(b - peak)
                den = 1.0 / (stat[ph, 1, cc, 1:2, lanes] * wa + stat_in[ph, cc, 1:2, lanes] * wb)
                done = acc[ph, 1, cc, :, lanes] * (wa * den) + acc_in[ph, cc, :, lanes] * (wb * den)
                ob[m, ph, cc * rows : (cc + 1) * rows] = done.T.astype(BF16)
            for m in (3 - place, (place + 2) % 4, place + 1 - 2 * x, place):
                return_o(m, ph, cc, start)

    step_cols = width // chunks

    def piece(n, yy, cc):
        at = pl.ds(pl.multiple_of((yy * 2 + cc) * rows, rows), rows)
        return jnp.dot(
            att[at, :], wo[:, n * step_cols : (n + 1) * step_cols], preferred_element_type=F32
        )

    cores = [
        [
            remote(core_out.at[h, n], core_in.at[h, n], q_send.at[h, n // 2, n % 2], core_recv.at[h, n], (s, partner))
            for n in range(chunks)
        ]
        for h in range(2)
    ]
    mesh = [
        remote(mesh_out.at[n], mesh_in.at[n], mesh_send.at[n], mesh_recv.at[n], (s, across))
        for n in range(chunks)
    ]

    def have_o(ph, cc):
        at = pl.ds(pl.multiple_of(((y + ph) % 2 * 2 + cc) * rows, rows), rows)
        for i in range(2):
            for g in range(2):
                ref = att.at[at, pl.ds((i * 2 + g) * head_dim, head_dim)]
                one = remote(ref, ref, kv_send.at[0, 0, 0, 0], o_recv.at[i * 2 + g, ph, cc], (s, partner))
                pl.when(jnp.logical_not(owner & (x == i) & (g == c)))(one.wait_recv)

    def mix(ph, cc):
        yy = (y + ph) % 2

        def give_core(block, n):
            core_out[ph, n] = piece(n, yy, block).astype(BF16)
            cores[ph][n].start()

        def take_core(n, value):
            cores[ph][n].wait_recv()
            value = value + core_in[ph, n].astype(F32)
            if ph == 1:
                mesh_out[n] = value.astype(BF16)
                mesh[n].start()
            else:
                mixed[n] = value

        if cc == 0:
            have_o(ph, 0)

            @pl.when(c == 1)
            def _():
                for n in range(chunks):
                    give_core(0, n)

            @pl.when(c == 0)
            def _():
                for n in range(chunks):
                    mixed[n] = piece(n, yy, 0)
                for n in range(chunks):
                    take_core(n, mixed[n])

            return

        @pl.when(c == (0 if cc == 1 else 1))
        def _():
            have_o(ph, 1)
            for n in range(chunks):
                if cc == 1:
                    give_core(1, n)
                    continue
                take_core(n, piece(n, yy, 1))

    take_q(0)
    prefix()
    have_q(0)
    have_own(0)
    sweeps(0, 0, 0, 1, False)
    sweeps(0, 0, 1, quads, True)
    take_q(1)
    have_q(1)
    take_mate(1)
    sweep(1, [latent((quad + n) % quads, 0) for n in range(quads)])
    have_own(1)
    sweep(1, [latent(quad, 1)])
    others = [(quad + n) % quads for n in range(1, quads)]
    for goal in others:
        have_kv(goal, 1)
    sweep(1, [latent(goal, 1) for goal in others])
    have_ctx()
    ctx_keys = jnp.concatenate([cb[k, 0] for k in range(2)], axis=0)
    ctx_values = jnp.concatenate([cb[k, 1] for k in range(2)], axis=0)
    ctx_values = ctx_values.astype(F32).T.astype(BF16)
    ctx_block = (lambda: ctx_keys, lambda: ctx_values, lift * math.log2(math.e))
    sweep(1, [ctx_block], send=True)
    for ph in range(2):
        send_kv(ph, (0, 1), "all", sent)
        send_q(ph, sent)
    merge(1)
    sweep(0, [latent(quad, 1)])
    mix(1, 0)
    mix(1, 1)
    sweep(0, [ctx_block] + [latent(goal, 1) for goal in others], send=True)
    mix(1, 2)
    merge(0)
    mix(0, 0)
    mix(0, 1)
    mix(0, 2)
    square = jnp.zeros((rows, 1), F32)
    for n in range(chunks):
        mesh[n].wait_recv()
        value = mixed[n] + mesh_in[n].astype(F32)
        mixed[n] = value
        square = square + jnp.sum(value * value, axis=-1, keepdims=True)
    inv = lax.rsqrt(square / width + NORM_EPS)
    for n in range(chunks):
        at = slice(n * step_cols, (n + 1) * step_cols)
        gate = mod[0:1, 2 * width + n * step_cols : 2 * width + (n + 1) * step_cols]
        out_ref[:, at] = (lat[t, :, at].astype(F32) + gate * (mixed[n] * inv)).astype(BF16)

    given = [one for ph in range(2) for cc in range(2) for one in give(ph, cc)]
    for one in sends + given + cores[0] + cores[1] + mesh:
        one.wait_send()
    for ph in range(2):
        pass_on(ph, sent)
        for m in range(4):
            for cc in range(2):
                return_o(m, ph, cc, sent)
    send_ctx(sent)


def mix_kernel(
    tp_count, chunks,
    att_ref, wo_hbm, wo_ref, wo_sem, lat_ref, gate_ref,
    out_ref,
    core_out, core_in, mesh_out, mesh_in, mixed, core_send, core_recv, mesh_send, mesh_recv,
):
    s, t = lax.axis_index("sp"), lax.axis_index("tp")
    y, c = t // 2, t % 2
    y_count = tp_count // 2
    partner = y * 2 + 1 - c
    rows, width = lat_ref.shape
    step = width // chunks
    peers = [((y + j) % y_count) * 2 + c for j in range(1, y_count)]
    pltpu.make_async_copy(wo_hbm, wo_ref, wo_sem.at[0]).wait()

    def piece(n, j, cc):
        yy = (y + j) % y_count
        at = pl.ds(pl.multiple_of((yy * 2 + cc) * rows, rows), rows)
        return jnp.dot(
            att_ref[at, :], wo_ref[:, n * step : (n + 1) * step], preferred_element_type=F32
        )

    order = list(range(1, y_count)) + [0]
    cores = [
        remote(core_out.at[n], core_in.at[n], core_send.at[n], core_recv.at[n], (s, partner))
        for n in range(chunks)
    ]
    sent = []
    for n in range(chunks + 1):
        if n < chunks:
            for j in order:
                core_out[n, j] = piece(n, j, 1 - c).astype(BF16)
            cores[n].start()
        if n == 0:
            continue
        m = n - 1
        own = [piece(m, j, c) for j in order]
        cores[m].wait_recv()
        for j, value in zip(order, own):
            value = value + core_in[m, j].astype(F32)
            if j == 0:
                mixed[m] = value
            else:
                mesh_out[m, j - 1] = value.astype(BF16)
                one = remote(
                    mesh_out.at[m, j - 1], mesh_in.at[m, j - 1], mesh_send.at[m, j - 1],
                    mesh_recv.at[m, j - 1], (s, peers[j - 1]),
                )
                one.start()
                sent.append(one)
    for one in sent:
        one.wait_recv()
    square = jnp.zeros((rows, 1), F32)
    for n in range(chunks):
        value = mixed[n]
        for j in range(1, y_count):
            value = value + mesh_in[n, j - 1].astype(F32)
        mixed[n] = value
        square = square + jnp.sum(value * value, axis=-1, keepdims=True)
    inv = lax.rsqrt(square / width + NORM_EPS)
    for n in range(chunks):
        at = slice(n * step, (n + 1) * step)
        out_ref[:, at] = (
            lat_ref[:, at].astype(F32) + gate_ref[:, at] * (mixed[n] * inv)
        ).astype(BF16)
    for one in sent + cores:
        one.wait_send()


def whole_kernel(sp_count, tp_count, x_count, head_dim, group, lift, chunks, counts, *refs):
    (
        cond, cond_1, mw, lat, ctx, wq, wk, wv, qg, kg, cos, sin, wo, lat_rows,
        out, qt, k, vt, ckv, gate, att, wo_vm, wo_sem, *rest,
    ) = refs
    front, middle, last = counts
    front_scratch, middle_scratch = rest[:front], rest[front : front + middle]
    front_kernel(
        sp_count, tp_count, head_dim, cond, cond_1, mw, lat, ctx, wq, wk, wv, qg, kg, cos, sin,
        qt, k, vt, ckv, gate, *front_scratch, wo, wo_vm, wo_sem,
    )
    attend_kernel(sp_count, x_count, group, lift, k, vt, ckv, qt, att, *middle_scratch)
    mix_kernel(
        tp_count, chunks, att, wo, wo_vm, wo_sem, lat_rows, gate, out, *rest[front + middle :]
    )


ANY = pl.BlockSpec(memory_space=pl.ANY)
VM = pl.BlockSpec(memory_space=pltpu.VMEM)
DMA = pltpu.SemaphoreType.DMA


def grid_tables(sp_count, all_rows, head_dim):
    quarter, lines, lane = head_dim // 4, all_rows // GRID_W, np.arange(128)
    inv_freq = np.float32(ROPE_BASE) ** (-np.arange(quarter, dtype=np.float32) / quarter)
    rows = np.arange(sp_count)[:, None] * lines + lane[None, :] % lines
    both = np.stack([rows, np.broadcast_to(lane % GRID_W, rows.shape)], axis=1).astype(np.float32)
    angles = (both[:, :, None, :] * inv_freq[None, None, :, None]).astype(np.float32)
    return jnp.asarray(np.cos(angles)), jnp.asarray(np.sin(angles))


def quad_call(args, out_weight, sp_count, head_dim, lift):
    mod_weight, latents, context, query_weight, key_matrix, value_matrix = args[2:8]
    rows, width = latents.shape
    ctx_rows = context.shape[0]
    mod_cols = mod_weight.shape[1]
    all_rows, z_count, quads, chunks = 4 * rows, sp_count // 2, sp_count // 4, 4
    step = width // chunks
    cos, sin = grid_tables(sp_count, all_rows, head_dim)
    block = max(all_rows, z_count * ctx_rows)
    scratch = [
        pltpu.VMEM(args[0].shape, F32),
        pltpu.VMEM(args[1].shape, F32),
        pltpu.VMEM(args[8].shape, F32),
        pltpu.VMEM(args[9].shape, F32),
        pltpu.VMEM(cos.shape[1:], F32),
        pltpu.VMEM(sin.shape[1:], F32),
        DMA((6,)),
        pltpu.VMEM(mod_weight.shape, F32),
        pltpu.VMEM((4, rows, width), BF16),
        pltpu.VMEM((quads, ctx_rows, width), BF16),
        pltpu.VMEM(query_weight.shape, BF16),
        pltpu.VMEM(key_matrix.shape, BF16),
        pltpu.VMEM(value_matrix.shape, BF16),
        pltpu.VMEM(out_weight.shape, BF16),
        pltpu.VMEM((2, head_dim // 4, all_rows), F32),
        pltpu.VMEM((2, head_dim // 4, all_rows), F32),
        pltpu.VMEM((sp_count, 2, mod_cols), F32),
        pltpu.VMEM((4, 2, mod_cols), F32),
        pltpu.VMEM((2, 4 * mod_cols), F32),
        pltpu.VMEM((2 * rows, width), BF16),
        pltpu.VMEM((2 * rows, width), F32),
        pltpu.VMEM((4, 4, head_dim, rows), BF16),
        pltpu.VMEM((2, all_rows, head_dim), BF16),
        pltpu.VMEM((2, head_dim, all_rows), BF16),
        pltpu.VMEM((2, 2, quads * ctx_rows, head_dim), BF16),
        pltpu.VMEM((2, 2, 2, head_dim, all_rows), BF16),
        pltpu.VMEM((quads, 2, all_rows, head_dim), BF16),
        pltpu.VMEM((quads, 2, head_dim, all_rows), BF16),
        pltpu.VMEM((2, 2, quads * ctx_rows, head_dim), BF16),
        pltpu.VMEM((2, 2, 2, 2, all_rows), F32),
        pltpu.VMEM((2, 2, 2, head_dim, all_rows), F32),
        pltpu.VMEM((2, 2, 2, all_rows), F32),
        pltpu.VMEM((2, 2, head_dim, all_rows), F32),
        pltpu.VMEM((2, block, all_rows), F32),
        pltpu.VMEM((2, block, all_rows), BF16),
        pltpu.VMEM((2, 1, all_rows), F32),
        pltpu.VMEM((4, 2, 2 * rows, head_dim), BF16),
        pltpu.VMEM((all_rows, 4 * head_dim), BF16),
        pltpu.VMEM((2, chunks, rows, step), BF16),
        pltpu.VMEM((2, chunks, rows, step), BF16),
        pltpu.VMEM((chunks, rows, step), BF16),
        pltpu.VMEM((chunks, rows, step), BF16),
        pltpu.VMEM((chunks, rows, step), F32),
        DMA((7,)),
        DMA((7,)),
        DMA((7,)),
        DMA((sp_count,)),
        DMA((sp_count,)),
        DMA((4,)),
        DMA((4,)),
        DMA((2, 2, quads, 2)),
        DMA((2, 2, z_count)),
        DMA((2,)),
        DMA((2,)),
        DMA((2, 2, 2)),
        DMA((2, 4, 2)),
        DMA((4, 2)),
        DMA((4, quads)),
        DMA((2, quads)),
        DMA((2, quads)),
        DMA((2, 2)),
        DMA((2, 2)),
        DMA((2, 2)),
        DMA((2, 2)),
        DMA((4, 2, 2)),
        DMA((2, chunks)),
        DMA((chunks,)),
        DMA((chunks,)),
    ]
    out = pl.pallas_call(
        functools.partial(quad_kernel, sp_count, head_dim, lift, chunks),
        out_shape=pltpu.VMEM((rows, width), BF16),
        in_specs=[pl.BlockSpec(memory_space=pltpu.HBM)] * 13,
        out_specs=VM,
        scratch_shapes=scratch,
        compiler_params=pltpu.CompilerParams(
            collective_id=0, has_side_effects=True, vmem_limit_bytes=VMEM_BYTES - 2 * rows * width * 2
        ),
        name="quad",
    )(*args, cos, sin, out_weight)
    return out


def body(
    latents,
    context,
    cond,
    ctx_cond,
    mod_weight,
    query_weight,
    key_matrix,
    value_matrix,
    out_weight,
    query_gain,
    key_gain,
):
    sp_count, tp_count = lax.axis_size("sp"), lax.axis_size("tp")
    x_count = row_size(sp_count)
    rows, width = latents.shape
    ctx_rows = context.shape[0]
    head_dim = query_gain.shape[0]
    heads = query_weight.shape[1] // head_dim
    kv_heads = key_matrix.shape[1] // head_dim
    all_rows = rows * tp_count
    mod_cols = mod_weight.shape[1]
    lift = math.log(sp_count * all_rows / (2.0 * sp_count * ctx_rows))
    group = heads // kv_heads
    args = (
        cond[None], ctx_cond[None], mod_weight, latents, context, query_weight, key_matrix, value_matrix,
        query_gain[None], key_gain[None],
    )
    wide = all_rows % GRID_W == 0 and all_rows == rows * 4 and rows % 128 == 0
    if wide and kv_heads == 2 and group == 2 and x_count == 2 and sp_count % 4 == 0 and ctx_rows % 32 == 0:
        return quad_call(args, out_weight, sp_count, head_dim, lift)
    chunks = 4
    y_count = tp_count // 2
    step = width // chunks
    far = max(y_count - 1, 1)
    positions = lax.axis_index("sp") * all_rows + jnp.arange(all_rows, dtype=jnp.int32)
    cos, sin = tables(positions, head_dim)
    shared = [
        pltpu.VMEM((heads, head_dim, all_rows), BF16),
        pltpu.VMEM((kv_heads, all_rows, head_dim), BF16),
        pltpu.VMEM((kv_heads, head_dim, all_rows), BF16),
        pltpu.VMEM((kv_heads, 2, ctx_rows, head_dim), BF16),
        pltpu.VMEM((1, width), F32),
        pltpu.VMEM((all_rows, heads * head_dim), BF16),
        pltpu.VMEM(out_weight.shape, BF16),
        DMA((1,)),
    ]
    front = [
        pltpu.VMEM(mod_weight.shape, F32),
        pltpu.VMEM((tp_count, rows, width), BF16),
        pltpu.VMEM(query_weight.shape, BF16),
        pltpu.VMEM(key_matrix.shape, BF16),
        pltpu.VMEM(value_matrix.shape, BF16),
        pltpu.VMEM((sp_count, 2, mod_cols), F32),
        pltpu.VMEM((tp_count, 2, mod_cols), F32),
        pltpu.VMEM((2, mod_cols * tp_count), F32),
        pltpu.VMEM((2 * rows, width), BF16),
        DMA((5,)),
        DMA((tp_count,)),
        DMA((tp_count,)),
        DMA((sp_count,)),
        DMA((sp_count,)),
        DMA((tp_count,)),
        DMA((tp_count,)),
    ]
    middle = [
        pltpu.VMEM((sp_count, kv_heads, all_rows, head_dim), BF16),
        pltpu.VMEM((sp_count, kv_heads, head_dim, all_rows), BF16),
        pltpu.VMEM((sp_count, kv_heads, 2, ctx_rows, head_dim), BF16),
        pltpu.VMEM((heads, 1, all_rows), F32),
        pltpu.VMEM((heads, 1, all_rows), F32),
        pltpu.VMEM((heads, head_dim, all_rows), F32),
        DMA((3,)),
    ]
    middle += [DMA((3, sp_count, x_count + 1)), DMA((3, sp_count))]
    last = [
        pltpu.VMEM((chunks, y_count, rows, step), BF16),
        pltpu.VMEM((chunks, y_count, rows, step), BF16),
        pltpu.VMEM((chunks, far, rows, step), BF16),
        pltpu.VMEM((chunks, far, rows, step), BF16),
        pltpu.VMEM((chunks, rows, step), F32),
        DMA((chunks,)),
        DMA((chunks,)),
        DMA((chunks, far)),
        DMA((chunks, far)),
    ]
    counts = (len(front), len(middle), len(last))
    return pl.pallas_call(
        functools.partial(
            whole_kernel, sp_count, tp_count, x_count, head_dim, group, lift, chunks, counts
        ),
        out_shape=jax.ShapeDtypeStruct((rows, width), BF16),
        in_specs=[VM, VM, ANY, ANY, VM, ANY, ANY, ANY, VM, VM, VM, VM, ANY, VM],
        out_specs=VM,
        scratch_shapes=shared + front + middle + last,
        compiler_params=pltpu.CompilerParams(
            collective_id=0, has_side_effects=True, vmem_limit_bytes=VMEM_BYTES
        ),
        name="whole",
    )(
        *args, cos, sin, out_weight, latents,
    )


def solution(mesh):
    placed = (
        P(("sp", "tp"), None),
        P("sp", None),
        P("sp"),
        P("sp"),
        P("sp", "tp"),
        P(None, "tp"),
        P(None, "tp"),
        P(None, "tp"),
        P("tp", None),
        P(),
        P(),
    )
    return jax.shard_map(
        body, mesh=mesh, in_specs=placed, out_specs=P(("sp", "tp"), None), check_vma=False
    )
```
